32 devices in a mesh: sp: 16 (over z, y, x), tp: 2 (over core).
Axes of the slice: x: 2, y: 2, z: 4, core: 2. Of those that a mesh axis runs over, the one named last changes fastest.
Arguments:
- tokens: bfloat16 [4096, 2048], P(('sp', 'tp')), may hold values from -6 to 6
- mix_gain: float32 [2048], replicated, may hold values from 0.1 to 1.9
- query_proj: bfloat16 [2048, 1536], P(None, 'tp'), may hold values from -4 to 4
- compressed_projection: bfloat16 [2048, 256], replicated, may hold values from -0.125 to 0.125
- compressed_norm_gain: float32 [256], replicated, may hold values from 0.1 to 1.9
- rope_proj: bfloat16 [2048, 64], replicated, may hold values from -0.125 to 0.125
- key_up: bfloat16 [256, 1024], P(None, 'tp'), may hold values from -4 to 4
- value_up_weight: bfloat16 [256, 1024], P(None, 'tp'), may hold values from -0.375 to 0.375
- scan_input: bfloat16 [2048, 2048], P('sp', 'tp'), may hold values from -0.125 to 0.125
- scan_gate: bfloat16 [2048, 2048], P('sp', 'tp'), may hold values from -0.125 to 0.125
- scan_write: bfloat16 [2048, 1024], P('sp', 'tp'), may hold values from -0.125 to 0.125
- scan_read: bfloat16 [2048, 1024], P('sp', 'tp'), may hold values from -0.125 to 0.125
- step_proj: bfloat16 [2048, 32], replicated, may hold values from -0.125 to 0.125
- conv_input: bfloat16 [4, 2048], P(None, 'tp'), may hold values from -3 to 3
- conv_write: bfloat16 [4, 1024], P(None, 'tp'), may hold values from -3 to 3
- conv_read: bfloat16 [4, 1024], P(None, 'tp'), may hold values from -3 to 3
- decay_log: float32 [32], P('tp'), may hold values from -16 to -2.8
- decay_offset: float32 [4096, 32], P('sp', 'tp'), may hold values from -2.2 to 0
- skip_gain: float32 [32], P('tp'), may hold values from 0.1 to 1.9
- group_gain: float32 [2048], P('tp'), may hold values from 0.1 to 1.9
Outputs:
- attended: bfloat16 [4096, 1024], P('sp', 'tp')
- scanned: bfloat16 [4096, 2048], P('sp', 'tp')
The draws below stay inside these ranges and needn't reach their ends.
All inputs are finite; a program needn't handle non-finite values.
Results may differ from the reference program's by a relative error of at most 0.017.
The reference program's roundings to bfloat16 on the way count: a program that leaves them out, or rounds other values in their place, can miss the bound.
Values may be sent and summed in bfloat16 or wider, within the bound.
A program may use at most 128 MiB of HBM per device.

```python
import jax
import jax.numpy as jnp
from jax import lax

MODEL_WIDTH = 2048
ATTENTION_HEADS = 8
UNROTATED_WIDTH = 128
ROPE = 64
VALUE_WIDTH = 128
LATENT_KEY_WIDTH = 256
SSM_HEADS = 32
SSM_DIM = 64
SSM_GROUPS = 8
SSM_STATE = 128
CONV = 4
BLOCK = 128
TOK_DEV = 256
SEQ = 4096


def draw_decay_log(key, part):
    pick_key, fast_key, slow_key = jax.random.split(jax.random.fold_in(key, 11), 3)
    fast = jax.random.uniform(pick_key, (SSM_HEADS,), jnp.float32) < 0.5
    fast_rate = jnp.exp(jax.random.uniform(fast_key, (SSM_HEADS,), jnp.float32, jnp.log(0.02), jnp.log(0.06)))
    slow_rate = jnp.exp(jax.random.uniform(slow_key, (SSM_HEADS,), jnp.float32, jnp.log(0.05), jnp.log(0.3))) / SEQ
    return jnp.log(jnp.where(fast, fast_rate, slow_rate)).astype(jnp.float32)


def draw_decay_offset(key, part):
    rate_key, place_key, depth_key = jax.random.split(jax.random.fold_in(key, 23), 3)
    blocks = SEQ // TOK_DEV
    rates = jnp.exp(jax.random.uniform(rate_key, (blocks, SSM_HEADS), jnp.float32, jnp.log(0.1), jnp.log(0.6)))
    reference_amount = -jnp.repeat(rates, TOK_DEV, axis=0) / SEQ
    places = jax.random.randint(place_key, (3,), 0, SEQ)
    layer_tiers = jnp.log(jax.random.uniform(depth_key, (3,), jnp.float32, 0.5, 0.8))
    match_flags = (jnp.arange(SEQ)[:, None] == places[None, :]).astype(jnp.float32)
    sudden_outlier = jnp.dot(match_flags, layer_tiers)[:, None]
    return (reference_amount + sudden_outlier).astype(jnp.float32)


def shared_direction(key):
    order_key, strength_key, direction_key = jax.random.split(jax.random.fold_in(key, 37), 3)
    chosen = (jax.random.permutation(order_key, ATTENTION_HEADS) < ATTENTION_HEADS // 2).astype(jnp.float32)
    strength = jnp.exp(jax.random.uniform(strength_key, (ATTENTION_HEADS,), jnp.float32, jnp.log(6.0), jnp.log(18.0)))
    direction = jax.random.normal(direction_key, (ATTENTION_HEADS, UNROTATED_WIDTH), jnp.float32)
    direction = direction / jnp.sqrt(jnp.sum(direction * direction, axis=1, keepdims=True))
    magnitude = jnp.sqrt(strength * jnp.sqrt(jnp.float32(UNROTATED_WIDTH + ROPE)))
    return direction * (magnitude * chosen)[:, None]


def draw_query_proj(key, part):
    planted = shared_direction(key)
    noise_random_key, along_sequence_key = jax.random.split(jax.random.fold_in(key, 41))
    reference_amount = jnp.clip(jax.random.normal(noise_random_key, (MODEL_WIDTH, ATTENTION_HEADS * (UNROTATED_WIDTH + ROPE)), jnp.float32), -6.0, 6.0) / jnp.sqrt(jnp.float32(MODEL_WIDTH))
    along_sequence = jax.random.normal(along_sequence_key, (MODEL_WIDTH,), jnp.float32)
    along_sequence = along_sequence / jnp.sqrt(jnp.sum(along_sequence * along_sequence))
    padded = jnp.concatenate([planted, jnp.zeros((ATTENTION_HEADS, ROPE), jnp.float32)], axis=1).reshape(ATTENTION_HEADS * (UNROTATED_WIDTH + ROPE))
    return jnp.clip(reference_amount + along_sequence[:, None] * padded[None, :], -4.0, 4.0).astype(jnp.bfloat16)


def draw_key_up(key, part):
    planted = shared_direction(key)
    noise_random_key, along_sequence_key = jax.random.split(jax.random.fold_in(key, 43))
    reference_amount = jnp.clip(jax.random.normal(noise_random_key, (LATENT_KEY_WIDTH, ATTENTION_HEADS * UNROTATED_WIDTH), jnp.float32), -6.0, 6.0) / jnp.sqrt(jnp.float32(LATENT_KEY_WIDTH))
    along_sequence = jax.random.normal(along_sequence_key, (LATENT_KEY_WIDTH,), jnp.float32)
    along_sequence = along_sequence / jnp.sqrt(jnp.sum(along_sequence * along_sequence))
    flat = planted.reshape(ATTENTION_HEADS * UNROTATED_WIDTH)
    return jnp.clip(reference_amount + along_sequence[:, None] * flat[None, :], -4.0, 4.0).astype(jnp.bfloat16)


def levels(own_key, shape, cuts, low, top_value):
    def one(dim, shards_of):
        draws = jax.random.uniform(jax.random.fold_in(jax.random.fold_in(own_key, 6), dim), (shards_of,), jnp.float32, low / len(cuts), top_value / len(cuts))
        return jnp.repeat(jnp.exp(draws), shape[dim] // shards_of).reshape((-1,) + (1,) * (len(shape) - dim - 1))

    level = one(*cuts[0])
    for cut in cuts[1:]:
        level = level * one(*cut)
    return level


def gaussian(own_key, extent, deviation, bound, shards=(), kind=jnp.bfloat16):
    drawn = jax.random.normal(own_key, extent, jnp.float32) * deviation
    if len(shards) > 0:
        drawn = levels(own_key, extent, shards, -0.22, 0.18) * drawn
    return jnp.clip(drawn, min=-bound, max=bound).astype(kind)


def setup_inputs(seed: int = 0) -> dict:
    seeds = jax.random.split(jax.random.key(seed), 21)
    return {
        "tokens": gaussian(seeds[0], (SEQ, MODEL_WIDTH), 1.0, 6.0, ((0, 32),)),
        "mix_gain": jnp.clip(1.0 + 0.18 * jax.random.normal(seeds[1], (MODEL_WIDTH,), jnp.float32), 0.1, 1.9),
        "query_proj": draw_query_proj(jax.random.fold_in(seeds[20], 71), 0),
        "compressed_projection": gaussian(seeds[3], (MODEL_WIDTH, LATENT_KEY_WIDTH), MODEL_WIDTH ** -0.5, 0.125),
        "compressed_norm_gain": jnp.clip(1.0 + 0.18 * jax.random.normal(seeds[4], (LATENT_KEY_WIDTH,), jnp.float32), 0.1, 1.9),
        "rope_proj": gaussian(seeds[5], (MODEL_WIDTH, ROPE), MODEL_WIDTH ** -0.5, 0.125),
        "key_up": draw_key_up(jax.random.fold_in(seeds[20], 71), 0),
        "value_up_weight": gaussian(seeds[7], (LATENT_KEY_WIDTH, ATTENTION_HEADS * VALUE_WIDTH), LATENT_KEY_WIDTH ** -0.5, 0.375, ((1, 2),)),
        "scan_input": gaussian(seeds[8], (MODEL_WIDTH, SSM_HEADS * SSM_DIM), MODEL_WIDTH ** -0.5, 0.125, ((0, 16), (1, 2))),
        "scan_gate": gaussian(seeds[9], (MODEL_WIDTH, SSM_HEADS * SSM_DIM), MODEL_WIDTH ** -0.5, 0.125, ((0, 16), (1, 2))),
        "scan_write": gaussian(seeds[10], (MODEL_WIDTH, SSM_GROUPS * SSM_STATE), MODEL_WIDTH ** -0.5, 0.125, ((0, 16), (1, 2))),
        "scan_read": gaussian(seeds[11], (MODEL_WIDTH, SSM_GROUPS * SSM_STATE), MODEL_WIDTH ** -0.5, 0.125, ((0, 16), (1, 2))),
        "step_proj": gaussian(seeds[12], (MODEL_WIDTH, SSM_HEADS), MODEL_WIDTH ** -0.5, 0.125),
        "conv_input": gaussian(seeds[13], (CONV, SSM_HEADS * SSM_DIM), CONV ** -0.5, 3.0, ((1, 2),)),
        "conv_write": gaussian(seeds[14], (CONV, SSM_GROUPS * SSM_STATE), CONV ** -0.5, 3.0, ((1, 2),)),
        "conv_read": gaussian(seeds[15], (CONV, SSM_GROUPS * SSM_STATE), CONV ** -0.5, 3.0, ((1, 2),)),
        "decay_log": draw_decay_log(jax.random.fold_in(seeds[20], 71), 0),
        "decay_offset": draw_decay_offset(jax.random.fold_in(seeds[20], 71), 0),
        "skip_gain": jnp.clip(1.0 + 0.18 * jax.random.normal(seeds[18], (SSM_HEADS,), jnp.float32), 0.1, 1.9),
        "group_gain": jnp.clip(1.0 + 0.18 * jax.random.normal(seeds[19], (SSM_HEADS * SSM_DIM,), jnp.float32), 0.1, 1.9),
    }


eps = 1e-06
theta = 10000.0
floor_score = -1e+30

def rms_scale(values, gain):
    wide = values.astype(jnp.float32)
    return wide * lax.rsqrt(lax.optimization_barrier(jnp.mean(wide * wide, axis=-1, keepdims=True)) + eps) * gain

def rotate(values, positions):
    half = values.shape[-1] // 2
    freqs = theta ** (-jnp.arange(half, dtype=jnp.float32) * 2.0 / values.shape[-1])
    angle = positions.astype(jnp.float32)[:, None] * freqs[None, :]
    cosine = jnp.cos(angle)
    sine = jnp.sin(angle)
    if values.ndim == 3:
        cosine = cosine[:, None, :]
        sine = sine[:, None, :]
    first = values[..., :half]
    second = values[..., half:]
    return jnp.concatenate([first * cosine - second * sine, second * cosine + first * sine], axis=-1)

def short_conv(values, edge, taps):
    span = taps.shape[0]
    length = values.shape[0]
    padded = jnp.concatenate([edge, values], axis=0).astype(jnp.float32)
    result = jnp.zeros(values.shape, jnp.float32)
    for index in range(span):
        result = result + taps[index].astype(jnp.float32)[None, :] * padded[index:index + length]
    return jax.nn.silu(result).astype(jnp.bfloat16)

def blockwise_scan(heads, steps, decays, writes, reads, state, block):
    count = heads.shape[0] // block
    best = lax.Precision.HIGHEST

    def split(values):
        return values.reshape((count, block) + values.shape[1:])

    def one_block(state, inputs):
        head_block, step_block, decay_block, write_block, read_block = inputs
        running = jnp.cumsum(decay_block, axis=0)
        causal = jnp.tril(jnp.ones((block, block), dtype=bool))[:, :, None, None]
        spread = running[:, None] - running[None, :]
        fading = jnp.where(causal, jnp.exp(jnp.where(causal, spread, 0.0)), 0.0)
        inner = jnp.einsum('lgn,sgn->lsg', read_block, write_block, precision=best)
        mixing = inner[..., None] * fading * step_block[None]
        within = jnp.einsum('lsgr,sgrp->lgrp', mixing, head_block, precision=best)
        carried = jnp.einsum('lgn,grpn->lgrp', read_block, state, precision=best) * jnp.exp(running)[..., None]
        to_end = jnp.exp(running[-1:] - running) * step_block
        update = jnp.einsum('sgn,sgr,sgrp->grpn', write_block, to_end, head_block, precision=best)
        state = jnp.exp(running[-1])[..., None, None] * state + update
        return (state, within + carried)
    state, outputs = lax.scan(one_block, state, (split(heads), split(steps), split(decays), split(writes), split(reads)))
    return (state, outputs.reshape(heads.shape))

def gated_norm(mixed, gate, gain):
    length = mixed.shape[0]
    groups = mixed.shape[1]
    flat = mixed.reshape(length, groups, -1)
    gated = flat * jax.nn.silu(gate.astype(jnp.float32)).reshape(length, groups, -1)
    scaled = gated * lax.rsqrt(lax.optimization_barrier(jnp.mean(gated * gated, axis=-1, keepdims=True)) + eps)
    return (scaled * gain.reshape(groups, -1)[None]).reshape(length, -1).astype(jnp.bfloat16)

def reference(tokens, mix_gain, query_proj, compressed_projection, compressed_norm_gain, rope_proj, key_up, value_up_weight, scan_input, scan_gate, scan_write, scan_read, step_proj, conv_input, conv_write, conv_read, decay_log, decay_offset, skip_gain, group_gain):
    positions = jnp.arange(SEQ, dtype=jnp.int32)
    normed = rms_scale(tokens, mix_gain).astype(jnp.bfloat16)
    query = jnp.dot(normed, query_proj, preferred_element_type=jnp.float32).astype(jnp.bfloat16)
    query = query.reshape(SEQ, ATTENTION_HEADS, UNROTATED_WIDTH + ROPE)
    query_plain = query[:, :, :UNROTATED_WIDTH]
    query_turned = rotate(query[:, :, UNROTATED_WIDTH:].astype(jnp.float32), positions).astype(jnp.bfloat16)
    latent = rms_scale(jnp.dot(normed, compressed_projection, preferred_element_type=jnp.float32), compressed_norm_gain).astype(jnp.bfloat16)
    key_turned = rotate(jnp.dot(normed, rope_proj, preferred_element_type=jnp.float32), positions).astype(jnp.bfloat16)
    key_plain = jnp.dot(latent, key_up, preferred_element_type=jnp.float32).astype(jnp.bfloat16).reshape(SEQ, ATTENTION_HEADS, UNROTATED_WIDTH)
    values = jnp.dot(latent, value_up_weight, preferred_element_type=jnp.float32).astype(jnp.bfloat16).reshape(SEQ, ATTENTION_HEADS, VALUE_WIDTH)
    scale = (UNROTATED_WIDTH + ROPE) ** (-0.5)

    def one_query_block(index):
        start = index * TOK_DEV
        q_plain = lax.dynamic_slice_in_dim(query_plain, start, TOK_DEV, 0).astype(jnp.float32)
        q_turned = lax.dynamic_slice_in_dim(query_turned, start, TOK_DEV, 0).astype(jnp.float32)
        q_positions = start + jnp.arange(TOK_DEV, dtype=jnp.int32)

        def visit(step, carry):
            highest, total, summed = carry
            k_start = step * TOK_DEV
            k_plain = lax.dynamic_slice_in_dim(key_plain, k_start, TOK_DEV, 0).astype(jnp.float32)
            k_turned = lax.dynamic_slice_in_dim(key_turned, k_start, TOK_DEV, 0).astype(jnp.float32)
            k_values = lax.dynamic_slice_in_dim(values, k_start, TOK_DEV, 0).astype(jnp.float32)
            k_positions = k_start + jnp.arange(TOK_DEV, dtype=jnp.int32)
            scores = jnp.einsum('qhd,khd->hqk', q_plain, k_plain) + jnp.einsum('qhd,kd->hqk', q_turned, k_turned)
            scores = scores * scale
            scores = jnp.where(k_positions[None, None, :] <= q_positions[None, :, None], scores, -jnp.inf)
            new_highest = jnp.maximum(highest, lax.optimization_barrier(jnp.max(scores, axis=-1)))
            weights = jnp.exp(scores - new_highest[..., None])
            shrink = jnp.exp(highest - new_highest)
            total = total * shrink + lax.optimization_barrier(jnp.sum(weights, axis=-1))
            rounded = lax.optimization_barrier(weights.astype(jnp.bfloat16)).astype(jnp.float32)
            summed = summed * shrink[..., None] + jnp.einsum('hqk,khd->hqd', rounded, k_values)
            return (new_highest, total, summed)
        initial_recurrent = (jnp.full((ATTENTION_HEADS, TOK_DEV), floor_score, jnp.float32), jnp.zeros((ATTENTION_HEADS, TOK_DEV), jnp.float32), jnp.zeros((ATTENTION_HEADS, TOK_DEV, VALUE_WIDTH), jnp.float32))
        highest, total, summed = lax.fori_loop(0, index + 1, visit, initial_recurrent)
        return (summed / total[..., None]).astype(jnp.bfloat16)
    blocks = lax.map(one_query_block, jnp.arange(SEQ // TOK_DEV, dtype=jnp.int32))
    attended = jnp.transpose(blocks, (0, 2, 1, 3)).reshape(SEQ, ATTENTION_HEADS * VALUE_WIDTH)
    groups = SSM_GROUPS
    per_group = SSM_HEADS // SSM_GROUPS
    head_raw = jnp.dot(normed, scan_input, preferred_element_type=jnp.float32).astype(jnp.bfloat16)
    gate = jnp.dot(normed, scan_gate, preferred_element_type=jnp.float32).astype(jnp.bfloat16)
    write_raw = jnp.dot(normed, scan_write, preferred_element_type=jnp.float32).astype(jnp.bfloat16)
    read_raw = jnp.dot(normed, scan_read, preferred_element_type=jnp.float32).astype(jnp.bfloat16)
    step_size = jax.nn.softplus(jnp.dot(normed, step_proj, preferred_element_type=jnp.float32))
    heads = short_conv(head_raw, jnp.zeros((CONV - 1, head_raw.shape[1]), jnp.bfloat16), conv_input)
    writes = short_conv(write_raw, jnp.zeros((CONV - 1, write_raw.shape[1]), jnp.bfloat16), conv_write)
    reads = short_conv(read_raw, jnp.zeros((CONV - 1, read_raw.shape[1]), jnp.bfloat16), conv_read)
    log_decay = -jnp.exp(decay_log)[None, :] * step_size + decay_offset
    head_values = heads.astype(jnp.float32).reshape(SEQ, groups, per_group, SSM_DIM)
    step_values = step_size.reshape(SEQ, groups, per_group)
    decay_values = log_decay.reshape(SEQ, groups, per_group)
    write_values = writes.astype(jnp.float32).reshape(SEQ, groups, SSM_STATE)
    output_entries = reads.astype(jnp.float32).reshape(SEQ, groups, SSM_STATE)
    empty_state = jnp.zeros((groups, per_group, SSM_DIM, SSM_STATE), jnp.float32)
    final_state, mixed = blockwise_scan(head_values, step_values, decay_values, write_values, output_entries, empty_state, BLOCK)
    mixed = mixed + skip_gain.reshape(groups, per_group)[None, :, :, None] * head_values
    scanned = gated_norm(mixed, gate, group_gain)
    return (attended, scanned)
```

```python
import jax
import jax.numpy as jnp
from jax import lax
from jax.experimental import pallas as pl
from jax.experimental.pallas import tpu as pltpu
from jax.sharding import PartitionSpec as P

UNROTATED_WIDTH = 128
ROPE = 64
VALUE_WIDTH = 128
SSM_DIM = 64
SSM_STATE = 128


eps = 1e-06
theta = 10000.0
floor_score = -1e30


def from_behind(value, axis, steps):
    count = lax.axis_size(axis)
    initial, last = (max(0, -steps), min(count, count - steps))
    return lax.ppermute(value, axis, [(source, source + steps) for source in range(initial, last)])


def rms_scale(values, gain):
    wide = values.astype(jnp.float32)
    return wide * lax.rsqrt(jnp.mean(wide * wide, axis=-1, keepdims=True) + eps) * gain


def rotate(values, positions):
    half = values.shape[-1] // 2
    freqs = theta ** (-jnp.arange(half, dtype=jnp.float32) * 2.0 / values.shape[-1])
    angle = positions.astype(jnp.float32)[:, None] * freqs[None, :]
    cosine = jnp.cos(angle)
    sine = jnp.sin(angle)
    if values.ndim == 3:
        cosine = cosine[:, None, :]
        sine = sine[:, None, :]
    first = values[..., :half]
    second = values[..., half:]
    return jnp.concatenate(
        [first * cosine - second * sine, second * cosine + first * sine], axis=-1
    )


def short_conv(values, edge, taps):
    span = taps.shape[0]
    length = values.shape[0]
    padded = jnp.concatenate([edge, values], axis=0).astype(jnp.float32)
    result = jnp.zeros(values.shape, jnp.float32)
    for index in range(span):
        result = result + taps[index].astype(jnp.float32)[None, :] * padded[index : index + length]
    return jax.nn.silu(result).astype(jnp.bfloat16)


def local_scan(heads, steps, decays, writes, reads):
    length = decays.shape[-1]
    running = jnp.einsum(
        "grs,ls->grl",
        decays,
        jnp.tril(jnp.ones((length, length), jnp.float32)),
        precision=lax.Precision.HIGHEST,
    )
    causal = jnp.tril(jnp.ones((length, length), dtype=bool))
    spread = jnp.where(causal, running[..., :, None] - running[..., None, :], -jnp.inf)
    inner = jnp.einsum("gln,gsn->gls", reads, writes, preferred_element_type=jnp.float32)
    mixing = inner[:, None] * jnp.exp(spread) * steps[:, :, None, :]
    within = jnp.einsum(
        "grls,grsp->grlp",
        mixing.astype(jnp.bfloat16),
        heads,
        preferred_element_type=jnp.float32,
    )
    to_end = jnp.exp(running[..., -1:] - running) * steps
    weighted = (heads.astype(jnp.float32) * to_end[..., None]).astype(jnp.bfloat16)
    state = jnp.einsum(
        "grsp,gsn->grpn", weighted, writes, preferred_element_type=jnp.float32
    )
    return running, state, within


def exchange(items, plane, name, number, columns=False):
    devices, cores = lax.axis_size("sp"), lax.axis_size("tp")
    planes = devices // plane
    counts = [{"plane": plane, "line": planes, "all": devices}[item[1]] for item in items]
    amount = len(items)
    starts = [sum(counts[:i]) for i in range(amount)]
    shared = any(item[2] for item in items)

    def kernel(*refs):
        ins, outs = refs[:amount], refs[amount : 2 * amount]
        send, recv, pass_send, pass_recv, own = refs[2 * amount :]
        here, core = lax.axis_index("sp"), lax.axis_index("tp")
        across, within = here // plane, here % plane

        def place(reach, step):
            if reach == "plane":
                slot = (within + step + plane) % plane
                return across * plane + slot, slot
            if reach == "line":
                slot = (across + step + planes) % planes
                return slot * plane + within, slot
            up, along = step // plane, step % plane
            if step < 0:
                up, along = -((-step) // plane), -((-step) % plane)
            slot = (across + up + planes) % planes * plane + (within + along + plane) % plane
            return slot, slot

        barrier = pltpu.get_barrier_semaphore()
        greeted = 0
        for reach in ("plane", "line"):
            if not any(item[1] in (reach, "all") for item in items):
                continue
            size = {"plane": plane, "line": planes}[reach]
            for step in range(1, size):
                pl.semaphore_signal(
                    barrier,
                    inc=1,
                    device_id=(place(reach, step)[0], core),
                    device_id_type=pl.DeviceIdType.MESH,
                )
                greeted += 1
        if shared:
            for turn in range(1, cores):
                pl.semaphore_signal(
                    barrier,
                    inc=1,
                    device_id=(here, (core + turn) % cores),
                    device_id_type=pl.DeviceIdType.MESH,
                )
                greeted += 1
        pl.semaphore_wait(barrier, greeted)

        def target(i, slot, who):
            if columns:
                size = ins[i].shape[-1]
                return outs[i].at[:, pl.ds(pl.multiple_of(slot * size, size), size)]
            return outs[i].at[slot, who] if items[i][2] else outs[i].at[slot]

        def sent(i, step):
            goal, goal_slot = place(items[i][1], step)
            mine = place(items[i][1], 0)[1]
            if items[i][1] == "all" and step % plane and step >= plane:
                from_line = place("all", -(step // plane * plane))[1]
                return pltpu.make_async_remote_copy(
                    src_ref=target(i, from_line, core),
                    dst_ref=target(i, from_line, core),
                    send_sem=send.at[starts[i] + step],
                    recv_sem=recv.at[starts[i] + step],
                    device_id=(place("plane", step % plane)[0], core),
                    device_id_type=pl.DeviceIdType.MESH,
                )
            return pltpu.make_async_remote_copy(
                src_ref=ins[i].at[goal_slot] if items[i][3] else ins[i],
                dst_ref=target(i, mine, core),
                send_sem=send.at[starts[i] + step],
                recv_sem=recv.at[starts[i] + step],
                device_id=(goal, core),
                device_id_type=pl.DeviceIdType.MESH,
            )

        def arrived(i, step):
            slot = place(items[i][1], -step)[1]
            return pltpu.make_async_remote_copy(
                src_ref=ins[i].at[slot] if items[i][3] else ins[i],
                dst_ref=target(i, slot, core),
                send_sem=send.at[starts[i] + step],
                recv_sem=recv.at[starts[i] + step],
                device_id=(here, core),
                device_id_type=pl.DeviceIdType.MESH,
            )

        def passed(i, step, turn, outgoing):
            slot = place(items[i][1], -step)[1]
            other = (core + turn) % cores
            owner = core if outgoing else (core - turn + cores) % cores
            return pltpu.make_async_remote_copy(
                src_ref=ins[i] if step == 0 else target(i, slot, core),
                dst_ref=target(i, slot, owner),
                send_sem=pass_send.at[(starts[i] + step) * cores + turn],
                recv_sem=pass_recv.at[(starts[i] + step) * cores + turn],
                device_id=(here, other),
                device_id_type=pl.DeviceIdType.MESH,
            )

        kept = []
        for i in range(amount):
            if items[i][1] == "all":
                for up in range(1, planes):
                    sent(i, up * plane).start()
                for step in range(1, plane):
                    sent(i, step).start()
        for i in range(amount):
            if items[i][1] != "all":
                for step in range(1, counts[i]):
                    sent(i, step).start()
        for i in range(amount):
            slot = place(items[i][1], 0)[1]
            local = pltpu.make_async_copy(
                ins[i].at[slot] if items[i][3] else ins[i], target(i, slot, core), own.at[i]
            )
            local.start()
            kept.append(local)
            if items[i][2]:
                for turn in range(1, cores):
                    passed(i, 0, turn, True).start()
        for i in range(amount):
            if items[i][1] == "all":
                for up in range(1, planes):
                    arrived(i, up * plane).wait_recv()
                    for step in range(up * plane + 1, (up + 1) * plane):
                        sent(i, step).start()
                    for turn in range(1, cores):
                        passed(i, up * plane, turn, True).start()
        for i in range(amount):
            for step in range(1, counts[i]):
                if items[i][1] == "all" and step % plane == 0:
                    continue
                arrived(i, step).wait_recv()
                if items[i][2]:
                    for turn in range(1, cores):
                        passed(i, step, turn, True).start()
        for i in range(amount):
            kept[i].wait()
            for step in range(counts[i]):
                if step > 0:
                    sent(i, step).wait_send()
                if items[i][2]:
                    for turn in range(1, cores):
                        passed(i, step, turn, True).wait_send()
                        passed(i, step, turn, False).wait_recv()

    shapes = []
    for (array, reach, over, selected), count in zip(items, counts):
        lead = (count, cores) if over else (count,)
        tail = array.shape[1:] if selected else array.shape
        if columns:
            lead, tail = (), (tail[0], count * tail[1])
        shapes.append(jax.ShapeDtypeStruct(lead + tail, array.dtype))
    slots = sum(counts)
    return pl.pallas_call(
        kernel,
        out_shape=shapes,
        in_specs=[pl.BlockSpec(memory_space=pltpu.VMEM)] * amount,
        out_specs=[pl.BlockSpec(memory_space=pl.ANY)] * amount,
        scratch_shapes=[
            pltpu.SemaphoreType.DMA((slots,)),
            pltpu.SemaphoreType.DMA((slots,)),
            pltpu.SemaphoreType.DMA((slots * cores,)),
            pltpu.SemaphoreType.DMA((slots * cores,)),
            pltpu.SemaphoreType.DMA((amount,)),
        ],
        compiler_params=pltpu.CompilerParams(
            collective_id=number, has_side_effects=True, vmem_limit_bytes=16 * 1024 * 1024
        ),
        cost_estimate=pl.CostEstimate(
            flops=10**8, bytes_accessed=4 * 2**20, transcendentals=0
        ),
        name=name,
    )(*[item[0] for item in items])


def plain_exchange(items, plane):
    results = []
    for array, reach, over, selected in items:
        value = array
        if over:
            value = lax.all_gather(value, "tp")
        if reach == "plane":
            value = value if selected else value[None]
        else:
            value = lax.all_gather(value, "sp")
        results.append(value)
    return results


def gated_norm(mixed, gate, gain):
    length = mixed.shape[0]
    groups = mixed.shape[1]
    flat = mixed.reshape(length, groups, -1)
    gated = flat * jax.nn.silu(gate.astype(jnp.float32)).reshape(length, groups, -1)
    scaled = gated * lax.rsqrt(jnp.mean(gated * gated, axis=-1, keepdims=True) + eps)
    return (scaled * gain.reshape(groups, -1)[None]).reshape(length, -1).astype(jnp.bfloat16)


def attend(query, cosine, sine, keys, key_up, value_up_weight, length):
    heads = key_up.shape[1] // UNROTATED_WIDTH
    latent_width = key_up.shape[0]
    whole = UNROTATED_WIDTH + ROPE
    half = ROPE // 2
    step = 2 * length if keys.shape[0] % (2 * length) == 0 else length
    scale = whole ** (-0.5)
    contract = (((1,), (1,)), ((), ()))

    def kernel(q_ref, cos_ref, sin_ref, k_ref, ku_ref, vu_ref, out_ref, q_all, top, total, summed):
        start = lax.axis_index("sp") * length
        for h in range(heads):
            base = h * whole
            turn = q_ref[:, base + UNROTATED_WIDTH : base + whole].astype(jnp.float32)
            first, second = turn[:, :half], turn[:, half:]
            turned = jnp.concatenate(
                [
                    first * cos_ref[...] - second * sin_ref[...],
                    second * cos_ref[...] + first * sin_ref[...],
                ],
                axis=1,
            )
            q_all[h] = jnp.concatenate(
                [q_ref[:, base : base + UNROTATED_WIDTH], turned.astype(jnp.bfloat16)], axis=1
            )
        top[...] = jnp.full(top.shape, floor_score, jnp.float32)
        total[...] = jnp.zeros(total.shape, jnp.float32)
        summed[...] = jnp.zeros(summed.shape, jnp.float32)
        row = start + lax.broadcasted_iota(jnp.int32, (length, step), 0)
        column = lax.broadcasted_iota(jnp.int32, (length, step), 1)

        def visit(j, carry):
            at = pl.ds(pl.multiple_of(j * step, step), step)
            latent = k_ref[at, :latent_width]
            turned = k_ref[at, latent_width : latent_width + ROPE]
            seen = column + j * step <= row
            plain = jnp.dot(latent, ku_ref[...], preferred_element_type=jnp.float32).astype(
                jnp.bfloat16
            )
            all_values = jnp.dot(latent, vu_ref[...], preferred_element_type=jnp.float32).astype(
                jnp.bfloat16
            )
            for h in range(heads):
                values = all_values[:, h * VALUE_WIDTH : (h + 1) * VALUE_WIDTH]
                key = jnp.concatenate(
                    [plain[:, h * UNROTATED_WIDTH : (h + 1) * UNROTATED_WIDTH], turned], axis=1
                )
                scores = (
                    lax.dot_general(q_all[h], key, contract, preferred_element_type=jnp.float32)
                    * scale
                )
                scores = jnp.where(seen, scores, -jnp.inf)
                old = top[h][:, :1]
                new = jnp.maximum(old, jnp.max(scores, axis=1, keepdims=True))
                weights = jnp.exp(scores - new)
                shrink = jnp.exp(old - new)
                now = jnp.sum(weights, axis=1, keepdims=True)
                total[h] = total[h] * shrink + now
                summed[h] = summed[h] * shrink + jnp.dot(
                    weights.astype(jnp.bfloat16), values, preferred_element_type=jnp.float32
                )
                top[h] = jnp.broadcast_to(new, top.shape[1:])
            return carry

        lax.fori_loop(0, (start + length + step - 1) // step, visit, 0)
        for h in range(heads):
            out_ref[:, h * VALUE_WIDTH : (h + 1) * VALUE_WIDTH] = (
                summed[h] / total[h][:, :1]
            ).astype(jnp.bfloat16)

    return pl.pallas_call(
        kernel,
        out_shape=jax.ShapeDtypeStruct((length, heads * VALUE_WIDTH), jnp.bfloat16),
        in_specs=[pl.BlockSpec(memory_space=pltpu.VMEM)] * 6,
        out_specs=pl.BlockSpec(memory_space=pltpu.VMEM),
        scratch_shapes=[
            pltpu.VMEM((heads, length, whole), jnp.bfloat16),
            pltpu.VMEM((heads, length, 128), jnp.float32),
            pltpu.VMEM((heads, length, 128), jnp.float32),
            pltpu.VMEM((heads, length, VALUE_WIDTH), jnp.float32),
        ],
        compiler_params=pltpu.CompilerParams(vmem_limit_bytes=40 * 1024 * 1024),
        cost_estimate=pl.CostEstimate(
            flops=4 * 10**10, bytes_accessed=4 * 2**20, transcendentals=0
        ),
        name="attend",
    )(query, cosine, sine, keys, key_up, value_up_weight)


def fused(
    plane,
    tokens,
    mix_gain,
    query_proj,
    compressed_projection,
    compressed_norm_gain,
    rope_proj,
    key_up,
    value_up_weight,
    scan_input,
    scan_gate,
    scan_write,
    scan_read,
    step_proj,
    conv_input,
    conv_write,
    conv_read,
    decay_log,
    decay_offset,
    skip_gain,
    group_gain,
):
    devices, cores = lax.axis_size("sp"), lax.axis_size("tp")
    planes = devices // plane
    part, width = tokens.shape
    length = part * cores
    depth = scan_input.shape[0]
    kblock = depth * plane
    hw, ww = scan_input.shape[1] // plane, scan_write.shape[1] // plane
    lower, wide = hw + 2 * ww, 2 * hw + 2 * ww
    bounds = ((0, lower), (lower, wide))
    own_heads = decay_log.shape[0] // plane
    heads = key_up.shape[1] // UNROTATED_WIDTH
    latent_width = key_up.shape[0]
    key_width = latent_width + 128
    whole = UNROTATED_WIDTH + ROPE
    half = ROPE // 2
    scale = whole ** (-0.5)
    span = conv_input.shape[0]
    edge = 16
    bf16, f32 = jnp.bfloat16, jnp.float32
    MESH = pl.DeviceIdType.MESH
    last_contract = (((1,), (1,)), ((), ()))
    first_contract = (((0,), (0,)), ((), ()))
    best = lax.Precision.HIGHEST
    group_step = 2

    def mm(a, b):
        return jnp.dot(a, b, preferred_element_type=f32)

    def kernel(
        tok, mix, wq_hbm, comp, comp_gain, rope, ku, vu, w_in, w_gate, w_write, w_read, w_step,
        t_in, t_write, t_read, dlog, doff, skip, ggain, freqs,
        att_out, scan_out,
        wq, packed, wbuf, rows, edges, keys, q_all, top, total, summed,
        stepw, steps, osend, obuf, projf, cbuf, ybuf, runs, before, decayed, state, dsum,
        ssend, tsend, srecv, trecv, incoming, stage,
        wq_sem, wsend, wrecv, zsend, ksend_up, ksend_plane, ksend_core, krecv,
        rsend, rsend_core, rrecv, o_send, o_recv, e_send, e_recv,
        s_send, s_recv, t_send, t_recv, out_send, out_recv,
    ):
        here, core = lax.axis_index("sp"), lax.axis_index("tp")
        z, n = here // plane, here % plane
        other = cores - 1 - core

        def rcopy(src, dst, ss, rs, sp, c):
            return pltpu.make_async_remote_copy(
                src_ref=src, dst_ref=dst, send_sem=ss, recv_sem=rs,
                device_id=(sp, c), device_id_type=MESH,
            )

        def peer(step):
            return z * plane + (n + step) % plane

        barrier = pltpu.get_barrier_semaphore()
        greeted = 0
        for step in range(1, plane):
            pl.semaphore_signal(barrier, inc=1, device_id=(peer(step), core), device_id_type=MESH)
            greeted += 1
        for step in range(1, planes):
            pl.semaphore_signal(
                barrier, inc=1, device_id=((z + step) % planes * plane + n, core),
                device_id_type=MESH,
            )
            greeted += 1
        pl.semaphore_signal(barrier, inc=1, device_id=(here, other), device_id_type=MESH)
        greeted += 1
        wq_copy = pltpu.make_async_copy(wq_hbm, wq, wq_sem)
        wq_copy.start()

        for m in range(plane):
            packed[m, :, :hw] = w_in[:, m * hw : (m + 1) * hw]
            packed[m, :, hw : hw + ww] = w_write[:, m * ww : (m + 1) * ww]
            packed[m, :, hw + ww : lower] = w_read[:, m * ww : (m + 1) * ww]
            packed[m, :, lower:] = w_gate[:, m * hw : (m + 1) * hw]
        wbuf[here] = packed[n]
        padded = jnp.concatenate(
            [doff[...], jnp.zeros((length, 128 - doff.shape[1]), f32)], axis=1
        )
        turned_offsets = padded.T
        for m in range(plane):
            osend[m, :own_heads] = turned_offsets[m * own_heads : (m + 1) * own_heads]
        obuf[n] = osend[n]

        def normed_rows(values, gain, count):
            mean = jnp.sum(values * values, axis=-1, keepdims=True) / count
            return values * lax.rsqrt(mean + eps) * gain

        normed = normed_rows(tok[...].astype(f32), mix[...], width).astype(bf16)

        def rows_at(slot, c):
            return pl.ds(pl.multiple_of(slot * length + c * part, part), part)

        for p in range(planes):
            rows[p, rows_at(n, core), :] = normed[:, p * kblock : (p + 1) * kblock]

        def angles(start, count):
            position = (start + lax.broadcasted_iota(jnp.int32, (count, 1), 0)).astype(f32)
            angle = position * freqs[...]
            return jnp.cos(angle), jnp.sin(angle)

        def turn(first, second, cosine, sine):
            return [first * cosine - second * sine, second * cosine + first * sine]

        latent = normed_rows(mm(normed, comp[...]), comp_gain[...], latent_width)
        small = mm(normed, rope[...])
        cosine, sine = angles(here * length + core * part, part)
        own_key = jnp.concatenate(
            [latent]
            + turn(small[:, :half], small[:, half:], cosine, sine)
            + [jnp.zeros((part, key_width - latent_width - ROPE), f32)],
            axis=1,
        ).astype(bf16)
        keys[here * cores + core] = own_key

        pl.semaphore_wait(barrier, greeted)

        def key_slot(sp, c):
            return keys.at[sp * cores + c]

        def key_copy(sp, c, ss, to_sp, to_c):
            return rcopy(
                key_slot(sp, c), key_slot(sp, c), ss, krecv.at[sp * cores + c], to_sp, to_c
            )

        def key_arrived(sp, c):
            key_copy(sp, c, ksend_up.at[0], here, core).wait_recv()

        def key_up_copy(d):
            return key_copy(here, core, ksend_up.at[d], here + d * plane, core)

        def key_plane_copy(d, step):
            return key_copy(
                here - d * plane, core, ksend_plane.at[d * plane + step], peer(step), core
            )

        def key_core_copy(sp):
            return key_copy(sp, core, ksend_core.at[sp], here, other)

        def chunk(group, index):
            low, high = bounds[group]
            return wbuf.at[index, :, low:high]

        def w_arrived(group, index):
            rcopy(
                chunk(group, index), chunk(group, index), zsend.at[0, group, index],
                wrecv.at[group, index], here, core,
            ).wait_recv()

        def w_plane_copy(group, step):
            low, high = bounds[group]
            goal = (n + step) % plane
            return rcopy(
                packed.at[goal, :, low:high], chunk(group, here), wsend.at[group, step],
                wrecv.at[group, here], z * plane + goal, core,
            )

        def z_copy(group, index, up):
            return rcopy(
                chunk(group, index), chunk(group, index), zsend.at[up, group, index],
                wrecv.at[group, index], here + (plane if up else -plane), core,
            )

        def has_next(up):
            return z + 1 < planes if up else z > 0

        def own_weights(group, steps_of):
            for step in steps_of:
                index = z * plane + (n - step + plane) % plane
                if step:
                    w_arrived(group, index)
                for up in (0, 1):
                    @pl.when(has_next(up))
                    def _():
                        z_copy(group, index, up).start()

        def far_weights(group, d, forward):
            for up in (0, 1):
                source = z - d if up else z + d
                exists = (source >= 0) & (source < planes)
                gate = has_next(up) if forward else jnp.logical_not(has_next(up))

                @pl.when(exists & gate)
                def _():
                    for q in range(plane):
                        index = source * plane + q
                        w_arrived(group, index)
                        if forward:
                            z_copy(group, index, up).start()

        for d in range(1, planes):
            @pl.when(z + d < planes)
            def _():
                key_up_copy(d).start()
        for step in range(1, plane):
            w_plane_copy(0, step).start()
        own_weights(0, (0,))
        for step in range(1, plane):
            key_plane_copy(0, step).start()
        key_core_copy(here).start()

        def row_copy(slot, ss, to_sp, to_c):
            at = rows.at[:, rows_at(slot, core), :]
            return rcopy(at, at, ss, rrecv.at[slot * cores + core], to_sp, to_c)

        def row_plane_copy(step):
            return row_copy(n, rsend.at[step], peer(step), core)

        def row_core_copy(slot):
            return row_copy(slot, rsend_core.at[slot], here, other)

        def row_arrived(slot, c):
            at = rows.at[:, rows_at(slot, c), :]
            rcopy(at, at, rsend.at[0], rrecv.at[slot * cores + c], here, core).wait_recv()

        def offset_copy(step):
            goal = (n + step) % plane
            return rcopy(
                osend.at[goal], obuf.at[n], o_send.at[step], o_recv.at[n],
                z * plane + goal, core,
            )

        row_core_copy(n).start()
        for step in range(1, plane):
            offset_copy(step).start()

        wq_copy.wait()
        row_arrived(n, other)
        own_rows = pl.ds(pl.multiple_of(n * length, length), length)
        query = mm(rows[0, own_rows, :], wq[:kblock, :])
        for p in range(1, planes):
            query += mm(rows[p, own_rows, :], wq[p * kblock : (p + 1) * kblock, :])
        query = query.astype(bf16)
        cosine, sine = angles(here * length, length)
        for h in range(heads):
            base = h * whole
            rope_part = query[:, base + UNROTATED_WIDTH : base + whole].astype(f32)
            q_all[h] = jnp.concatenate(
                [query[:, base : base + UNROTATED_WIDTH]]
                + [
                    v.astype(bf16)
                    for v in turn(rope_part[:, :half], rope_part[:, half:], cosine, sine)
                ],
                axis=1,
            )
        top[...] = jnp.full(top.shape, floor_score, f32)
        total[...] = jnp.zeros(total.shape, f32)
        summed[...] = jnp.zeros(summed.shape, f32)

        own_weights(0, range(1, plane))
        for d in range(1, planes):
            @pl.when(z >= d)
            def _():
                key_arrived(here - d * plane, core)
                for step in range(1, plane):
                    key_plane_copy(d, step).start()
                key_core_copy(here - d * plane).start()
        for step in range(1, plane):
            w_plane_copy(1, step).start()
        for step in range(1, plane):
            row_plane_copy(step).start()

        def pass_keys(d):
            for step in range(1, plane):
                sp = (z - d) * plane + (n + step) % plane
                key_arrived(sp, core)
                key_core_copy(sp).start()

        def other_keys(d):
            for q in range(plane):
                key_arrived((z - d) * plane + q, other)

        size = group_step * length
        row = lax.broadcasted_iota(jnp.int32, (length, size), 0)
        column = lax.broadcasted_iota(jnp.int32, (length, size), 1)

        def visit(first_block, limit):
            count = group_step * cores
            block = keys[pl.ds(first_block * cores, count)].reshape(size, key_width)
            lat = block[:, :latent_width]
            turned = block[:, latent_width : latent_width + ROPE]
            plain = mm(lat, ku[...]).astype(bf16)
            all_values = mm(lat, vu[...]).astype(bf16)
            if limit is not None:
                seen = column <= row + limit
            for h in range(heads):
                values = all_values[:, h * VALUE_WIDTH : (h + 1) * VALUE_WIDTH]
                key = jnp.concatenate(
                    [plain[:, h * UNROTATED_WIDTH : (h + 1) * UNROTATED_WIDTH], turned], axis=1
                )
                scores = (
                    lax.dot_general(q_all[h], key, last_contract, preferred_element_type=f32)
                    * scale
                )
                if limit is not None:
                    scores = jnp.where(seen, scores, -jnp.inf)
                old = top[h][:, :1]
                new = jnp.maximum(old, jnp.max(scores, axis=1, keepdims=True))
                weights = jnp.exp(scores - new)
                shrink = jnp.exp(old - new)
                now = jnp.sum(weights, axis=1, keepdims=True)
                total[h] = total[h] * shrink + now
                summed[h] = summed[h] * shrink + mm(weights.astype(bf16), values)
                top[h] = jnp.broadcast_to(new, top.shape[1:])

        pass_keys(0)
        other_keys(0)

        def near(j, carry):
            visit(z * plane + j * group_step, (n - j * group_step) * length)
            return carry

        lax.fori_loop(0, n // group_step + 1, near, 0)

        def further(d, carry):
            far_weights(0, d, True)

            @pl.when(d == 1)
            def _():
                own_weights(1, range(plane))

            @pl.when(z >= d)
            def _():
                pass_keys(d)
                other_keys(d)

                def inner(j, carry):
                    visit((z - d) * plane + j * group_step, None)
                    return carry

                lax.fori_loop(0, plane // group_step, inner, 0)

            return carry

        lax.fori_loop(1, planes, further, 0)
        for h in range(heads):
            att_out[:, h * VALUE_WIDTH : (h + 1) * VALUE_WIDTH] = (
                summed[h] / total[h][:, :1]
            ).astype(bf16)

        for step in range(1, plane):
            slot = (n + step) % plane
            row_arrived(slot, core)
            row_core_copy(slot).start()
        for step in range(1, plane):
            row_arrived((n + step) % plane, other)
        tail_at = plane * length - edge

        def edge_copy():
            return rcopy(
                rows.at[:, tail_at : tail_at + edge, :], edges, e_send, e_recv,
                here + plane, core,
            )

        @pl.when(z + 1 < planes)
        def _():
            edge_copy().start()

        lane = lax.broadcasted_iota(jnp.int32, (w_step.shape[1], 128), 1)
        which = lax.broadcasted_iota(jnp.int32, (w_step.shape[1], 128), 0)
        first_head = (core * plane + n) * own_heads
        chosen = ((which == lane + first_head) & (lane < own_heads)).astype(bf16)
        stepw[...] = mm(w_step[...], chosen).astype(bf16)

        def tile(k):
            return pl.ds(pl.multiple_of(k * length, length), length)

        def step_tile(k, carry):
            raw = mm(rows[0, tile(k), :], stepw[:kblock, :])
            for p in range(1, planes):
                raw += mm(rows[p, tile(k), :], stepw[p * kblock : (p + 1) * kblock, :])
            steps[k] = jnp.maximum(raw, 0.0) + jnp.log1p(jnp.exp(-jnp.abs(raw)))
            return carry

        lax.fori_loop(0, plane, step_tile, 0)
        for d in range(1, planes):
            far_weights(1, d, True)
        for d in range(1, planes):
            far_weights(0, d, False)

        def project(p, values, group):
            low, high = bounds[group]
            block = wbuf[p * plane : (p + 1) * plane, :, low:high]
            return mm(values, block.reshape(kblock, high - low))

        @pl.when(z > 0)
        def _():
            rcopy(edges, edges, e_send, e_recv, here, core).wait_recv()
            first = project(0, edges[0], 0)
            for p in range(1, planes):
                first += project(p, edges[p], 0)
            projf[:edge, :] = first.astype(bf16).astype(f32)

        @pl.when(z == 0)
        def _():
            projf[:edge, :] = jnp.zeros((edge, lower), f32)

        def project_tile(k, carry):
            out = project(0, rows[0, tile(k), :], 0)
            for p in range(1, planes):
                out += project(p, rows[p, tile(k), :], 0)
            at = pl.ds(pl.multiple_of(k * length + edge, edge), length)
            projf[at, :] = out.astype(bf16).astype(f32)
            return carry

        lax.fori_loop(0, plane, project_tile, 0)

        taps = jnp.concatenate(
            [
                t_in[:, pl.ds(pl.multiple_of(n * hw, hw), hw)],
                t_write[:, pl.ds(pl.multiple_of(n * ww, ww), ww)],
                t_read[:, pl.ds(pl.multiple_of(n * ww, ww), ww)],
            ],
            axis=1,
        ).astype(f32)

        def conv_tile(k, carry):
            base = pl.ds(pl.multiple_of(k * length, length), length + edge)
            for low in range(0, lower, 128):
                at = slice(low, low + 128)
                values = projf[base, at]
                result = jnp.zeros((length, 128), f32)
                for i in range(span):
                    shift = edge - span + 1 + i
                    result = result + taps[i : i + 1, at] * values[shift : shift + length]
                cbuf[tile(k), at] = (result * jax.nn.sigmoid(result)).astype(bf16)
            return carry

        lax.fori_loop(0, plane, conv_tile, 0)

        for step in range(1, plane):
            slot = (n - step + plane) % plane
            rcopy(
                obuf.at[slot], obuf.at[slot], o_send.at[0], o_recv.at[slot], here, core
            ).wait_recv()
        lane_row = lax.broadcasted_iota(jnp.int32, (1, 128), 1)
        rate = jnp.zeros((1, 128), f32)
        for h in range(own_heads):
            rate = jnp.where(lane_row == h, dlog[n * own_heads + h], rate)
        rate = -jnp.exp(rate)
        causal = lax.broadcasted_iota(jnp.int32, (length, length), 0) >= lax.broadcasted_iota(
            jnp.int32, (length, length), 1
        )
        tri = causal.astype(f32)

        def per_lane(columns):
            return jnp.concatenate(
                [
                    jnp.broadcast_to(columns[:, h : h + 1], (columns.shape[0], SSM_DIM))
                    for h in range(own_heads)
                ],
                axis=1,
            )

        def per_row(values):
            return jnp.concatenate(
                [
                    jnp.broadcast_to(values[:, h : h + 1], (SSM_DIM, SSM_STATE))
                    for h in range(own_heads)
                ],
                axis=0,
            )

        state[...] = jnp.zeros(state.shape, f32)
        dsum[...] = jnp.zeros(dsum.shape, f32)

        def scan_tile(k, carry):
            step_col = steps[k]
            off_col = jnp.concatenate(
                [obuf[k], jnp.zeros((128 - obuf.shape[1], length), f32)], axis=0
            ).T
            decay = jnp.where(lane_row < own_heads, rate * step_col + off_col, 0.0)
            running = jnp.dot(tri, decay, precision=best, preferred_element_type=f32)
            runs[k] = running
            run_row, step_row = running.T, step_col.T
            x = cbuf[tile(k), :hw]
            w = cbuf[tile(k), hw : hw + ww]
            r = cbuf[tile(k), hw + ww : lower]
            inner = lax.dot_general(r, w, last_contract, preferred_element_type=f32)
            for h in range(own_heads):
                at = slice(h * SSM_DIM, (h + 1) * SSM_DIM)
                spread = jnp.where(
                    causal, running[:, h : h + 1] - run_row[h : h + 1, :], -jnp.inf
                )
                mixing = inner * jnp.exp(spread) * step_row[h : h + 1, :]
                ybuf[tile(k), at] = (
                    mm(mixing.astype(bf16), x[:, at])
                    + skip[n * own_heads + h] * x[:, at].astype(f32)
                )
            last = running[length - 1 : length, :]
            to_end = jnp.exp(last - running) * step_col
            weighted = (x.astype(f32) * per_lane(to_end)).astype(bf16)
            update = lax.dot_general(weighted, w, first_contract, preferred_element_type=f32)
            before[k] = state[...]
            decayed[k] = dsum[...]
            state[...] = per_row(jnp.exp(last)) * state[...] + update
            dsum[...] = dsum[...] + last
            return carry

        lax.fori_loop(0, plane, scan_tile, 0)

        ssend[...] = state[...].astype(bf16)
        tsend[...] = dsum[...]

        def state_copies(d):
            to = here + d * plane
            return (
                rcopy(ssend, srecv.at[z], s_send.at[d], s_recv.at[z], to, core),
                rcopy(tsend, trecv.at[z], t_send.at[d], t_recv.at[z], to, core),
            )

        for d in range(1, planes):
            @pl.when(z + d < planes)
            def _():
                for copy in state_copies(d):
                    copy.start()

        for d in range(1, planes):
            far_weights(1, d, False)
        incoming[...] = jnp.zeros(incoming.shape, f32)
        for p in range(planes - 1):
            @pl.when(p < z)
            def _():
                rcopy(
                    ssend, srecv.at[p], s_send.at[0], s_recv.at[p], here, core
                ).wait_recv()
                rcopy(
                    tsend, trecv.at[p], t_send.at[0], t_recv.at[p], here, core
                ).wait_recv()
                incoming[...] = per_row(jnp.exp(trecv[p][:1])) * incoming[...] + srecv[
                    p
                ].astype(f32)

        own_columns = pl.ds(pl.multiple_of(n * hw, hw), hw)
        gain = ggain[:, own_columns]

        def out_copy(k):
            return rcopy(
                stage.at[k], scan_out.at[:, own_columns], out_send.at[k], out_recv.at[n],
                z * plane + k, core,
            )

        def finish(i, carry):
            k = (n + 1 + i) % plane
            gate = project(0, rows[0, tile(k), :], 1)
            for p in range(1, planes):
                gate += project(p, rows[p, tile(k), :], 1)
            gate = gate.astype(bf16).astype(f32)
            entered = (
                before[k] + per_row(jnp.exp(decayed[k][:1])) * incoming[...]
            ).astype(bf16)
            carried = lax.dot_general(
                cbuf[tile(k), hw + ww : lower], entered, last_contract,
                preferred_element_type=f32,
            )
            mixed = ybuf[tile(k), :] + carried * per_lane(jnp.exp(runs[k]))
            gated = mixed * (gate * jax.nn.sigmoid(gate))
            out = normed_rows(gated, gain, hw).astype(bf16)
            stage[k] = out

            @pl.when(k != n)
            def _():
                out_copy(k).start()

            @pl.when(k == n)
            def _():
                scan_out[:, own_columns] = out

            return carry

        lax.fori_loop(0, plane, finish, 0)
        for step in range(1, plane):
            slot = (n + step) % plane
            at = scan_out.at[:, pl.ds(pl.multiple_of(slot * hw, hw), hw)]
            rcopy(stage.at[0], at, out_send.at[0], out_recv.at[slot], here, core).wait_recv()

        for d in range(1, planes):
            @pl.when(z + d < planes)
            def _():
                key_up_copy(d).wait_send()
                for copy in state_copies(d):
                    copy.wait_send()
        for d in range(planes):
            @pl.when(z >= d)
            def _():
                for step in range(1, plane):
                    key_plane_copy(d, step).wait_send()
                for q in range(plane):
                    key_core_copy((z - d) * plane + q).wait_send()
        for step in range(1, plane):
            for group in (0, 1):
                w_plane_copy(group, step).wait_send()
            row_plane_copy(step).wait_send()
            offset_copy(step).wait_send()
            out_copy((n + step) % plane).wait_send()
        for slot in range(plane):
            row_core_copy(slot).wait_send()

        @pl.when(z + 1 < planes)
        def _():
            edge_copy().wait_send()

        for up in (0, 1):
            for p in range(planes):
                @pl.when(((p <= z) if up else (p >= z)) & has_next(up))
                def _():
                    for q in range(plane):
                        for group in (0, 1):
                            z_copy(group, p * plane + q, up).wait_send()

    vmem = pl.BlockSpec(memory_space=pltpu.VMEM)
    smem = pl.BlockSpec(memory_space=pltpu.SMEM)
    hbm = pl.BlockSpec(memory_space=pltpu.HBM)
    freqs = theta ** (-jnp.arange(half, dtype=f32) * 2.0 / ROPE)
    dma = pltpu.SemaphoreType.DMA
    positions = plane * length
    return pl.pallas_call(
        kernel,
        out_shape=(
            jax.ShapeDtypeStruct((length, heads * VALUE_WIDTH), bf16),
            jax.ShapeDtypeStruct((length, scan_input.shape[1]), bf16),
        ),
        in_specs=[vmem, vmem, hbm] + [vmem] * 13 + [smem, vmem, smem, vmem, vmem],
        out_specs=(vmem, vmem),
        scratch_shapes=[
            pltpu.VMEM(query_proj.shape, bf16),
            pltpu.VMEM((plane, depth, wide), bf16),
            pltpu.VMEM((devices, depth, wide), bf16),
            pltpu.VMEM((planes, positions, kblock), bf16),
            pltpu.VMEM((planes, edge, kblock), bf16),
            pltpu.VMEM((devices * cores, part, key_width), bf16),
            pltpu.VMEM((heads, length, whole), bf16),
            pltpu.VMEM((heads, length, 128), f32),
            pltpu.VMEM((heads, length, 128), f32),
            pltpu.VMEM((heads, length, VALUE_WIDTH), f32),
            pltpu.VMEM((width, 128), bf16),
            pltpu.VMEM((plane, length, 128), f32),
            pltpu.VMEM((plane, 8, length), f32),
            pltpu.VMEM((plane, 8, length), f32),
            pltpu.VMEM((edge + positions, lower), f32),
            pltpu.VMEM((positions, lower), bf16),
            pltpu.VMEM((positions, hw), f32),
            pltpu.VMEM((plane, length, 128), f32),
            pltpu.VMEM((plane, own_heads * SSM_DIM, SSM_STATE), f32),
            pltpu.VMEM((plane, 8, 128), f32),
            pltpu.VMEM((own_heads * SSM_DIM, SSM_STATE), f32),
            pltpu.VMEM((8, 128), f32),
            pltpu.VMEM((own_heads * SSM_DIM, SSM_STATE), bf16),
            pltpu.VMEM((8, 128), f32),
            pltpu.VMEM((planes, own_heads * SSM_DIM, SSM_STATE), bf16),
            pltpu.VMEM((planes, 8, 128), f32),
            pltpu.VMEM((own_heads * SSM_DIM, SSM_STATE), f32),
            pltpu.VMEM((plane, length, hw), bf16),
            dma,
            dma((2, plane)),
            dma((2, devices)),
            dma((2, 2, devices)),
            dma((planes,)),
            dma((planes * plane,)),
            dma((devices,)),
            dma((devices * cores,)),
            dma((plane,)),
            dma((plane,)),
            dma((plane * cores,)),
            dma((plane,)),
            dma((plane,)),
            dma,
            dma,
            dma((planes,)),
            dma((planes,)),
            dma((planes,)),
            dma((planes,)),
            dma((plane,)),
            dma((plane,)),
        ],
        compiler_params=pltpu.CompilerParams(
            collective_id=1, has_side_effects=True, vmem_limit_bytes=60 * 1024 * 1024
        ),
        name="fused",
    )(
        tokens,
        mix_gain[None, :],
        query_proj,
        compressed_projection,
        compressed_norm_gain[None, :],
        rope_proj,
        key_up,
        value_up_weight,
        scan_input,
        scan_gate,
        scan_write,
        scan_read,
        step_proj,
        conv_input,
        conv_write,
        conv_read,
        decay_log,
        decay_offset,
        skip_gain,
        group_gain[None, :],
        freqs[None, :],
    )


def shards(
    tokens,
    mix_gain,
    query_proj,
    compressed_projection,
    compressed_norm_gain,
    rope_proj,
    key_up,
    value_up_weight,
    scan_input,
    scan_gate,
    scan_write,
    scan_read,
    step_proj,
    conv_input,
    conv_write,
    conv_read,
    decay_log,
    decay_offset,
    skip_gain,
    group_gain,
):
    groups = scan_write.shape[1] // SSM_STATE
    devices, cores = lax.axis_size("sp"), lax.axis_size("tp")
    plane = groups if devices % groups == 0 else 1
    planes = devices // plane
    sp_index, core = lax.axis_index("sp"), lax.axis_index("tp")
    across, within = sp_index // plane, sp_index % plane
    own_groups = groups // plane
    direct = plane > 1
    if direct and cores == 2 and own_groups == 1 and plane % 2 == 0 and planes > 1:
        return fused(
            plane,
            tokens,
            mix_gain,
            query_proj,
            compressed_projection,
            compressed_norm_gain,
            rope_proj,
            key_up,
            value_up_weight,
            scan_input,
            scan_gate,
            scan_write,
            scan_read,
            step_proj,
            conv_input,
            conv_write,
            conv_read,
            decay_log,
            decay_offset,
            skip_gain,
            group_gain,
        )

    def move(items, name, number, columns=False):
        if direct:
            return exchange(items, plane, name, number, columns)
        return plain_exchange(items, plane)

    depth = scan_input.shape[0]
    widths = [w.shape[1] // plane for w in (scan_input, scan_gate, scan_write, scan_read)]
    offsets = [sum(widths[:i]) for i in range(4)]
    packed = jnp.stack(
        [
            jnp.concatenate(
                [
                    w[:, n * size : (n + 1) * size]
                    for w, size in zip((scan_input, scan_gate, scan_write, scan_read), widths)
                ],
                axis=1,
            )
            for n in range(plane)
        ]
    )
    (part_weights,) = move([(packed, "plane", False, True)], "weights_in_plane", 1)
    weights = lax.all_gather(
        part_weights.reshape(plane * depth, -1),
        "sp",
        axis=0,
        tiled=True,
        axis_index_groups=[[p * plane + n for p in range(planes)] for n in range(plane)],
    )

    own_normed = rms_scale(tokens, mix_gain).astype(jnp.bfloat16)
    part = tokens.shape[0]
    length = part * cores
    latent_width = compressed_projection.shape[1]
    small = jnp.dot(
        own_normed,
        jnp.concatenate([compressed_projection, rope_proj], axis=1),
        preferred_element_type=jnp.float32,
    )
    latent = rms_scale(small[:, :latent_width], compressed_norm_gain).astype(jnp.bfloat16)
    part_positions = sp_index * length + core * part + jnp.arange(part, dtype=jnp.int32)
    key_turned = rotate(small[:, latent_width:], part_positions).astype(jnp.bfloat16)
    padding = jnp.zeros((part, -(latent_width + ROPE) % 128), jnp.bfloat16)
    own_keys = jnp.concatenate([latent, key_turned, padding], axis=1)
    all_keys, all_rows, offsets_seen = move(
        [
            (own_keys, "all", True, False),
            (own_normed, "plane", True, False),
            (decay_offset.T, "plane", False, False),
        ],
        "rows_and_keys",
        2,
    )
    all_keys = all_keys.reshape(devices * length, -1)
    all_rows = all_rows.reshape(plane * length, -1)
    edge_rows = from_behind(all_rows[plane * length - 8 :], "sp", plane)
    positions = sp_index * length + jnp.arange(length, dtype=jnp.int32)
    rows = lax.dynamic_slice_in_dim(all_rows, within * length, length, 0)
    query = jnp.dot(rows, query_proj, preferred_element_type=jnp.float32).astype(jnp.bfloat16)
    half = ROPE // 2
    freqs = theta ** (-jnp.arange(half, dtype=jnp.float32) * 2.0 / ROPE)
    angle = positions.astype(jnp.float32)[:, None] * freqs[None, :]
    attended = attend(
        query, jnp.cos(angle), jnp.sin(angle), all_keys, key_up, value_up_weight, length
    )

    def own_part(array, axis, size):
        return lax.dynamic_slice_in_dim(array, within * size, size, axis)

    local_heads = decay_log.shape[0]
    own_heads = local_heads // plane
    per_group = local_heads // groups
    step_raw = jnp.dot(
        all_rows,
        lax.dynamic_slice_in_dim(
            step_proj, core * local_heads + within * own_heads, own_heads, 1
        ),
        preferred_element_type=jnp.float32,
    )
    step_size = jax.nn.softplus(step_raw)
    own_offset = own_part(offsets_seen, 1, own_heads)
    step_values = jnp.transpose(step_size.reshape(plane, length, own_heads), (0, 2, 1))
    decay_values = (
        -jnp.exp(own_part(decay_log, 0, own_heads))[None, :, None] * step_values + own_offset
    )

    projected = jnp.dot(all_rows, weights, preferred_element_type=jnp.float32).astype(jnp.bfloat16)
    edge = jnp.dot(edge_rows, weights, preferred_element_type=jnp.float32).astype(jnp.bfloat16)
    span = conv_input.shape[0] - 1

    def convolved(i, taps):
        at = slice(offsets[i], offsets[i] + widths[i])
        return short_conv(projected[:, at], edge[8 - span :, at], own_part(taps, 1, widths[i]))

    head_conv = convolved(0, conv_input)
    gate = projected[:, offsets[1] : offsets[1] + widths[1]]
    writes = convolved(2, conv_write)
    reads = convolved(3, conv_read)
    blocks = plane * own_groups

    def by_block(values, last):
        split = values.reshape(plane, length, own_groups, last)
        return jnp.transpose(split, (0, 2, 1, 3)).reshape(blocks, length, last)

    head_values = jnp.transpose(
        head_conv.reshape(plane, length, own_groups, per_group, SSM_DIM), (0, 2, 3, 1, 4)
    ).reshape(blocks, per_group, length, SSM_DIM)
    write_values = by_block(writes, SSM_STATE)
    read_values = by_block(reads, SSM_STATE)
    running, state, mixed = local_scan(
        head_values,
        step_values.reshape(blocks, per_group, length),
        decay_values.reshape(blocks, per_group, length),
        write_values,
        read_values,
    )
    states = state.reshape(plane, own_heads, SSM_DIM, SSM_STATE)
    totals = running[..., -1].reshape(plane, own_heads)
    before, decayed = [jnp.zeros_like(states[0])], [jnp.zeros_like(totals[0])]
    for index in range(plane):
        before.append(jnp.exp(totals[index])[:, None, None] * before[-1] + states[index])
        decayed.append(totals[index] + decayed[-1])
    sent_total = jnp.pad(decayed[-1][None, :], ((0, 7), (0, 128 - own_heads)))
    seen_states, seen_totals = move(
        [
            (before[-1].reshape(-1, SSM_STATE).astype(jnp.bfloat16), "line", False, False),
            (sent_total, "line", False, False),
        ],
        "states",
        3,
    )
    seen_states = seen_states.reshape(planes, own_heads, SSM_DIM, SSM_STATE).astype(jnp.float32)
    seen_totals = seen_totals[:, 0, :own_heads]
    index = jnp.arange(planes)
    between = (index[None, :] > index[:, None]) & (index[None, :] < across)
    path = jnp.sum(jnp.where(between[:, :, None], seen_totals[None], 0.0), axis=1)
    reached = (index < across)[:, None]
    factor = jnp.where(reached, jnp.exp(path), 0.0)
    incoming = jnp.sum(seen_states * factor[:, :, None, None], axis=0)
    entered = jnp.stack(
        [
            before[k] + jnp.exp(decayed[k])[:, None, None] * incoming
            for k in range(plane)
        ]
    ).reshape(blocks, per_group, SSM_DIM, SSM_STATE)
    carried = jnp.einsum(
        "gln,grpn->grlp",
        read_values,
        entered.astype(jnp.bfloat16),
        preferred_element_type=jnp.float32,
    )
    skip = jnp.broadcast_to(
        own_part(skip_gain, 0, own_heads).reshape(1, own_groups, per_group),
        (plane, own_groups, per_group),
    ).reshape(blocks, per_group, 1, 1)
    mixed = (
        mixed
        + carried * jnp.exp(running)[..., None]
        + skip * head_values.astype(jnp.float32)
    )
    mixed = jnp.transpose(
        mixed.reshape(plane, own_groups, per_group, length, SSM_DIM), (0, 3, 1, 2, 4)
    ).reshape(plane * length, own_groups, per_group, SSM_DIM)
    scanned = gated_norm(mixed, gate, own_part(group_gain, 0, widths[0]))
    (columns,) = move(
        [(scanned.reshape(plane, length, -1), "plane", False, True)], "outputs_in_plane", 4, True
    )
    scanned = columns.reshape(length, -1)
    return (attended, scanned)


def solution(mesh):
    in_specs = (
        P(("sp", "tp"), None),
        P(),
        P(None, "tp"),
        P(),
        P(),
        P(),
        P(None, "tp"),
        P(None, "tp"),
        P("sp", "tp"),
        P("sp", "tp"),
        P("sp", "tp"),
        P("sp", "tp"),
        P(),
        P(None, "tp"),
        P(None, "tp"),
        P(None, "tp"),
        P("tp"),
        P("sp", "tp"),
        P("tp"),
        P("tp"),
    )
    out_specs = (P("sp", "tp"), P("sp", "tp"))
    return jax.shard_map(shards, mesh=mesh, in_specs=in_specs, out_specs=out_specs, check_vma=False)
```

```python
import jax
import jax.numpy as jnp
import numpy as np
from jax import lax
from jax.experimental import pallas as pl
from jax.experimental.pallas import tpu as pltpu
from jax.sharding import PartitionSpec as P

UNROTATED_WIDTH = 128
ROPE = 64
VALUE_WIDTH = 128
SSM_DIM = 64
SSM_STATE = 128


eps = 1e-06
theta = 10000.0
floor_score = -1e30


def from_behind(value, axis, steps):
    count = lax.axis_size(axis)
    initial, last = (max(0, -steps), min(count, count - steps))
    return lax.ppermute(value, axis, [(source, source + steps) for source in range(initial, last)])


def rms_scale(values, gain):
    wide = values.astype(jnp.float32)
    return wide * lax.rsqrt(jnp.mean(wide * wide, axis=-1, keepdims=True) + eps) * gain


def rotate(values, positions):
    half = values.shape[-1] // 2
    freqs = theta ** (-jnp.arange(half, dtype=jnp.float32) * 2.0 / values.shape[-1])
    angle = positions.astype(jnp.float32)[:, None] * freqs[None, :]
    cosine = jnp.cos(angle)
    sine = jnp.sin(angle)
    if values.ndim == 3:
        cosine = cosine[:, None, :]
        sine = sine[:, None, :]
    first = values[..., :half]
    second = values[..., half:]
    return jnp.concatenate(
        [first * cosine - second * sine, second * cosine + first * sine], axis=-1
    )


def short_conv(values, edge, taps):
    span = taps.shape[0]
    length = values.shape[0]
    padded = jnp.concatenate([edge, values], axis=0).astype(jnp.float32)
    result = jnp.zeros(values.shape, jnp.float32)
    for index in range(span):
        result = result + taps[index].astype(jnp.float32)[None, :] * padded[index : index + length]
    return jax.nn.silu(result).astype(jnp.bfloat16)


def local_scan(heads, steps, decays, writes, reads):
    length = decays.shape[-1]
    running = jnp.einsum(
        "grs,ls->grl",
        decays,
        jnp.tril(jnp.ones((length, length), jnp.float32)),
        precision=lax.Precision.HIGHEST,
    )
    causal = jnp.tril(jnp.ones((length, length), dtype=bool))
    spread = jnp.where(causal, running[..., :, None] - running[..., None, :], -jnp.inf)
    inner = jnp.einsum("gln,gsn->gls", reads, writes, preferred_element_type=jnp.float32)
    mixing = inner[:, None] * jnp.exp(spread) * steps[:, :, None, :]
    within = jnp.einsum(
        "grls,grsp->grlp",
        mixing.astype(jnp.bfloat16),
        heads,
        preferred_element_type=jnp.float32,
    )
    to_end = jnp.exp(running[..., -1:] - running) * steps
    weighted = (heads.astype(jnp.float32) * to_end[..., None]).astype(jnp.bfloat16)
    state = jnp.einsum(
        "grsp,gsn->grpn", weighted, writes, preferred_element_type=jnp.float32
    )
    return running, state, within


def exchange(items, plane, name, number, columns=False):
    devices, cores = lax.axis_size("sp"), lax.axis_size("tp")
    planes = devices // plane
    counts = [{"plane": plane, "line": planes, "all": devices}[item[1]] for item in items]
    amount = len(items)
    starts = [sum(counts[:i]) for i in range(amount)]
    shared = any(item[2] for item in items)

    def kernel(*refs):
        ins, outs = refs[:amount], refs[amount : 2 * amount]
        send, recv, pass_send, pass_recv, own = refs[2 * amount :]
        here, core = lax.axis_index("sp"), lax.axis_index("tp")
        across, within = here // plane, here % plane

        def place(reach, step):
            if reach == "plane":
                slot = (within + step + plane) % plane
                return across * plane + slot, slot
            if reach == "line":
                slot = (across + step + planes) % planes
                return slot * plane + within, slot
            up, along = step // plane, step % plane
            if step < 0:
                up, along = -((-step) // plane), -((-step) % plane)
            slot = (across + up + planes) % planes * plane + (within + along + plane) % plane
            return slot, slot

        barrier = pltpu.get_barrier_semaphore()
        greeted = 0
        for reach in ("plane", "line"):
            if not any(item[1] in (reach, "all") for item in items):
                continue
            size = {"plane": plane, "line": planes}[reach]
            for step in range(1, size):
                pl.semaphore_signal(
                    barrier,
                    inc=1,
                    device_id=(place(reach, step)[0], core),
                    device_id_type=pl.DeviceIdType.MESH,
                )
                greeted += 1
        if shared:
            for turn in range(1, cores):
                pl.semaphore_signal(
                    barrier,
                    inc=1,
                    device_id=(here, (core + turn) % cores),
                    device_id_type=pl.DeviceIdType.MESH,
                )
                greeted += 1
        pl.semaphore_wait(barrier, greeted)

        def target(i, slot, who):
            if columns:
                size = ins[i].shape[-1]
                return outs[i].at[:, pl.ds(pl.multiple_of(slot * size, size), size)]
            return outs[i].at[slot, who] if items[i][2] else outs[i].at[slot]

        def sent(i, step):
            goal, goal_slot = place(items[i][1], step)
            mine = place(items[i][1], 0)[1]
            if items[i][1] == "all" and step % plane and step >= plane:
                from_line = place("all", -(step // plane * plane))[1]
                return pltpu.make_async_remote_copy(
                    src_ref=target(i, from_line, core),
                    dst_ref=target(i, from_line, core),
                    send_sem=send.at[starts[i] + step],
                    recv_sem=recv.at[starts[i] + step],
                    device_id=(place("plane", step % plane)[0], core),
                    device_id_type=pl.DeviceIdType.MESH,
                )
            return pltpu.make_async_remote_copy(
                src_ref=ins[i].at[goal_slot] if items[i][3] else ins[i],
                dst_ref=target(i, mine, core),
                send_sem=send.at[starts[i] + step],
                recv_sem=recv.at[starts[i] + step],
                device_id=(goal, core),
                device_id_type=pl.DeviceIdType.MESH,
            )

        def arrived(i, step):
            slot = place(items[i][1], -step)[1]
            return pltpu.make_async_remote_copy(
                src_ref=ins[i].at[slot] if items[i][3] else ins[i],
                dst_ref=target(i, slot, core),
                send_sem=send.at[starts[i] + step],
                recv_sem=recv.at[starts[i] + step],
                device_id=(here, core),
                device_id_type=pl.DeviceIdType.MESH,
            )

        def passed(i, step, turn, outgoing):
            slot = place(items[i][1], -step)[1]
            other = (core + turn) % cores
            owner = core if outgoing else (core - turn + cores) % cores
            return pltpu.make_async_remote_copy(
                src_ref=ins[i] if step == 0 else target(i, slot, core),
                dst_ref=target(i, slot, owner),
                send_sem=pass_send.at[(starts[i] + step) * cores + turn],
                recv_sem=pass_recv.at[(starts[i] + step) * cores + turn],
                device_id=(here, other),
                device_id_type=pl.DeviceIdType.MESH,
            )

        kept = []
        for i in range(amount):
            if items[i][1] == "all":
                for up in range(1, planes):
                    sent(i, up * plane).start()
                for step in range(1, plane):
                    sent(i, step).start()
        for i in range(amount):
            if items[i][1] != "all":
                for step in range(1, counts[i]):
                    sent(i, step).start()
        for i in range(amount):
            slot = place(items[i][1], 0)[1]
            local = pltpu.make_async_copy(
                ins[i].at[slot] if items[i][3] else ins[i], target(i, slot, core), own.at[i]
            )
            local.start()
            kept.append(local)
            if items[i][2]:
                for turn in range(1, cores):
                    passed(i, 0, turn, True).start()
        for i in range(amount):
            if items[i][1] == "all":
                for up in range(1, planes):
                    arrived(i, up * plane).wait_recv()
                    for step in range(up * plane + 1, (up + 1) * plane):
                        sent(i, step).start()
                    for turn in range(1, cores):
                        passed(i, up * plane, turn, True).start()
        for i in range(amount):
            for step in range(1, counts[i]):
                if items[i][1] == "all" and step % plane == 0:
                    continue
                arrived(i, step).wait_recv()
                if items[i][2]:
                    for turn in range(1, cores):
                        passed(i, step, turn, True).start()
        for i in range(amount):
            kept[i].wait()
            for step in range(counts[i]):
                if step > 0:
                    sent(i, step).wait_send()
                if items[i][2]:
                    for turn in range(1, cores):
                        passed(i, step, turn, True).wait_send()
                        passed(i, step, turn, False).wait_recv()

    shapes = []
    for (array, reach, over, selected), count in zip(items, counts):
        lead = (count, cores) if over else (count,)
        tail = array.shape[1:] if selected else array.shape
        if columns:
            lead, tail = (), (tail[0], count * tail[1])
        shapes.append(jax.ShapeDtypeStruct(lead + tail, array.dtype))
    slots = sum(counts)
    return pl.pallas_call(
        kernel,
        out_shape=shapes,
        in_specs=[pl.BlockSpec(memory_space=pltpu.VMEM)] * amount,
        out_specs=[pl.BlockSpec(memory_space=pl.ANY)] * amount,
        scratch_shapes=[
            pltpu.SemaphoreType.DMA((slots,)),
            pltpu.SemaphoreType.DMA((slots,)),
            pltpu.SemaphoreType.DMA((slots * cores,)),
            pltpu.SemaphoreType.DMA((slots * cores,)),
            pltpu.SemaphoreType.DMA((amount,)),
        ],
        compiler_params=pltpu.CompilerParams(
            collective_id=number, has_side_effects=True, vmem_limit_bytes=16 * 1024 * 1024
        ),
        cost_estimate=pl.CostEstimate(
            flops=10**8, bytes_accessed=4 * 2**20, transcendentals=0
        ),
        name=name,
    )(*[item[0] for item in items])


def plain_exchange(items, plane):
    results = []
    for array, reach, over, selected in items:
        value = array
        if over:
            value = lax.all_gather(value, "tp")
        if reach == "plane":
            value = value if selected else value[None]
        else:
            value = lax.all_gather(value, "sp")
        results.append(value)
    return results


def gated_norm(mixed, gate, gain):
    length = mixed.shape[0]
    groups = mixed.shape[1]
    flat = mixed.reshape(length, groups, -1)
    gated = flat * jax.nn.silu(gate.astype(jnp.float32)).reshape(length, groups, -1)
    scaled = gated * lax.rsqrt(jnp.mean(gated * gated, axis=-1, keepdims=True) + eps)
    return (scaled * gain.reshape(groups, -1)[None]).reshape(length, -1).astype(jnp.bfloat16)


def attend(query, cosine, sine, keys, key_up, value_up_weight, length):
    heads = key_up.shape[1] // UNROTATED_WIDTH
    latent_width = key_up.shape[0]
    whole = UNROTATED_WIDTH + ROPE
    half = ROPE // 2
    step = 2 * length if keys.shape[0] % (2 * length) == 0 else length
    scale = whole ** (-0.5)
    contract = (((1,), (1,)), ((), ()))

    def kernel(q_ref, cos_ref, sin_ref, k_ref, ku_ref, vu_ref, out_ref, q_all, top, total, summed):
        start = lax.axis_index("sp") * length
        for h in range(heads):
            base = h * whole
            turn = q_ref[:, base + UNROTATED_WIDTH : base + whole].astype(jnp.float32)
            first, second = turn[:, :half], turn[:, half:]
            turned = jnp.concatenate(
                [
                    first * cos_ref[...] - second * sin_ref[...],
                    second * cos_ref[...] + first * sin_ref[...],
                ],
                axis=1,
            )
            q_all[h] = jnp.concatenate(
                [q_ref[:, base : base + UNROTATED_WIDTH], turned.astype(jnp.bfloat16)], axis=1
            )
        top[...] = jnp.full(top.shape, floor_score, jnp.float32)
        total[...] = jnp.zeros(total.shape, jnp.float32)
        summed[...] = jnp.zeros(summed.shape, jnp.float32)
        row = start + lax.broadcasted_iota(jnp.int32, (length, step), 0)
        column = lax.broadcasted_iota(jnp.int32, (length, step), 1)

        def visit(j, carry):
            at = pl.ds(pl.multiple_of(j * step, step), step)
            latent = k_ref[at, :latent_width]
            turned = k_ref[at, latent_width : latent_width + ROPE]
            seen = column + j * step <= row
            plain = jnp.dot(latent, ku_ref[...], preferred_element_type=jnp.float32).astype(
                jnp.bfloat16
            )
            all_values = jnp.dot(latent, vu_ref[...], preferred_element_type=jnp.float32).astype(
                jnp.bfloat16
            )
            for h in range(heads):
                values = all_values[:, h * VALUE_WIDTH : (h + 1) * VALUE_WIDTH]
                key = jnp.concatenate(
                    [plain[:, h * UNROTATED_WIDTH : (h + 1) * UNROTATED_WIDTH], turned], axis=1
                )
                scores = (
                    lax.dot_general(q_all[h], key, contract, preferred_element_type=jnp.float32)
                    * scale
                )
                scores = jnp.where(seen, scores, -jnp.inf)
                old = top[h][:, :1]
                new = jnp.maximum(old, jnp.max(scores, axis=1, keepdims=True))
                weights = jnp.exp(scores - new)
                shrink = jnp.exp(old - new)
                now = jnp.sum(weights, axis=1, keepdims=True)
                total[h] = total[h] * shrink + now
                summed[h] = summed[h] * shrink + jnp.dot(
                    weights.astype(jnp.bfloat16), values, preferred_element_type=jnp.float32
                )
                top[h] = jnp.broadcast_to(new, top.shape[1:])
            return carry

        lax.fori_loop(0, (start + length + step - 1) // step, visit, 0)
        for h in range(heads):
            out_ref[:, h * VALUE_WIDTH : (h + 1) * VALUE_WIDTH] = (
                summed[h] / total[h][:, :1]
            ).astype(jnp.bfloat16)

    return pl.pallas_call(
        kernel,
        out_shape=jax.ShapeDtypeStruct((length, heads * VALUE_WIDTH), jnp.bfloat16),
        in_specs=[pl.BlockSpec(memory_space=pltpu.VMEM)] * 6,
        out_specs=pl.BlockSpec(memory_space=pltpu.VMEM),
        scratch_shapes=[
            pltpu.VMEM((heads, length, whole), jnp.bfloat16),
            pltpu.VMEM((heads, length, 128), jnp.float32),
            pltpu.VMEM((heads, length, 128), jnp.float32),
            pltpu.VMEM((heads, length, VALUE_WIDTH), jnp.float32),
        ],
        compiler_params=pltpu.CompilerParams(vmem_limit_bytes=40 * 1024 * 1024),
        cost_estimate=pl.CostEstimate(
            flops=4 * 10**10, bytes_accessed=4 * 2**20, transcendentals=0
        ),
        name="attend",
    )(query, cosine, sine, keys, key_up, value_up_weight)


def fused(
    plane,
    tokens,
    mix_gain,
    query_proj,
    compressed_projection,
    compressed_norm_gain,
    rope_proj,
    key_up,
    value_up_weight,
    scan_input,
    scan_gate,
    scan_write,
    scan_read,
    step_proj,
    conv_input,
    conv_write,
    conv_read,
    decay_log,
    decay_offset,
    skip_gain,
    group_gain,
):
    devices, cores = lax.axis_size("sp"), lax.axis_size("tp")
    planes = devices // plane
    part, width = tokens.shape
    length = part * cores
    depth = scan_input.shape[0]
    kblock = depth * plane
    hw, ww = scan_input.shape[1] // plane, scan_write.shape[1] // plane
    lower, wide = hw + 2 * ww, 2 * hw + 2 * ww
    bounds = ((0, lower), (lower, wide))
    own_heads = decay_log.shape[0] // plane
    heads = key_up.shape[1] // UNROTATED_WIDTH
    latent_width = key_up.shape[0]
    key_rows = (latent_width + ROPE) * part // 128
    whole = UNROTATED_WIDTH + ROPE
    half = ROPE // 2
    scale = whole ** (-0.5)
    span = conv_input.shape[0]
    edge = 16
    bf16, f32 = jnp.bfloat16, jnp.float32
    MESH = pl.DeviceIdType.MESH
    last_contract = (((1,), (1,)), ((), ()))
    first_contract = (((0,), (0,)), ((), ()))
    best = lax.Precision.HIGHEST
    group_step = 2

    def mm(a, b):
        return jnp.dot(a, b, preferred_element_type=f32)

    def kernel(
        *refs
    ):
        sources, (dlog, skip) = refs[:loaded], refs[loaded : loaded + 2]
        att_out, scan_out = refs[loaded + 2 : loaded + 4]
        targets = refs[loaded + 4 : 2 * loaded + 4]
        (
            w_in, w_write, w_read, w_gate, tok, mix, comp, comp_gain, rope, freqs, wq, ku, vu,
            doff, w_step, t_in, t_write, t_read, ggain,
        ) = targets
        (
            load_sem, packed, wbuf, rows, keys, q_all, top, total, summed, stepw, steps, osend,
            obuf, projf, gatef, cbuf, ybuf, runs, before, decayed, state, dsum, ssend, tsend,
            srecv, trecv, incoming, stage, wsend, wrecv, zsend, ksend_up, ksend_plane,
            ksend_core, krecv, rsend, rsend_core, rrecv, rdiag_send,
            rdiag_recv, o_send, o_recv, e_send, e_recv, s_send, s_recv, t_send, t_recv,
            out_send, out_recv,
        ) = refs[2 * loaded + 4 :]
        here, core = lax.axis_index("sp"), lax.axis_index("tp")
        z, n = here // plane, here % plane
        other = cores - 1 - core
        beside, above, across = n + 1 - 2 * (n % 2), (n + 2) % plane, plane - 1 - n
        at_end = (z == 0) | (z == planes - 1)
        nearest = (z + planes - 1) // planes
        farthest = planes - 1 - z

        loads = [
            pltpu.make_async_copy(source, target, load_sem.at[i])
            for i, (source, target) in enumerate(zip(sources, targets))
        ]
        for load in loads:
            load.start()

        def rcopy(src, dst, ss, rs, sp, c):
            return pltpu.make_async_remote_copy(
                src_ref=src, dst_ref=dst, send_sem=ss, recv_sem=rs,
                device_id=(sp, c), device_id_type=MESH,
            )

        def peer(step):
            return z * plane + (n + step) % plane

        barrier = pltpu.get_barrier_semaphore()
        greeted = 0
        for step in range(1, plane):
            pl.semaphore_signal(barrier, inc=1, device_id=(peer(step), core), device_id_type=MESH)
            greeted += 1
        for step in range(1, planes):
            pl.semaphore_signal(
                barrier, inc=1, device_id=((z + step) % planes * plane + n, core),
                device_id_type=MESH,
            )
            greeted += 1
        pl.semaphore_signal(barrier, inc=1, device_id=(here, other), device_id_type=MESH)
        greeted += 1
        for load in loads[:4]:
            load.wait()

        for m in range(plane):
            packed[m, :, :hw] = w_in[:, m * hw : (m + 1) * hw]
            packed[m, :, hw : hw + ww] = w_write[:, m * ww : (m + 1) * ww]
            packed[m, :, hw + ww : lower] = w_read[:, m * ww : (m + 1) * ww]
            packed[m, :, lower:] = w_gate[:, m * hw : (m + 1) * hw]
        wbuf[here] = packed[n]

        pl.semaphore_wait(barrier, greeted)

        def key_slot(sp, c):
            return keys.at[sp * cores + c]

        def key_copy(sp, c, ss, to_sp, to_c):
            return rcopy(
                key_slot(sp, c), key_slot(sp, c), ss, krecv.at[sp * cores + c], to_sp, to_c
            )

        def key_arrived(sp, c):
            key_copy(sp, c, ksend_up.at[0], here, core).wait_recv()

        def key_up_copy(d):
            return key_copy(here, core, ksend_up.at[d], here + d * plane, core)

        sides = (beside, above)

        def key_plane_copy(d, step):
            return key_copy(
                here - d * plane, core, ksend_plane.at[d * plane + step], peer(step), core
            )

        def key_core_copy(sp):
            return key_copy(sp, core, ksend_core.at[sp], here, other)

        sides = (beside, above)

        def chunk(group, index):
            low, high = bounds[group]
            return wbuf.at[index, :, low:high]

        def w_arrived(group, index):
            rcopy(
                chunk(group, index), chunk(group, index), zsend.at[0, group, index],
                wrecv.at[group, index], here, core,
            ).wait_recv()

        def w_plane_copy(group, step):
            low, high = bounds[group]
            goal = (n + step) % plane
            return rcopy(
                packed.at[goal, :, low:high], chunk(group, here), wsend.at[group, step],
                wrecv.at[group, here], z * plane + goal, core,
            )

        def z_copy(group, index, up):
            return rcopy(
                chunk(group, index), chunk(group, index), zsend.at[up, group, index],
                wrecv.at[group, index], here + (plane if up else -plane), core,
            )

        def has_next(up):
            return z + 1 < planes if up else z > 0

        def own_weights(group, steps_of):
            for step in steps_of:
                index = z * plane + (n - step + plane) % plane
                if step:
                    w_arrived(group, index)
                for up in (0, 1):
                    @pl.when(has_next(up))
                    def _():
                        z_copy(group, index, up).start()

        def far_weights(group, d, forward):
            for up in (0, 1):
                source = z - d if up else z + d
                exists = (source >= 0) & (source < planes)
                gate = has_next(up) if forward else jnp.logical_not(has_next(up))

                @pl.when(exists & gate)
                def _():
                    for q in range(plane):
                        index = source * plane + q
                        w_arrived(group, index)
                        if forward:
                            z_copy(group, index, up).start()

        for step in range(1, plane):
            w_plane_copy(0, step).start()
        own_weights(0, (0,))

        for load in loads[4:10]:
            load.wait()
        def normed_rows(values, gain, count):
            mean = jnp.sum(values * values, axis=-1, keepdims=True) / count
            return values * lax.rsqrt(mean + eps) * gain

        normed = normed_rows(tok[...].astype(f32), mix[...], width).astype(bf16)

        def rows_at(slot, c):
            return pl.ds(pl.multiple_of(slot * length + c * part, part), part)

        for p in range(planes):
            rows[p, rows_at(n, core), :] = normed[:, p * kblock : (p + 1) * kblock]

        def angles(start, count):
            position = (start + lax.broadcasted_iota(jnp.int32, (count, 1), 0)).astype(f32)
            angle = position * freqs[...]
            return jnp.cos(angle), jnp.sin(angle)

        def turn(first, second, cosine, sine):
            return [first * cosine - second * sine, second * cosine + first * sine]

        latent = normed_rows(mm(normed, comp[...]), comp_gain[...], latent_width)
        small = lax.dot_general(normed, rope[...], last_contract, preferred_element_type=f32)
        cosine, sine = angles(here * length + core * part, part)
        own_slot = here * cores + core
        for low in range(0, latent_width, 128):
            keys[own_slot, low * part // 128 : (low + 128) * part // 128] = latent[
                :, low : low + 128
            ].astype(bf16)
        turned_key = jnp.concatenate(
            turn(small[:, :half], small[:, half:], cosine, sine), axis=1
        ).astype(bf16)
        keys[own_slot, latent_width * part // 128 :] = jnp.concatenate(
            [turned_key[: part // 2], turned_key[part // 2 :]], axis=1
        )

        for d in range(1, planes):
            @pl.when(z + d < planes)
            def _():
                key_up_copy(d).start()
        for step in range(1, plane):
            key_plane_copy(0, step).start()
        key_core_copy(here).start()

        def row_copy(slot, ss, to_sp, to_c):
            at = rows.at[:, rows_at(slot, core), :]
            return rcopy(at, at, ss, rrecv.at[slot * cores + core], to_sp, to_c)

        def row_plane_copy(side):
            return row_copy(n, rsend.at[side], z * plane + sides[side], core)

        def row_part(slot, side, to_sp):
            low, high = side * planes // 2, (side + 1) * planes // 2
            at = rows.at[low:high, rows_at(slot, core), :]
            return rcopy(at, at, rdiag_send.at[side], rdiag_recv.at[side], to_sp, core)

        def row_relay(side):
            return row_part(sides[side], side, z * plane + sides[1 - side])

        def row_core_copy(slot):
            return row_copy(slot, rsend_core.at[slot], here, other)

        def row_arrived(slot, c):
            at = rows.at[:, rows_at(slot, c), :]
            rcopy(at, at, rsend.at[0], rrecv.at[slot * cores + c], here, core).wait_recv()

        def offset_copy(step):
            goal = (n + step) % plane
            return rcopy(
                osend.at[goal], obuf.at[n], o_send.at[step], o_recv.at[n],
                z * plane + goal, core,
            )

        row_core_copy(n).start()

        positions = plane * length
        at_edge = rows.at[:, positions : positions + edge, :]
        closing = (n == plane - 1) & (core == cores - 1)

        def edge_up_copy():
            return rcopy(
                rows.at[:, positions - edge : positions, :], at_edge, e_send.at[0], e_recv,
                here + plane, core,
            )

        def edge_plane_copy(step):
            return rcopy(at_edge, at_edge, e_send.at[step], e_recv, peer(step), core)

        def edge_core_copy():
            return rcopy(at_edge, at_edge, e_send.at[plane], e_recv, here, other)

        def edge_arrived():
            rcopy(at_edge, at_edge, e_send.at[0], e_recv, here, core).wait_recv()

        @pl.when(closing & (z + 1 < planes))
        def _():
            edge_up_copy().start()

        for load in loads[10:]:
            load.wait()
        for m in range(plane):
            osend[m, :own_heads] = doff[m * own_heads : (m + 1) * own_heads]
        obuf[n] = osend[n]

        @pl.when(z == 0)
        def _():
            rows[:, plane * length :, :] = jnp.zeros((planes, edge, kblock), bf16)

        row_arrived(n, other)
        own_rows = pl.ds(pl.multiple_of(n * length, length), length)
        query = mm(rows[0, own_rows, :], wq[:kblock, :])
        for p in range(1, planes):
            query += mm(rows[p, own_rows, :], wq[p * kblock : (p + 1) * kblock, :])
        query = query.astype(bf16)
        cosine, sine = angles(here * length, length)
        for h in range(heads):
            base = h * whole
            rope_part = query[:, base + UNROTATED_WIDTH : base + whole].astype(f32)
            q_all[h] = jnp.concatenate(
                [query[:, base : base + UNROTATED_WIDTH]]
                + [
                    v.astype(bf16)
                    for v in turn(rope_part[:, :half], rope_part[:, half:], cosine, sine)
                ],
                axis=1,
            )
        top[...] = jnp.full(top.shape, floor_score, f32)
        total[...] = jnp.zeros(total.shape, f32)
        summed[...] = jnp.zeros(summed.shape, f32)

        own_weights(0, range(1, plane))
        for d in range(1, planes):
            @pl.when(z >= d)
            def _():
                key_arrived(here - d * plane, core)
                for step in range(1, plane):
                    key_plane_copy(d, step).start()
                key_core_copy(here - d * plane).start()

        @pl.when(closing & (z > 0))
        def _():
            edge_arrived()
            for step in range(1, plane):
                edge_plane_copy(step).start()
            edge_core_copy().start()

        for step in range(1, plane):
            w_plane_copy(1, step).start()
        for side in (0, 1):
            row_plane_copy(side).start()
        for step in range(1, plane):
            offset_copy(step).start()

        def pass_keys(d):
            for step in range(1, plane):
                sp = (z - d) * plane + (n + step) % plane
                key_arrived(sp, core)
                key_core_copy(sp).start()

        def other_keys(d):
            for q in range(plane):
                key_arrived((z - d) * plane + q, other)

        size = group_step * length
        row = lax.broadcasted_iota(jnp.int32, (length, size), 0)
        column = lax.broadcasted_iota(jnp.int32, (length, size), 1)

        def visit(first_block, limit):
            count = group_step * cores
            block = keys[pl.ds(first_block * cores, count)]
            lat = jnp.concatenate(
                [
                    block[:, low * part // 128 : (low + 128) * part // 128].reshape(size, 128)
                    for low in range(0, latent_width, 128)
                ],
                axis=1,
            )
            turned = block[:, latent_width * part // 128 :]
            turned = jnp.concatenate([turned[:, :, :ROPE], turned[:, :, ROPE:]], axis=1)
            turned = turned.reshape(size, ROPE)
            plain = mm(lat, ku[...]).astype(bf16)
            all_values = mm(lat, vu[...]).astype(bf16)
            if limit is not None:
                seen = column <= row + limit
            for h in range(heads):
                values = all_values[:, h * VALUE_WIDTH : (h + 1) * VALUE_WIDTH]
                key = jnp.concatenate(
                    [plain[:, h * UNROTATED_WIDTH : (h + 1) * UNROTATED_WIDTH], turned], axis=1
                )
                scores = (
                    lax.dot_general(q_all[h], key, last_contract, preferred_element_type=f32)
                    * scale
                )
                if limit is not None:
                    scores = jnp.where(seen, scores, -jnp.inf)
                old = top[h][:, :1]
                new = jnp.maximum(old, jnp.max(scores, axis=1, keepdims=True))
                weights = jnp.exp(scores - new)
                shrink = jnp.exp(old - new)
                now = jnp.sum(weights, axis=1, keepdims=True)
                total[h] = total[h] * shrink + now
                summed[h] = summed[h] * shrink + mm(weights.astype(bf16), values)
                top[h] = jnp.broadcast_to(new, top.shape[1:])

        pass_keys(0)

        @pl.when(z >= 1)
        def _():
            pass_keys(1)

        far_weights(0, 1, True)
        other_keys(0)

        def near(j, carry):
            visit(z * plane + j * group_step, (n - j * group_step) * length)
            return carry

        lax.fori_loop(0, n // group_step + 1, near, 0)

        def further(d, carry):
            @pl.when(z > d)
            def _():
                pass_keys(d + 1)

            @pl.when(d == 1)
            def _():
                own_weights(1, range(plane))

            @pl.when(z >= d)
            def _():
                other_keys(d)

                def inner(j, carry):
                    visit((z - d) * plane + j * group_step, None)
                    return carry

                lax.fori_loop(0, plane // group_step, inner, 0)

            return carry

        lax.fori_loop(1, planes, further, 0)
        for h in range(heads):
            att_out[:, h * VALUE_WIDTH : (h + 1) * VALUE_WIDTH] = (
                summed[h] / total[h][:, :1]
            ).astype(bf16)

        @pl.when((z > 0) & (core == cores - 1) & (n < plane - 1))
        def _():
            edge_arrived()
            edge_core_copy().start()

        for side in (0, 1):
            row_arrived(sides[side], core)
            row_relay(side).start()
            row_core_copy(sides[side]).start()
        for d in range(2, planes - 1):
            far_weights(0, d, True)
        far_weights(1, 1, True)
        for side in (0, 1):
            row_part(across, side, here).wait_recv()
        row_core_copy(across).start()
        for step in range(1, plane):
            row_arrived((n + step) % plane, other)
        for d in range(1, planes - 1):
            far_weights(0, d, False)

        def tile(k):
            return pl.ds(pl.multiple_of(k * length, length), length)

        def project(p, values, group):
            low, high = bounds[group]
            block = wbuf[pl.ds(p * plane, plane), :, low:high]
            return mm(values, block.reshape(kblock, high - low))

        def sum_near(group, at, store):
            @pl.when(at_end)
            def _():
                out = project(nearest, rows[nearest, at, :], group)
                for p in range(1, planes - 1):
                    out += project(nearest + p, rows[nearest + p, at, :], group)
                store(out, False)

            @pl.when(jnp.logical_not(at_end))
            def _():
                out = project(0, rows[0, at, :], group)
                for p in range(1, planes):
                    out += project(p, rows[p, at, :], group)
                store(out, False)

        def sum_far(group, at, store):
            store(project(farthest, rows[farthest, at, :], group), True)

        strip = (positions + edge) // 5
        strips = (positions + edge) // strip

        def put(low, count, out, add):
            at = pl.ds(low, count)
            projf[at, :] = projf[at, :] + out if add else out

        def every_strip(method):
            def body(i, carry):
                def store(out, add):
                    put(pl.multiple_of(i * strip + edge, edge), strip, out, add)

                method(0, pl.ds(pl.multiple_of(i * strip, edge), strip), store)
                return carry

            lax.fori_loop(0, strips - 1, body, 0)

        def last_strip(method):
            low = (strips - 1) * strip

            def store(out, add):
                put(low + edge, strip - edge, out[: strip - edge], add)
                put(0, edge, out[strip - edge :], add)

            method(0, slice(low, low + strip), store)

        every_strip(sum_near)

        @pl.when((z > 0) & (core < cores - 1))
        def _():
            edge_arrived()

        last_strip(sum_near)
        lane = lax.broadcasted_iota(jnp.int32, (128, w_step.shape[0]), 0)
        which = lax.broadcasted_iota(jnp.int32, (128, w_step.shape[0]), 1)
        first_head = (core * plane + n) * own_heads
        chosen = ((which == lane + first_head) & (lane < own_heads)).astype(bf16)
        stepw[...] = mm(chosen, w_step[...]).astype(bf16)

        def step_tile(k, carry):
            raw = jnp.zeros((length, 128), f32)
            for p in range(planes):
                raw += lax.dot_general(
                    rows[p, tile(k), :], stepw[:, p * kblock : (p + 1) * kblock],
                    last_contract, preferred_element_type=f32,
                )
            steps[k] = jnp.maximum(raw, 0.0) + jnp.log1p(jnp.exp(-jnp.abs(raw)))
            return carry

        lax.fori_loop(0, plane, step_tile, 0)
        far_weights(0, planes - 1, False)

        @pl.when(at_end)
        def _():
            every_strip(sum_far)
            last_strip(sum_far)

        taps = jnp.concatenate(
            [
                t_in[:, pl.ds(pl.multiple_of(n * hw, hw), hw)],
                t_write[:, pl.ds(pl.multiple_of(n * ww, ww), ww)],
                t_read[:, pl.ds(pl.multiple_of(n * ww, ww), ww)],
            ],
            axis=1,
        ).astype(f32)

        def conv_tile(k, carry):
            base = pl.ds(pl.multiple_of(k * length, length), length + edge)
            for low in range(0, lower, 128):
                at = slice(low, low + 128)
                values = projf[base, at].astype(bf16).astype(f32)
                result = jnp.zeros((length, 128), f32)
                for i in range(span):
                    shift = edge - span + 1 + i
                    result = result + taps[i : i + 1, at] * values[shift : shift + length]
                cbuf[tile(k), at] = (result * jax.nn.sigmoid(result)).astype(bf16)
            return carry

        lax.fori_loop(0, plane, conv_tile, 0)

        for step in range(1, plane):
            slot = (n - step + plane) % plane
            rcopy(
                obuf.at[slot], obuf.at[slot], o_send.at[0], o_recv.at[slot], here, core
            ).wait_recv()
        lane_row = lax.broadcasted_iota(jnp.int32, (1, 128), 1)
        rate = jnp.zeros((1, 128), f32)
        for h in range(own_heads):
            rate = jnp.where(lane_row == h, dlog[n * own_heads + h], rate)
        rate = -jnp.exp(rate)
        causal = lax.broadcasted_iota(jnp.int32, (length, length), 0) >= lax.broadcasted_iota(
            jnp.int32, (length, length), 1
        )
        tri = causal.astype(f32)

        def per_lane(columns):
            return jnp.concatenate(
                [
                    jnp.broadcast_to(columns[:, h : h + 1], (columns.shape[0], SSM_DIM))
                    for h in range(own_heads)
                ],
                axis=1,
            )

        def per_row(values):
            return jnp.concatenate(
                [
                    jnp.broadcast_to(values[:, h : h + 1], (SSM_DIM, SSM_STATE))
                    for h in range(own_heads)
                ],
                axis=0,
            )

        state[...] = jnp.zeros(state.shape, f32)
        dsum[...] = jnp.zeros(dsum.shape, f32)

        def scan_tile(k, carry):
            step_col = steps[k]
            off_col = jnp.concatenate(
                [obuf[k], jnp.zeros((128 - obuf.shape[1], length), f32)], axis=0
            ).T
            decay = jnp.where(lane_row < own_heads, rate * step_col + off_col, 0.0)
            running = jnp.dot(tri, decay, precision=best, preferred_element_type=f32)
            runs[k] = running
            run_row, step_row = running.T, step_col.T
            x = cbuf[tile(k), :hw]
            w = cbuf[tile(k), hw : hw + ww]
            r = cbuf[tile(k), hw + ww : lower]
            inner = lax.dot_general(r, w, last_contract, preferred_element_type=f32)
            for h in range(own_heads):
                at = slice(h * SSM_DIM, (h + 1) * SSM_DIM)
                spread = jnp.where(
                    causal, running[:, h : h + 1] - run_row[h : h + 1, :], -jnp.inf
                )
                mixing = inner * jnp.exp(spread) * step_row[h : h + 1, :]
                ybuf[tile(k), at] = (
                    mm(mixing.astype(bf16), x[:, at])
                    + skip[n * own_heads + h] * x[:, at].astype(f32)
                )
            last = running[length - 1 : length, :]
            to_end = jnp.exp(last - running) * step_col
            weighted = (x.astype(f32) * per_lane(to_end)).astype(bf16)
            update = lax.dot_general(weighted, w, first_contract, preferred_element_type=f32)
            before[k] = state[...]
            decayed[k] = dsum[...]
            state[...] = per_row(jnp.exp(last)) * state[...] + update
            dsum[...] = dsum[...] + last
            return carry

        lax.fori_loop(0, plane, scan_tile, 0)

        ssend[...] = state[...].astype(bf16)
        tsend[...] = dsum[...]

        def state_copies(d):
            to = here + d * plane
            return (
                rcopy(ssend, srecv.at[z], s_send.at[d], s_recv.at[z], to, core),
                rcopy(tsend, trecv.at[z], t_send.at[d], t_recv.at[z], to, core),
            )

        for d in range(1, planes):
            @pl.when(z + d < planes)
            def _():
                for copy in state_copies(d):
                    copy.start()

        for d in range(2, planes):
            far_weights(1, d, True)
        for d in range(1, planes - 1):
            far_weights(1, d, False)

        def gate_tile(k, carry):
            def store(out, add):
                gatef[tile(k), :] = out

            sum_near(1, tile(k), store)
            return carry

        lax.fori_loop(0, plane, gate_tile, 0)
        far_weights(1, planes - 1, False)
        incoming[...] = jnp.zeros(incoming.shape, f32)
        for p in range(planes - 1):
            @pl.when(p < z)
            def _():
                rcopy(
                    ssend, srecv.at[p], s_send.at[0], s_recv.at[p], here, core
                ).wait_recv()
                rcopy(
                    tsend, trecv.at[p], t_send.at[0], t_recv.at[p], here, core
                ).wait_recv()
                incoming[...] = per_row(jnp.exp(trecv[p][:1])) * incoming[...] + srecv[
                    p
                ].astype(f32)

        own_columns = pl.ds(pl.multiple_of(n * hw, hw), hw)
        gain = ggain[:, own_columns]

        def out_copy(k):
            return rcopy(
                stage.at[k], scan_out.at[:, own_columns], out_send.at[k], out_recv.at[n],
                z * plane + k, core,
            )

        def finish(i, carry):
            flip = plane - 1 - i
            k = (n // 2 + flip // 2) % 2 * 2 + (n + flip) % 2

            @pl.when(at_end)
            def _():
                def store(out, add):
                    gatef[tile(k), :] = gatef[tile(k), :] + out

                sum_far(1, tile(k), store)

            gate = gatef[tile(k), :].astype(bf16).astype(f32)
            entered = (
                before[k] + per_row(jnp.exp(decayed[k][:1])) * incoming[...]
            ).astype(bf16)
            carried = lax.dot_general(
                cbuf[tile(k), hw + ww : lower], entered, last_contract,
                preferred_element_type=f32,
            )
            mixed = ybuf[tile(k), :] + carried * per_lane(jnp.exp(runs[k]))
            gated = mixed * (gate * jax.nn.sigmoid(gate))
            out = normed_rows(gated, gain, hw).astype(bf16)
            stage[k] = out

            @pl.when(k != n)
            def _():
                out_copy(k).start()

            @pl.when(k == n)
            def _():
                scan_out[:, own_columns] = out

            return carry

        lax.fori_loop(0, plane, finish, 0)
        for step in range(1, plane):
            slot = (n + step) % plane
            at = scan_out.at[:, pl.ds(pl.multiple_of(slot * hw, hw), hw)]
            rcopy(stage.at[0], at, out_send.at[0], out_recv.at[slot], here, core).wait_recv()

        for d in range(1, planes):
            @pl.when(z + d < planes)
            def _():
                key_up_copy(d).wait_send()
                for copy in state_copies(d):
                    copy.wait_send()
        for d in range(planes):
            @pl.when(z >= d)
            def _():
                for step in range(1, plane):
                    key_plane_copy(d, step).wait_send()
                for q in range(plane):
                    key_core_copy((z - d) * plane + q).wait_send()
        for step in range(1, plane):
            for group in (0, 1):
                w_plane_copy(group, step).wait_send()
            offset_copy(step).wait_send()
            out_copy((n + step) % plane).wait_send()
        for side in (0, 1):
            row_plane_copy(side).wait_send()
            row_relay(side).wait_send()
        for slot in range(plane):
            row_core_copy(slot).wait_send()

        @pl.when(closing & (z + 1 < planes))
        def _():
            edge_up_copy().wait_send()

        @pl.when(closing & (z > 0))
        def _():
            for step in range(1, plane):
                edge_plane_copy(step).wait_send()

        @pl.when((z > 0) & (core == cores - 1))
        def _():
            edge_core_copy().wait_send()

        for up in (0, 1):
            for p in range(planes):
                @pl.when(((p <= z) if up else (p >= z)) & has_next(up))
                def _():
                    for q in range(plane):
                        for group in (0, 1):
                            z_copy(group, p * plane + q, up).wait_send()

    vmem = pl.BlockSpec(memory_space=pltpu.VMEM)
    smem = pl.BlockSpec(memory_space=pltpu.SMEM)
    hbm = pl.BlockSpec(memory_space=pltpu.HBM)
    freqs = np.float32(theta) ** (-np.arange(half, dtype=np.float32) * np.float32(2.0 / ROPE))
    inputs = (
        scan_input,
        scan_write,
        scan_read,
        scan_gate,
        tokens,
        mix_gain[None, :],
        compressed_projection,
        compressed_norm_gain[None, :],
        rope_proj.T,
        jnp.asarray(freqs[None, :], f32),
        query_proj,
        key_up,
        value_up_weight,
        decay_offset.T,
        step_proj.T,
        conv_input,
        conv_write,
        conv_read,
        group_gain[None, :],
    )
    loaded = len(inputs)
    dma = pltpu.SemaphoreType.DMA
    positions = plane * length
    results = (
        jax.ShapeDtypeStruct((length, heads * VALUE_WIDTH), bf16),
        jax.ShapeDtypeStruct((length, scan_input.shape[1]), bf16),
    )
    outs = pl.pallas_call(
        kernel,
        out_shape=results,
        in_specs=[hbm] * loaded + [smem, smem],
        out_specs=(vmem, vmem),
        scratch_shapes=[pltpu.VMEM(value.shape, value.dtype) for value in inputs]
        + [
            dma((loaded,)),
            pltpu.VMEM((plane, depth, wide), bf16),
            pltpu.VMEM((devices, depth, wide), bf16),
            pltpu.VMEM((planes, positions + edge, kblock), bf16),
            pltpu.VMEM((devices * cores, key_rows, 128), bf16),
            pltpu.VMEM((heads, length, whole), bf16),
            pltpu.VMEM((heads, length, 128), f32),
            pltpu.VMEM((heads, length, 128), f32),
            pltpu.VMEM((heads, length, VALUE_WIDTH), f32),
            pltpu.VMEM((128, width), bf16),
            pltpu.VMEM((plane, length, 128), f32),
            pltpu.VMEM((plane, 8, length), f32),
            pltpu.VMEM((plane, 8, length), f32),
            pltpu.VMEM((edge + positions, lower), f32),
            pltpu.VMEM((positions, hw), f32),
            pltpu.VMEM((positions, lower), bf16),
            pltpu.VMEM((positions, hw), f32),
            pltpu.VMEM((plane, length, 128), f32),
            pltpu.VMEM((plane, own_heads * SSM_DIM, SSM_STATE), f32),
            pltpu.VMEM((plane, 8, 128), f32),
            pltpu.VMEM((own_heads * SSM_DIM, SSM_STATE), f32),
            pltpu.VMEM((8, 128), f32),
            pltpu.VMEM((own_heads * SSM_DIM, SSM_STATE), bf16),
            pltpu.VMEM((8, 128), f32),
            pltpu.VMEM((planes, own_heads * SSM_DIM, SSM_STATE), bf16),
            pltpu.VMEM((planes, 8, 128), f32),
            pltpu.VMEM((own_heads * SSM_DIM, SSM_STATE), f32),
            pltpu.VMEM((plane, length, hw), bf16),
            dma((2, plane)),
            dma((2, devices)),
            dma((2, 2, devices)),
            dma((planes,)),
            dma((devices,)),
            dma((devices,)),
            dma((devices * cores,)),
            dma((2,)),
            dma((plane,)),
            dma((plane * cores,)),
            dma((2,)),
            dma((2,)),
            dma((plane,)),
            dma((plane,)),
            dma((plane + 1,)),
            dma,
            dma((planes,)),
            dma((planes,)),
            dma((planes,)),
            dma((planes,)),
            dma((plane,)),
            dma((plane,)),
        ],
        compiler_params=pltpu.CompilerParams(
            collective_id=1, has_side_effects=True, vmem_limit_bytes=60 * 1024 * 1024
        ),
        name="fused",
    )(*inputs, decay_log, skip_gain)

    def settle(a_in, b_in, a_out, b_out, a_mid, b_mid, ins, leaves):
        rows_each = length // 2
        pieces = [(a_in, a_mid, a_out)] + [
            tuple(ref.at[low : low + rows_each] for ref in (b_in, b_mid, b_out))
            for low in (0, rows_each)
        ]
        first = [
            pltpu.make_async_copy(source, middle, ins.at[i])
            for i, (source, middle, _) in enumerate(pieces)
        ]
        second = [
            pltpu.make_async_copy(middle, target, leaves.at[i])
            for i, (_, middle, target) in enumerate(pieces)
        ]
        for copy in first:
            copy.start()
        for copy, after in zip(first, second):
            copy.wait()
            after.start()
        for copy in second:
            copy.wait()

    return pl.pallas_call(
        settle,
        out_shape=results,
        in_specs=[hbm, hbm],
        out_specs=(hbm, hbm),
        scratch_shapes=[pltpu.VMEM(value.shape, value.dtype) for value in results]
        + [dma((3,)), dma((3,))],
        compiler_params=pltpu.CompilerParams(vmem_limit_bytes=60 * 1024 * 1024),
        name="settle",
    )(*outs)


def shards(
    tokens,
    mix_gain,
    query_proj,
    compressed_projection,
    compressed_norm_gain,
    rope_proj,
    key_up,
    value_up_weight,
    scan_input,
    scan_gate,
    scan_write,
    scan_read,
    step_proj,
    conv_input,
    conv_write,
    conv_read,
    decay_log,
    decay_offset,
    skip_gain,
    group_gain,
):
    groups = scan_write.shape[1] // SSM_STATE
    devices, cores = lax.axis_size("sp"), lax.axis_size("tp")
    plane = groups if devices % groups == 0 else 1
    planes = devices // plane
    sp_index, core = lax.axis_index("sp"), lax.axis_index("tp")
    across, within = sp_index // plane, sp_index % plane
    own_groups = groups // plane
    direct = plane > 1
    if direct and cores == 2 and own_groups == 1 and plane == 4 and planes > 1:
        return fused(
            plane,
            tokens,
            mix_gain,
            query_proj,
            compressed_projection,
            compressed_norm_gain,
            rope_proj,
            key_up,
            value_up_weight,
            scan_input,
            scan_gate,
            scan_write,
            scan_read,
            step_proj,
            conv_input,
            conv_write,
            conv_read,
            decay_log,
            decay_offset,
            skip_gain,
            group_gain,
        )

    def move(items, name, number, columns=False):
        if direct:
            return exchange(items, plane, name, number, columns)
        return plain_exchange(items, plane)

    depth = scan_input.shape[0]
    widths = [w.shape[1] // plane for w in (scan_input, scan_gate, scan_write, scan_read)]
    offsets = [sum(widths[:i]) for i in range(4)]
    packed = jnp.stack(
        [
            jnp.concatenate(
                [
                    w[:, n * size : (n + 1) * size]
                    for w, size in zip((scan_input, scan_gate, scan_write, scan_read), widths)
                ],
                axis=1,
            )
            for n in range(plane)
        ]
    )
    (part_weights,) = move([(packed, "plane", False, True)], "weights_in_plane", 1)
    weights = lax.all_gather(
        part_weights.reshape(plane * depth, -1),
        "sp",
        axis=0,
        tiled=True,
        axis_index_groups=[[p * plane + n for p in range(planes)] for n in range(plane)],
    )

    own_normed = rms_scale(tokens, mix_gain).astype(jnp.bfloat16)
    part = tokens.shape[0]
    length = part * cores
    latent_width = compressed_projection.shape[1]
    small = jnp.dot(
        own_normed,
        jnp.concatenate([compressed_projection, rope_proj], axis=1),
        preferred_element_type=jnp.float32,
    )
    latent = rms_scale(small[:, :latent_width], compressed_norm_gain).astype(jnp.bfloat16)
    part_positions = sp_index * length + core * part + jnp.arange(part, dtype=jnp.int32)
    key_turned = rotate(small[:, latent_width:], part_positions).astype(jnp.bfloat16)
    padding = jnp.zeros((part, -(latent_width + ROPE) % 128), jnp.bfloat16)
    own_keys = jnp.concatenate([latent, key_turned, padding], axis=1)
    all_keys, all_rows, offsets_seen = move(
        [
            (own_keys, "all", True, False),
            (own_normed, "plane", True, False),
            (decay_offset.T, "plane", False, False),
        ],
        "rows_and_keys",
        2,
    )
    all_keys = all_keys.reshape(devices * length, -1)
    all_rows = all_rows.reshape(plane * length, -1)
    edge_rows = from_behind(all_rows[plane * length - 8 :], "sp", plane)
    positions = sp_index * length + jnp.arange(length, dtype=jnp.int32)
    rows = lax.dynamic_slice_in_dim(all_rows, within * length, length, 0)
    query = jnp.dot(rows, query_proj, preferred_element_type=jnp.float32).astype(jnp.bfloat16)
    half = ROPE // 2
    freqs = theta ** (-jnp.arange(half, dtype=jnp.float32) * 2.0 / ROPE)
    angle = positions.astype(jnp.float32)[:, None] * freqs[None, :]
    attended = attend(
        query, jnp.cos(angle), jnp.sin(angle), all_keys, key_up, value_up_weight, length
    )

    def own_part(array, axis, size):
        return lax.dynamic_slice_in_dim(array, within * size, size, axis)

    local_heads = decay_log.shape[0]
    own_heads = local_heads // plane
    per_group = local_heads // groups
    step_raw = jnp.dot(
        all_rows,
        lax.dynamic_slice_in_dim(
            step_proj, core * local_heads + within * own_heads, own_heads, 1
        ),
        preferred_element_type=jnp.float32,
    )
    step_size = jax.nn.softplus(step_raw)
    own_offset = own_part(offsets_seen, 1, own_heads)
    step_values = jnp.transpose(step_size.reshape(plane, length, own_heads), (0, 2, 1))
    decay_values = (
        -jnp.exp(own_part(decay_log, 0, own_heads))[None, :, None] * step_values + own_offset
    )

    projected = jnp.dot(all_rows, weights, preferred_element_type=jnp.float32).astype(jnp.bfloat16)
    edge = jnp.dot(edge_rows, weights, preferred_element_type=jnp.float32).astype(jnp.bfloat16)
    span = conv_input.shape[0] - 1

    def convolved(i, taps):
        at = slice(offsets[i], offsets[i] + widths[i])
        return short_conv(projected[:, at], edge[8 - span :, at], own_part(taps, 1, widths[i]))

    head_conv = convolved(0, conv_input)
    gate = projected[:, offsets[1] : offsets[1] + widths[1]]
    writes = convolved(2, conv_write)
    reads = convolved(3, conv_read)
    blocks = plane * own_groups

    def by_block(values, last):
        split = values.reshape(plane, length, own_groups, last)
        return jnp.transpose(split, (0, 2, 1, 3)).reshape(blocks, length, last)

    head_values = jnp.transpose(
        head_conv.reshape(plane, length, own_groups, per_group, SSM_DIM), (0, 2, 3, 1, 4)
    ).reshape(blocks, per_group, length, SSM_DIM)
    write_values = by_block(writes, SSM_STATE)
    read_values = by_block(reads, SSM_STATE)
    running, state, mixed = local_scan(
        head_values,
        step_values.reshape(blocks, per_group, length),
        decay_values.reshape(blocks, per_group, length),
        write_values,
        read_values,
    )
    states = state.reshape(plane, own_heads, SSM_DIM, SSM_STATE)
    totals = running[..., -1].reshape(plane, own_heads)
    before, decayed = [jnp.zeros_like(states[0])], [jnp.zeros_like(totals[0])]
    for index in range(plane):
        before.append(jnp.exp(totals[index])[:, None, None] * before[-1] + states[index])
        decayed.append(totals[index] + decayed[-1])
    sent_total = jnp.pad(decayed[-1][None, :], ((0, 7), (0, 128 - own_heads)))
    seen_states, seen_totals = move(
        [
            (before[-1].reshape(-1, SSM_STATE).astype(jnp.bfloat16), "line", False, False),
            (sent_total, "line", False, False),
        ],
        "states",
        3,
    )
    seen_states = seen_states.reshape(planes, own_heads, SSM_DIM, SSM_STATE).astype(jnp.float32)
    seen_totals = seen_totals[:, 0, :own_heads]
    index = jnp.arange(planes)
    between = (index[None, :] > index[:, None]) & (index[None, :] < across)
    path = jnp.sum(jnp.where(between[:, :, None], seen_totals[None], 0.0), axis=1)
    reached = (index < across)[:, None]
    factor = jnp.where(reached, jnp.exp(path), 0.0)
    incoming = jnp.sum(seen_states * factor[:, :, None, None], axis=0)
    entered = jnp.stack(
        [
            before[k] + jnp.exp(decayed[k])[:, None, None] * incoming
            for k in range(plane)
        ]
    ).reshape(blocks, per_group, SSM_DIM, SSM_STATE)
    carried = jnp.einsum(
        "gln,grpn->grlp",
        read_values,
        entered.astype(jnp.bfloat16),
        preferred_element_type=jnp.float32,
    )
    skip = jnp.broadcast_to(
        own_part(skip_gain, 0, own_heads).reshape(1, own_groups, per_group),
        (plane, own_groups, per_group),
    ).reshape(blocks, per_group, 1, 1)
    mixed = (
        mixed
        + carried * jnp.exp(running)[..., None]
        + skip * head_values.astype(jnp.float32)
    )
    mixed = jnp.transpose(
        mixed.reshape(plane, own_groups, per_group, length, SSM_DIM), (0, 3, 1, 2, 4)
    ).reshape(plane * length, own_groups, per_group, SSM_DIM)
    scanned = gated_norm(mixed, gate, own_part(group_gain, 0, widths[0]))
    (columns,) = move(
        [(scanned.reshape(plane, length, -1), "plane", False, True)], "outputs_in_plane", 4, True
    )
    scanned = columns.reshape(length, -1)
    return (attended, scanned)


def solution(mesh):
    in_specs = (
        P(("sp", "tp"), None),
        P(),
        P(None, "tp"),
        P(),
        P(),
        P(),
        P(None, "tp"),
        P(None, "tp"),
        P("sp", "tp"),
        P("sp", "tp"),
        P("sp", "tp"),
        P("sp", "tp"),
        P(),
        P(None, "tp"),
        P(None, "tp"),
        P(None, "tp"),
        P("tp"),
        P("sp", "tp"),
        P("tp"),
        P("tp"),
    )
    out_specs = (P("sp", "tp"), P("sp", "tp"))
    return jax.shard_map(shards, mesh=mesh, in_specs=in_specs, out_specs=out_specs, check_vma=False)
```

```python
import jax
import jax.numpy as jnp
import numpy as np
from jax import lax
from jax.experimental import pallas as pl
from jax.experimental.pallas import tpu as pltpu
from jax.sharding import PartitionSpec as P

UNROTATED_WIDTH = 128
ROPE = 64
VALUE_WIDTH = 128
SSM_DIM = 64
SSM_STATE = 128


eps = 1e-06
theta = 10000.0
floor_score = -1e30


def from_behind(value, axis, steps):
    count = lax.axis_size(axis)
    initial, last = (max(0, -steps), min(count, count - steps))
    return lax.ppermute(value, axis, [(source, source + steps) for source in range(initial, last)])


def rms_scale(values, gain):
    wide = values.astype(jnp.float32)
    return wide * lax.rsqrt(jnp.mean(wide * wide, axis=-1, keepdims=True) + eps) * gain


def rotate(values, positions):
    half = values.shape[-1] // 2
    freqs = theta ** (-jnp.arange(half, dtype=jnp.float32) * 2.0 / values.shape[-1])
    angle = positions.astype(jnp.float32)[:, None] * freqs[None, :]
    cosine = jnp.cos(angle)
    sine = jnp.sin(angle)
    if values.ndim == 3:
        cosine = cosine[:, None, :]
        sine = sine[:, None, :]
    first = values[..., :half]
    second = values[..., half:]
    return jnp.concatenate(
        [first * cosine - second * sine, second * cosine + first * sine], axis=-1
    )


def short_conv(values, edge, taps):
    span = taps.shape[0]
    length = values.shape[0]
    padded = jnp.concatenate([edge, values], axis=0).astype(jnp.float32)
    result = jnp.zeros(values.shape, jnp.float32)
    for index in range(span):
        result = result + taps[index].astype(jnp.float32)[None, :] * padded[index : index + length]
    return jax.nn.silu(result).astype(jnp.bfloat16)


def local_scan(heads, steps, decays, writes, reads):
    length = decays.shape[-1]
    running = jnp.einsum(
        "grs,ls->grl",
        decays,
        jnp.tril(jnp.ones((length, length), jnp.float32)),
        precision=lax.Precision.HIGHEST,
    )
    causal = jnp.tril(jnp.ones((length, length), dtype=bool))
    spread = jnp.where(causal, running[..., :, None] - running[..., None, :], -jnp.inf)
    inner = jnp.einsum("gln,gsn->gls", reads, writes, preferred_element_type=jnp.float32)
    mixing = inner[:, None] * jnp.exp(spread) * steps[:, :, None, :]
    within = jnp.einsum(
        "grls,grsp->grlp",
        mixing.astype(jnp.bfloat16),
        heads,
        preferred_element_type=jnp.float32,
    )
    to_end = jnp.exp(running[..., -1:] - running) * steps
    weighted = (heads.astype(jnp.float32) * to_end[..., None]).astype(jnp.bfloat16)
    state = jnp.einsum(
        "grsp,gsn->grpn", weighted, writes, preferred_element_type=jnp.float32
    )
    return running, state, within


def exchange(items, plane, name, number, columns=False):
    devices, cores = lax.axis_size("sp"), lax.axis_size("tp")
    planes = devices // plane
    counts = [{"plane": plane, "line": planes, "all": devices}[item[1]] for item in items]
    amount = len(items)
    starts = [sum(counts[:i]) for i in range(amount)]
    shared = any(item[2] for item in items)

    def kernel(*refs):
        ins, outs = refs[:amount], refs[amount : 2 * amount]
        send, recv, pass_send, pass_recv, own = refs[2 * amount :]
        here, core = lax.axis_index("sp"), lax.axis_index("tp")
        across, within = here // plane, here % plane

        def place(reach, step):
            if reach == "plane":
                slot = (within + step + plane) % plane
                return across * plane + slot, slot
            if reach == "line":
                slot = (across + step + planes) % planes
                return slot * plane + within, slot
            up, along = step // plane, step % plane
            if step < 0:
                up, along = -((-step) // plane), -((-step) % plane)
            slot = (across + up + planes) % planes * plane + (within + along + plane) % plane
            return slot, slot

        barrier = pltpu.get_barrier_semaphore()
        greeted = 0
        for reach in ("plane", "line"):
            if not any(item[1] in (reach, "all") for item in items):
                continue
            size = {"plane": plane, "line": planes}[reach]
            for step in range(1, size):
                pl.semaphore_signal(
                    barrier,
                    inc=1,
                    device_id=(place(reach, step)[0], core),
                    device_id_type=pl.DeviceIdType.MESH,
                )
                greeted += 1
        if shared:
            for turn in range(1, cores):
                pl.semaphore_signal(
                    barrier,
                    inc=1,
                    device_id=(here, (core + turn) % cores),
                    device_id_type=pl.DeviceIdType.MESH,
                )
                greeted += 1
        pl.semaphore_wait(barrier, greeted)

        def target(i, slot, who):
            if columns:
                size = ins[i].shape[-1]
                return outs[i].at[:, pl.ds(pl.multiple_of(slot * size, size), size)]
            return outs[i].at[slot, who] if items[i][2] else outs[i].at[slot]

        def sent(i, step):
            goal, goal_slot = place(items[i][1], step)
            mine = place(items[i][1], 0)[1]
            if items[i][1] == "all" and step % plane and step >= plane:
                from_line = place("all", -(step // plane * plane))[1]
                return pltpu.make_async_remote_copy(
                    src_ref=target(i, from_line, core),
                    dst_ref=target(i, from_line, core),
                    send_sem=send.at[starts[i] + step],
                    recv_sem=recv.at[starts[i] + step],
                    device_id=(place("plane", step % plane)[0], core),
                    device_id_type=pl.DeviceIdType.MESH,
                )
            return pltpu.make_async_remote_copy(
                src_ref=ins[i].at[goal_slot] if items[i][3] else ins[i],
                dst_ref=target(i, mine, core),
                send_sem=send.at[starts[i] + step],
                recv_sem=recv.at[starts[i] + step],
                device_id=(goal, core),
                device_id_type=pl.DeviceIdType.MESH,
            )

        def arrived(i, step):
            slot = place(items[i][1], -step)[1]
            return pltpu.make_async_remote_copy(
                src_ref=ins[i].at[slot] if items[i][3] else ins[i],
                dst_ref=target(i, slot, core),
                send_sem=send.at[starts[i] + step],
                recv_sem=recv.at[starts[i] + step],
                device_id=(here, core),
                device_id_type=pl.DeviceIdType.MESH,
            )

        def passed(i, step, turn, outgoing):
            slot = place(items[i][1], -step)[1]
            other = (core + turn) % cores
            owner = core if outgoing else (core - turn + cores) % cores
            return pltpu.make_async_remote_copy(
                src_ref=ins[i] if step == 0 else target(i, slot, core),
                dst_ref=target(i, slot, owner),
                send_sem=pass_send.at[(starts[i] + step) * cores + turn],
                recv_sem=pass_recv.at[(starts[i] + step) * cores + turn],
                device_id=(here, other),
                device_id_type=pl.DeviceIdType.MESH,
            )

        kept = []
        for i in range(amount):
            if items[i][1] == "all":
                for up in range(1, planes):
                    sent(i, up * plane).start()
                for step in range(1, plane):
                    sent(i, step).start()
        for i in range(amount):
            if items[i][1] != "all":
                for step in range(1, counts[i]):
                    sent(i, step).start()
        for i in range(amount):
            slot = place(items[i][1], 0)[1]
            local = pltpu.make_async_copy(
                ins[i].at[slot] if items[i][3] else ins[i], target(i, slot, core), own.at[i]
            )
            local.start()
            kept.append(local)
            if items[i][2]:
                for turn in range(1, cores):
                    passed(i, 0, turn, True).start()
        for i in range(amount):
            if items[i][1] == "all":
                for up in range(1, planes):
                    arrived(i, up * plane).wait_recv()
                    for step in range(up * plane + 1, (up + 1) * plane):
                        sent(i, step).start()
                    for turn in range(1, cores):
                        passed(i, up * plane, turn, True).start()
        for i in range(amount):
            for step in range(1, counts[i]):
                if items[i][1] == "all" and step % plane == 0:
                    continue
                arrived(i, step).wait_recv()
                if items[i][2]:
                    for turn in range(1, cores):
                        passed(i, step, turn, True).start()
        for i in range(amount):
            kept[i].wait()
            for step in range(counts[i]):
                if step > 0:
                    sent(i, step).wait_send()
                if items[i][2]:
                    for turn in range(1, cores):
                        passed(i, step, turn, True).wait_send()
                        passed(i, step, turn, False).wait_recv()

    shapes = []
    for (array, reach, over, selected), count in zip(items, counts):
        lead = (count, cores) if over else (count,)
        tail = array.shape[1:] if selected else array.shape
        if columns:
            lead, tail = (), (tail[0], count * tail[1])
        shapes.append(jax.ShapeDtypeStruct(lead + tail, array.dtype))
    slots = sum(counts)
    return pl.pallas_call(
        kernel,
        out_shape=shapes,
        in_specs=[pl.BlockSpec(memory_space=pltpu.VMEM)] * amount,
        out_specs=[pl.BlockSpec(memory_space=pl.ANY)] * amount,
        scratch_shapes=[
            pltpu.SemaphoreType.DMA((slots,)),
            pltpu.SemaphoreType.DMA((slots,)),
            pltpu.SemaphoreType.DMA((slots * cores,)),
            pltpu.SemaphoreType.DMA((slots * cores,)),
            pltpu.SemaphoreType.DMA((amount,)),
        ],
        compiler_params=pltpu.CompilerParams(
            collective_id=number, has_side_effects=True, vmem_limit_bytes=16 * 1024 * 1024
        ),
        cost_estimate=pl.CostEstimate(
            flops=10**8, bytes_accessed=4 * 2**20, transcendentals=0
        ),
        name=name,
    )(*[item[0] for item in items])


def plain_exchange(items, plane):
    results = []
    for array, reach, over, selected in items:
        value = array
        if over:
            value = lax.all_gather(value, "tp")
        if reach == "plane":
            value = value if selected else value[None]
        else:
            value = lax.all_gather(value, "sp")
        results.append(value)
    return results


def gated_norm(mixed, gate, gain):
    length = mixed.shape[0]
    groups = mixed.shape[1]
    flat = mixed.reshape(length, groups, -1)
    gated = flat * jax.nn.silu(gate.astype(jnp.float32)).reshape(length, groups, -1)
    scaled = gated * lax.rsqrt(jnp.mean(gated * gated, axis=-1, keepdims=True) + eps)
    return (scaled * gain.reshape(groups, -1)[None]).reshape(length, -1).astype(jnp.bfloat16)


def attend(query, cosine, sine, keys, key_up, value_up_weight, length):
    heads = key_up.shape[1] // UNROTATED_WIDTH
    latent_width = key_up.shape[0]
    whole = UNROTATED_WIDTH + ROPE
    half = ROPE // 2
    step = 2 * length if keys.shape[0] % (2 * length) == 0 else length
    scale = whole ** (-0.5)
    contract = (((1,), (1,)), ((), ()))

    def kernel(q_ref, cos_ref, sin_ref, k_ref, ku_ref, vu_ref, out_ref, q_all, top, total, summed):
        start = lax.axis_index("sp") * length
        for h in range(heads):
            base = h * whole
            turn = q_ref[:, base + UNROTATED_WIDTH : base + whole].astype(jnp.float32)
            first, second = turn[:, :half], turn[:, half:]
            turned = jnp.concatenate(
                [
                    first * cos_ref[...] - second * sin_ref[...],
                    second * cos_ref[...] + first * sin_ref[...],
                ],
                axis=1,
            )
            q_all[h] = jnp.concatenate(
                [q_ref[:, base : base + UNROTATED_WIDTH], turned.astype(jnp.bfloat16)], axis=1
            )
        top[...] = jnp.full(top.shape, floor_score, jnp.float32)
        total[...] = jnp.zeros(total.shape, jnp.float32)
        summed[...] = jnp.zeros(summed.shape, jnp.float32)
        row = start + lax.broadcasted_iota(jnp.int32, (length, step), 0)
        column = lax.broadcasted_iota(jnp.int32, (length, step), 1)

        def visit(j, carry):
            at = pl.ds(pl.multiple_of(j * step, step), step)
            latent = k_ref[at, :latent_width]
            turned = k_ref[at, latent_width : latent_width + ROPE]
            seen = column + j * step <= row
            plain = jnp.dot(latent, ku_ref[...], preferred_element_type=jnp.float32).astype(
                jnp.bfloat16
            )
            all_values = jnp.dot(latent, vu_ref[...], preferred_element_type=jnp.float32).astype(
                jnp.bfloat16
            )
            for h in range(heads):
                values = all_values[:, h * VALUE_WIDTH : (h + 1) * VALUE_WIDTH]
                key = jnp.concatenate(
                    [plain[:, h * UNROTATED_WIDTH : (h + 1) * UNROTATED_WIDTH], turned], axis=1
                )
                scores = (
                    lax.dot_general(q_all[h], key, contract, preferred_element_type=jnp.float32)
                    * scale
                )
                scores = jnp.where(seen, scores, -jnp.inf)
                old = top[h][:, :1]
                new = jnp.maximum(old, jnp.max(scores, axis=1, keepdims=True))
                weights = jnp.exp(scores - new)
                shrink = jnp.exp(old - new)
                now = jnp.sum(weights, axis=1, keepdims=True)
                total[h] = total[h] * shrink + now
                summed[h] = summed[h] * shrink + jnp.dot(
                    weights.astype(jnp.bfloat16), values, preferred_element_type=jnp.float32
                )
                top[h] = jnp.broadcast_to(new, top.shape[1:])
            return carry

        lax.fori_loop(0, (start + length + step - 1) // step, visit, 0)
        for h in range(heads):
            out_ref[:, h * VALUE_WIDTH : (h + 1) * VALUE_WIDTH] = (
                summed[h] / total[h][:, :1]
            ).astype(jnp.bfloat16)

    return pl.pallas_call(
        kernel,
        out_shape=jax.ShapeDtypeStruct((length, heads * VALUE_WIDTH), jnp.bfloat16),
        in_specs=[pl.BlockSpec(memory_space=pltpu.VMEM)] * 6,
        out_specs=pl.BlockSpec(memory_space=pltpu.VMEM),
        scratch_shapes=[
            pltpu.VMEM((heads, length, whole), jnp.bfloat16),
            pltpu.VMEM((heads, length, 128), jnp.float32),
            pltpu.VMEM((heads, length, 128), jnp.float32),
            pltpu.VMEM((heads, length, VALUE_WIDTH), jnp.float32),
        ],
        compiler_params=pltpu.CompilerParams(vmem_limit_bytes=40 * 1024 * 1024),
        cost_estimate=pl.CostEstimate(
            flops=4 * 10**10, bytes_accessed=4 * 2**20, transcendentals=0
        ),
        name="attend",
    )(query, cosine, sine, keys, key_up, value_up_weight)


def fused(
    plane,
    tokens,
    mix_gain,
    query_proj,
    compressed_projection,
    compressed_norm_gain,
    rope_proj,
    key_up,
    value_up_weight,
    scan_input,
    scan_gate,
    scan_write,
    scan_read,
    step_proj,
    conv_input,
    conv_write,
    conv_read,
    decay_log,
    decay_offset,
    skip_gain,
    group_gain,
):
    devices, cores = lax.axis_size("sp"), lax.axis_size("tp")
    planes = devices // plane
    part, width = tokens.shape
    length = part * cores
    depth = scan_input.shape[0]
    kblock = depth * plane
    hw, ww = scan_input.shape[1] // plane, scan_write.shape[1] // plane
    lower, wide = hw + 2 * ww, 2 * hw + 2 * ww
    bounds = ((0, lower), (lower, wide))
    own_heads = decay_log.shape[0] // plane
    heads = key_up.shape[1] // UNROTATED_WIDTH
    latent_width = key_up.shape[0]
    key_rows = (latent_width + ROPE) * part // 128
    whole = UNROTATED_WIDTH + ROPE
    half = ROPE // 2
    scale = whole ** (-0.5)
    span = conv_input.shape[0]
    edge = 16
    bf16, f32 = jnp.bfloat16, jnp.float32
    MESH = pl.DeviceIdType.MESH
    last_contract = (((1,), (1,)), ((), ()))
    first_contract = (((0,), (0,)), ((), ()))
    best = lax.Precision.HIGHEST
    group_step = 2

    def mm(a, b):
        return jnp.dot(a, b, preferred_element_type=f32)

    def kernel(
        *refs
    ):
        sources, (att_out, scan_out) = refs[:loaded], refs[loaded : loaded + 2]
        targets = refs[loaded + 2 : 2 * loaded + 2]
        (
            w_in, w_write, w_read, w_gate, tok, mix, comp, comp_gain, rope, freqs, wq, ku, vu,
            doff, w_step, t_in, t_write, t_read, ggain, dlog, skip,
        ) = targets
        (
            load_sem, packed, wbuf, rows, keys, q_all, top, total, summed, stepw, steps, osend,
            obuf, projf, gatef, cbuf, ybuf, runs, before, decayed, state, dsum, ssend, tsend,
            srecv, trecv, incoming, stage, wsend, wrecv, zsend, ksend_up, ksend_plane,
            ksend_core, krecv, rsend, rsend_core, rrecv, rdiag_send,
            rhalf, o_send, o_recv, e_send, e_recv, s_send, s_recv, t_send, t_recv,
            out_send, out_recv,
        ) = refs[2 * loaded + 2 :]
        here, core = lax.axis_index("sp"), lax.axis_index("tp")
        z, n = here // plane, here % plane
        other = cores - 1 - core
        beside, above, across = n + 1 - 2 * (n % 2), (n + 2) % plane, plane - 1 - n
        at_end = (z == 0) | (z == planes - 1)
        nearest = (z + planes - 1) // planes
        farthest = planes - 1 - z

        loads = [
            pltpu.make_async_copy(source, target, load_sem.at[i])
            for i, (source, target) in enumerate(zip(sources, targets))
        ]
        for load in loads:
            load.start()

        def rcopy(src, dst, ss, rs, sp, c):
            return pltpu.make_async_remote_copy(
                src_ref=src, dst_ref=dst, send_sem=ss, recv_sem=rs,
                device_id=(sp, c), device_id_type=MESH,
            )

        def peer(step):
            return z * plane + (n + step) % plane

        barrier = pltpu.get_barrier_semaphore()
        greeted = 0
        for step in range(1, plane):
            pl.semaphore_signal(barrier, inc=1, device_id=(peer(step), core), device_id_type=MESH)
            greeted += 1
        for step in range(1, planes):
            pl.semaphore_signal(
                barrier, inc=1, device_id=((z + step) % planes * plane + n, core),
                device_id_type=MESH,
            )
            greeted += 1
        pl.semaphore_signal(barrier, inc=1, device_id=(here, other), device_id_type=MESH)
        greeted += 1
        for load in loads[:4]:
            load.wait()

        for m in range(plane):
            packed[m, :, :hw] = w_in[:, m * hw : (m + 1) * hw]
            packed[m, :, hw : hw + ww] = w_write[:, m * ww : (m + 1) * ww]
            packed[m, :, hw + ww : lower] = w_read[:, m * ww : (m + 1) * ww]
            packed[m, :, lower:] = w_gate[:, m * hw : (m + 1) * hw]
        wbuf[here] = packed[n]

        pl.semaphore_wait(barrier, greeted)

        def key_slot(sp, c):
            return keys.at[sp * cores + c]

        def key_copy(sp, c, ss, to_sp, to_c):
            return rcopy(
                key_slot(sp, c), key_slot(sp, c), ss, krecv.at[sp * cores + c], to_sp, to_c
            )

        def key_arrived(sp, c):
            key_copy(sp, c, ksend_up.at[0], here, core).wait_recv()

        def key_up_copy(d):
            return key_copy(here, core, ksend_up.at[d], here + d * plane, core)

        sides = (beside, above)

        def key_plane_copy(d, step):
            return key_copy(
                here - d * plane, core, ksend_plane.at[d * plane + step], peer(step), core
            )

        def key_core_copy(sp):
            return key_copy(sp, core, ksend_core.at[sp], here, other)

        sides = (beside, above)

        def chunk(group, index):
            low, high = bounds[group]
            return wbuf.at[index, :, low:high]

        def w_arrived(group, index):
            rcopy(
                chunk(group, index), chunk(group, index), zsend.at[0, group, index],
                wrecv.at[group, index], here, core,
            ).wait_recv()

        def w_plane_copy(group, step):
            low, high = bounds[group]
            goal = (n + step) % plane
            return rcopy(
                packed.at[goal, :, low:high], chunk(group, here), wsend.at[group, step],
                wrecv.at[group, here], z * plane + goal, core,
            )

        def z_copy(group, index, up):
            return rcopy(
                chunk(group, index), chunk(group, index), zsend.at[up, group, index],
                wrecv.at[group, index], here + (plane if up else -plane), core,
            )

        def has_next(up):
            return z + 1 < planes if up else z > 0

        def own_weights(group, steps_of):
            for step in steps_of:
                index = z * plane + (n - step + plane) % plane
                if step:
                    w_arrived(group, index)
                for up in (0, 1):
                    @pl.when(has_next(up))
                    def _():
                        z_copy(group, index, up).start()

        def far_weights(group, d, forward, pieces=range(plane)):
            for up in (0, 1):
                source = z - d if up else z + d
                exists = (source >= 0) & (source < planes)
                gate = has_next(up) if forward else jnp.logical_not(has_next(up))

                @pl.when(exists & gate)
                def _():
                    for step in pieces:
                        index = source * plane + (n - step + plane) % plane
                        w_arrived(group, index)
                        if forward:
                            z_copy(group, index, up).start()

        for step in range(1, plane):
            w_plane_copy(0, step).start()
        own_weights(0, (0,))
        own_weights(1, (0,))

        for load in loads[4:10]:
            load.wait()
        def normed_rows(values, gain, count):
            mean = jnp.sum(values * values, axis=-1, keepdims=True) / count
            return values * lax.rsqrt(mean + eps) * gain

        normed = normed_rows(tok[...].astype(f32), mix[...], width).astype(bf16)

        def rows_at(slot, c):
            return pl.ds(pl.multiple_of(slot * length + c * part, part), part)

        for p in range(planes):
            rows[p, rows_at(n, core), :] = normed[:, p * kblock : (p + 1) * kblock]

        def angles(start, count):
            position = (start + lax.broadcasted_iota(jnp.int32, (count, 1), 0)).astype(f32)
            angle = position * freqs[...]
            return jnp.cos(angle), jnp.sin(angle)

        def turn(first, second, cosine, sine):
            return [first * cosine - second * sine, second * cosine + first * sine]

        latent = normed_rows(mm(normed, comp[...]), comp_gain[...], latent_width)
        small = lax.dot_general(normed, rope[...], last_contract, preferred_element_type=f32)
        cosine, sine = angles(here * length + core * part, part)
        own_slot = here * cores + core
        for low in range(0, latent_width, 128):
            keys[own_slot, low * part // 128 : (low + 128) * part // 128] = latent[
                :, low : low + 128
            ].astype(bf16)
        turned_key = jnp.concatenate(
            turn(small[:, :half], small[:, half:], cosine, sine), axis=1
        ).astype(bf16)
        keys[own_slot, latent_width * part // 128 :] = jnp.concatenate(
            [turned_key[: part // 2], turned_key[part // 2 :]], axis=1
        )

        for d in range(1, planes):
            @pl.when(z + d < planes)
            def _():
                key_up_copy(d).start()
        key_core_copy(here).start()

        def row_copy(slot, ss, to_sp, to_c):
            at = rows.at[:, rows_at(slot, core), :]
            return rcopy(at, at, ss, rrecv.at[slot * cores + core], to_sp, to_c)

        def row_part(slot, part_of, ss, rs, to_sp):
            low, high = part_of * planes // 2, (part_of + 1) * planes // 2
            at = rows.at[low:high, rows_at(slot, core), :]
            return rcopy(at, at, ss, rs, to_sp, core)

        def row_plane_copy(side, part_of):
            return row_part(
                n, part_of, rsend.at[side, part_of], rhalf.at[n, part_of],
                z * plane + sides[side],
            )

        def row_half_arrived(slot, part_of):
            row_part(
                slot, part_of, rsend.at[0, 0], rhalf.at[slot, part_of], here
            ).wait_recv()

        def row_relay(side):
            slot = sides[side]
            return row_part(
                slot, side, rdiag_send.at[side], rhalf.at[slot, side],
                z * plane + sides[1 - side],
            )

        def row_core_copy(slot):
            return row_copy(slot, rsend_core.at[slot], here, other)

        def row_arrived(slot, c):
            at = rows.at[:, rows_at(slot, c), :]
            rcopy(at, at, rsend.at[0], rrecv.at[slot * cores + c], here, core).wait_recv()

        def offset_copy(step):
            goal = (n + step) % plane
            return rcopy(
                osend.at[goal], obuf.at[n], o_send.at[step], o_recv.at[n],
                z * plane + goal, core,
            )

        row_core_copy(n).start()

        positions = plane * length
        at_edge = rows.at[:, positions : positions + edge, :]
        closing = (n == plane - 1) & (core == cores - 1)

        def edge_up_copy():
            return rcopy(
                rows.at[:, positions - edge : positions, :], at_edge, e_send.at[0], e_recv,
                here + plane, core,
            )

        def edge_plane_copy(step):
            return rcopy(at_edge, at_edge, e_send.at[step], e_recv, peer(step), core)

        def edge_core_copy():
            return rcopy(at_edge, at_edge, e_send.at[plane], e_recv, here, other)

        def edge_arrived():
            rcopy(at_edge, at_edge, e_send.at[0], e_recv, here, core).wait_recv()

        @pl.when(closing & (z + 1 < planes))
        def _():
            edge_up_copy().start()

        for load in loads[10:]:
            load.wait()
        for m in range(plane):
            osend[m, :own_heads] = doff[m * own_heads : (m + 1) * own_heads]
        obuf[n] = osend[n]

        @pl.when(z == 0)
        def _():
            rows[:, plane * length :, :] = jnp.zeros((planes, edge, kblock), bf16)

        row_arrived(n, other)
        own_rows = pl.ds(pl.multiple_of(n * length, length), length)
        query = mm(rows[0, own_rows, :], wq[:kblock, :])
        for p in range(1, planes):
            query += mm(rows[p, own_rows, :], wq[p * kblock : (p + 1) * kblock, :])
        query = query.astype(bf16)
        cosine, sine = angles(here * length, length)
        for h in range(heads):
            base = h * whole
            rope_part = query[:, base + UNROTATED_WIDTH : base + whole].astype(f32)
            q_all[h] = jnp.concatenate(
                [query[:, base : base + UNROTATED_WIDTH]]
                + [
                    v.astype(bf16)
                    for v in turn(rope_part[:, :half], rope_part[:, half:], cosine, sine)
                ],
                axis=1,
            )
        top[...] = jnp.full(top.shape, floor_score, f32)
        total[...] = jnp.zeros(total.shape, f32)
        summed[...] = jnp.zeros(summed.shape, f32)

        own_weights(0, range(1, plane))
        for step in range(1, plane):
            key_plane_copy(0, step).start()
        for d in range(1, planes):
            @pl.when(z >= d)
            def _():
                key_arrived(here - d * plane, core)
                for step in range(1, plane):
                    key_plane_copy(d, step).start()
                key_core_copy(here - d * plane).start()

        @pl.when(closing & (z > 0))
        def _():
            edge_arrived()
            for step in range(1, plane):
                edge_plane_copy(step).start()
            edge_core_copy().start()

        for step in range(1, plane):
            w_plane_copy(1, step).start()
        for first in (0, 1):
            for side in (0, 1):
                row_plane_copy(side, (side + first) % 2).start()
        for step in range(1, plane):
            offset_copy(step).start()

        def pass_keys(d):
            for step in range(1, plane):
                sp = (z - d) * plane + (n + step) % plane
                key_arrived(sp, core)
                key_core_copy(sp).start()

        def other_keys(d):
            for q in range(plane):
                key_arrived((z - d) * plane + q, other)

        size = group_step * length
        row = lax.broadcasted_iota(jnp.int32, (length, size), 0)
        column = lax.broadcasted_iota(jnp.int32, (length, size), 1)

        def visit(first_block, limit):
            count = group_step * cores
            block = keys[pl.ds(first_block * cores, count)]
            lat = jnp.concatenate(
                [
                    block[:, low * part // 128 : (low + 128) * part // 128].reshape(size, 128)
                    for low in range(0, latent_width, 128)
                ],
                axis=1,
            )
            turned = block[:, latent_width * part // 128 :]
            turned = jnp.concatenate([turned[:, :, :ROPE], turned[:, :, ROPE:]], axis=1)
            turned = turned.reshape(size, ROPE)
            plain = mm(lat, ku[...]).astype(bf16)
            all_values = mm(lat, vu[...]).astype(bf16)
            if limit is not None:
                seen = column <= row + limit
            for h in range(heads):
                values = all_values[:, h * VALUE_WIDTH : (h + 1) * VALUE_WIDTH]
                key = jnp.concatenate(
                    [plain[:, h * UNROTATED_WIDTH : (h + 1) * UNROTATED_WIDTH], turned], axis=1
                )
                scores = (
                    lax.dot_general(q_all[h], key, last_contract, preferred_element_type=f32)
                    * scale
                )
                if limit is not None:
                    scores = jnp.where(seen, scores, -jnp.inf)
                old = top[h][:, :1]
                new = jnp.maximum(old, jnp.max(scores, axis=1, keepdims=True))
                weights = jnp.exp(scores - new)
                shrink = jnp.exp(old - new)
                now = jnp.sum(weights, axis=1, keepdims=True)
                total[h] = total[h] * shrink + now
                summed[h] = summed[h] * shrink + mm(weights.astype(bf16), values)
                top[h] = jnp.broadcast_to(new, top.shape[1:])

        pass_keys(0)

        @pl.when(z >= 1)
        def _():
            pass_keys(1)

        far_weights(0, 1, True)
        other_keys(0)

        def near(j, carry):
            visit(z * plane + j * group_step, (n - j * group_step) * length)
            return carry

        lax.fori_loop(0, n // group_step + 1, near, 0)

        late = min(2, planes - 1)

        def further(d, carry):
            @pl.when(z > d)
            def _():
                pass_keys(d + 1)

            @pl.when(d == late)
            def _():
                own_weights(1, range(1, plane))

            @pl.when(z >= d)
            def _():
                other_keys(d)

                def inner(j, carry):
                    visit((z - d) * plane + j * group_step, None)
                    return carry

                lax.fori_loop(0, plane // group_step, inner, 0)

            return carry

        lax.fori_loop(1, planes, further, 0)
        for h in range(heads):
            att_out[:, h * VALUE_WIDTH : (h + 1) * VALUE_WIDTH] = (
                summed[h] / total[h][:, :1]
            ).astype(bf16)

        @pl.when((z > 0) & (core == cores - 1) & (n < plane - 1))
        def _():
            edge_arrived()
            edge_core_copy().start()

        for side in (0, 1):
            row_half_arrived(sides[side], side)
            row_relay(side).start()
        for side in (0, 1):
            row_half_arrived(sides[side], 1 - side)
            row_core_copy(sides[side]).start()
        for d in range(2, planes - 1):
            far_weights(0, d, True)
        far_weights(1, 1, True)
        for d in range(1, planes - 1):
            far_weights(0, d, False)

        def tile(k):
            return pl.ds(pl.multiple_of(k * length, length), length)

        def project(p, values, group):
            low, high = bounds[group]
            block = wbuf[pl.ds(p * plane, plane), :, low:high]
            return mm(values, block.reshape(kblock, high - low))

        def sum_near(group, at, store):
            @pl.when(at_end)
            def _():
                out = project(nearest, rows[nearest, at, :], group)
                for p in range(1, planes - 1):
                    out += project(nearest + p, rows[nearest + p, at, :], group)
                store(out, False)

            @pl.when(jnp.logical_not(at_end))
            def _():
                out = project(0, rows[0, at, :], group)
                for p in range(1, planes):
                    out += project(p, rows[p, at, :], group)
                store(out, False)

        def sum_far(group, at, store):
            store(project(farthest, rows[farthest, at, :], group), True)

        def into(low, count):
            def store(out, add):
                at = pl.ds(low, count)
                projf[at, :] = projf[at, :] + out if add else out

            return store

        def edge_sum(method):
            method(0, pl.ds(positions, edge), into(0, edge))

        def tile_sum(method, k):
            method(0, tile(k), into(pl.multiple_of(k * length + edge, edge), length))

        lane = lax.broadcasted_iota(jnp.int32, (128, w_step.shape[0]), 0)
        which = lax.broadcasted_iota(jnp.int32, (128, w_step.shape[0]), 1)
        first_head = (core * plane + n) * own_heads
        chosen = ((which == lane + first_head) & (lane < own_heads)).astype(bf16)
        stepw[...] = mm(chosen, w_step[...]).astype(bf16)

        def step_tile(k):
            raw = jnp.zeros((length, 128), f32)
            for p in range(planes):
                raw += lax.dot_general(
                    rows[p, tile(k), :], stepw[:, p * kblock : (p + 1) * kblock],
                    last_contract, preferred_element_type=f32,
                )
            steps[k] = jnp.maximum(raw, 0.0) + jnp.log1p(jnp.exp(-jnp.abs(raw)))

        @pl.when((z > 0) & (core < cores - 1))
        def _():
            edge_arrived()

        edge_sum(sum_near)

        def turned_slot(flip):
            return (n // 2 + flip // 2) % 2 * 2 + (n + flip) % 2

        def first_sums(flip, carry):
            slot = turned_slot(flip)

            @pl.when(flip == plane - 1)
            def _():
                for part_of in (0, 1):
                    row_half_arrived(across, part_of)
                row_core_copy(across).start()

            @pl.when(flip > 0)
            def _():
                row_arrived(slot, other)

            tile_sum(sum_near, slot)
            step_tile(slot)
            return carry

        lax.fori_loop(0, plane, first_sums, 0)
        far_weights(0, planes - 1, False)

        @pl.when(at_end)
        def _():
            edge_sum(sum_far)

            def last_sums(k, carry):
                tile_sum(sum_far, k)
                return carry

            lax.fori_loop(0, plane, last_sums, 0)

        for d in range(2, planes - 1):
            far_weights(1, d, True, range(plane - 1))

        taps = jnp.concatenate(
            [
                t_in[:, pl.ds(pl.multiple_of(n * hw, hw), hw)],
                t_write[:, pl.ds(pl.multiple_of(n * ww, ww), ww)],
                t_read[:, pl.ds(pl.multiple_of(n * ww, ww), ww)],
            ],
            axis=1,
        ).astype(f32)

        def conv_tile(k, carry):
            base = pl.ds(pl.multiple_of(k * length, length), length + edge)
            for low in range(0, lower, 128):
                at = slice(low, low + 128)
                values = projf[base, at].astype(bf16).astype(f32)
                result = jnp.zeros((length, 128), f32)
                for i in range(span):
                    shift = edge - span + 1 + i
                    result = result + taps[i : i + 1, at] * values[shift : shift + length]
                cbuf[tile(k), at] = (result * jax.nn.sigmoid(result)).astype(bf16)
            return carry

        lax.fori_loop(0, plane, conv_tile, 0)

        for step in range(1, plane):
            slot = (n - step + plane) % plane
            rcopy(
                obuf.at[slot], obuf.at[slot], o_send.at[0], o_recv.at[slot], here, core
            ).wait_recv()
        lane_row = lax.broadcasted_iota(jnp.int32, (1, 128), 1)
        rate = jnp.zeros((1, 128), f32)
        for h in range(own_heads):
            rate = jnp.where(lane_row == h, dlog[n * own_heads + h], rate)
        rate = -jnp.exp(rate)
        causal = lax.broadcasted_iota(jnp.int32, (length, length), 0) >= lax.broadcasted_iota(
            jnp.int32, (length, length), 1
        )
        tri = causal.astype(f32)

        def per_lane(columns):
            return jnp.concatenate(
                [
                    jnp.broadcast_to(columns[:, h : h + 1], (columns.shape[0], SSM_DIM))
                    for h in range(own_heads)
                ],
                axis=1,
            )

        def per_row(values):
            return jnp.concatenate(
                [
                    jnp.broadcast_to(values[:, h : h + 1], (SSM_DIM, SSM_STATE))
                    for h in range(own_heads)
                ],
                axis=0,
            )

        state[...] = jnp.zeros(state.shape, f32)
        dsum[...] = jnp.zeros(dsum.shape, f32)

        def scan_tile(k, carry):
            step_col = steps[k]
            off_col = jnp.concatenate(
                [obuf[k], jnp.zeros((128 - obuf.shape[1], length), f32)], axis=0
            ).T
            decay = jnp.where(lane_row < own_heads, rate * step_col + off_col, 0.0)
            running = jnp.dot(tri, decay, precision=best, preferred_element_type=f32)
            runs[k] = running
            run_row, step_row = running.T, step_col.T
            x = cbuf[tile(k), :hw]
            w = cbuf[tile(k), hw : hw + ww]
            r = cbuf[tile(k), hw + ww : lower]
            inner = lax.dot_general(r, w, last_contract, preferred_element_type=f32)
            for h in range(own_heads):
                at = slice(h * SSM_DIM, (h + 1) * SSM_DIM)
                spread = jnp.where(
                    causal, running[:, h : h + 1] - run_row[h : h + 1, :], -jnp.inf
                )
                mixing = inner * jnp.exp(spread) * step_row[h : h + 1, :]
                ybuf[tile(k), at] = (
                    mm(mixing.astype(bf16), x[:, at])
                    + skip[n * own_heads + h] * x[:, at].astype(f32)
                )
            last = running[length - 1 : length, :]
            to_end = jnp.exp(last - running) * step_col
            weighted = (x.astype(f32) * per_lane(to_end)).astype(bf16)
            update = lax.dot_general(weighted, w, first_contract, preferred_element_type=f32)
            before[k] = state[...]
            decayed[k] = dsum[...]
            state[...] = per_row(jnp.exp(last)) * state[...] + update
            dsum[...] = dsum[...] + last
            return carry

        lax.fori_loop(0, plane, scan_tile, 0)

        def state_arrived(p):
            rcopy(ssend, srecv.at[p], s_send.at[0], s_recv.at[p], here, core).wait_recv()
            rcopy(tsend, trecv.at[p], t_send.at[0], t_recv.at[p], here, core).wait_recv()

        def state_copies(d):
            to = here + d * plane
            return (
                rcopy(ssend, srecv.at[z], s_send.at[d], s_recv.at[z], to, core),
                rcopy(tsend, trecv.at[z], t_send.at[d], t_recv.at[z], to, core),
            )

        def to_send(d):
            return (z + d < planes) & ((z == 0) | (d == 1))

        @pl.when((z > 1) & (z + 1 < planes))
        def _():
            state_arrived(z - 1)
            ssend[...] = (
                per_row(jnp.exp(dsum[:1])) * srecv[z - 1].astype(f32) + state[...]
            ).astype(bf16)
            tsend[...] = dsum[...] + trecv[z - 1]

        @pl.when(z <= 1)
        def _():
            ssend[...] = state[...].astype(bf16)
            tsend[...] = dsum[...]

        for d in range(1, planes):
            @pl.when(to_send(d))
            def _():
                for copy in state_copies(d):
                    copy.start()

        for d in range(2, planes - 1):
            far_weights(1, d, True, range(plane - 1, plane))
        for d in range(1, planes - 1):
            far_weights(1, d, False)

        def gate_tile(k, carry):
            def store(out, add):
                gatef[tile(k), :] = out

            sum_near(1, tile(k), store)
            return carry

        lax.fori_loop(0, plane, gate_tile, 0)
        @pl.when((z > 1) & (z + 1 == planes))
        def _():
            state_arrived(z - 1)

        @pl.when(z > 0)
        def _():
            state_arrived(0)

        @pl.when(z == 1)
        def _():
            incoming[...] = srecv[0].astype(f32)

        @pl.when(z > 1)
        def _():
            incoming[...] = (
                per_row(jnp.exp(trecv[z - 1][:1])) * srecv[0].astype(f32)
                + srecv[z - 1].astype(f32)
            )

        def carry_tile(k, carry):
            entered = (
                before[k] + per_row(jnp.exp(decayed[k][:1])) * incoming[...]
            ).astype(bf16)
            carried = lax.dot_general(
                cbuf[tile(k), hw + ww : lower], entered, last_contract,
                preferred_element_type=f32,
            )
            ybuf[tile(k), :] = ybuf[tile(k), :] + carried * per_lane(jnp.exp(runs[k]))
            return carry

        @pl.when(z == 0)
        def _():
            incoming[...] = jnp.zeros(incoming.shape, f32)

        lax.fori_loop(0, plane, carry_tile, 0)
        far_weights(1, planes - 1, False)
        own_columns = pl.ds(pl.multiple_of(n * hw, hw), hw)
        gain = ggain[:, own_columns]

        def out_copy(k):
            return rcopy(
                stage.at[k], scan_out.at[:, own_columns], out_send.at[k], out_recv.at[n],
                z * plane + k, core,
            )

        def finish(i, carry):
            k = turned_slot(plane - 1 - i)

            @pl.when(at_end)
            def _():
                def store(out, add):
                    gatef[tile(k), :] = gatef[tile(k), :] + out

                sum_far(1, tile(k), store)

            gate = gatef[tile(k), :].astype(bf16).astype(f32)
            mixed = ybuf[tile(k), :]
            gated = mixed * (gate * jax.nn.sigmoid(gate))
            out = normed_rows(gated, gain, hw).astype(bf16)
            stage[k] = out

            @pl.when(k != n)
            def _():
                out_copy(k).start()

            @pl.when(k == n)
            def _():
                scan_out[:, own_columns] = out

            return carry

        lax.fori_loop(0, plane, finish, 0)
        for step in range(1, plane):
            slot = (n + step) % plane
            at = scan_out.at[:, pl.ds(pl.multiple_of(slot * hw, hw), hw)]
            rcopy(stage.at[0], at, out_send.at[0], out_recv.at[slot], here, core).wait_recv()

        for d in range(1, planes):
            @pl.when(z + d < planes)
            def _():
                key_up_copy(d).wait_send()

            @pl.when(to_send(d))
            def _():
                for copy in state_copies(d):
                    copy.wait_send()

        for d in range(planes):
            @pl.when(z >= d)
            def _():
                for step in range(1, plane):
                    key_plane_copy(d, step).wait_send()
                for q in range(plane):
                    key_core_copy((z - d) * plane + q).wait_send()
        for step in range(1, plane):
            for group in (0, 1):
                w_plane_copy(group, step).wait_send()
            offset_copy(step).wait_send()
            out_copy((n + step) % plane).wait_send()
        for side in (0, 1):
            for part_of in (0, 1):
                row_plane_copy(side, part_of).wait_send()
            row_relay(side).wait_send()
        for slot in range(plane):
            row_core_copy(slot).wait_send()

        @pl.when(closing & (z + 1 < planes))
        def _():
            edge_up_copy().wait_send()

        @pl.when(closing & (z > 0))
        def _():
            for step in range(1, plane):
                edge_plane_copy(step).wait_send()

        @pl.when((z > 0) & (core == cores - 1))
        def _():
            edge_core_copy().wait_send()

        for up in (0, 1):
            for p in range(planes):
                @pl.when(((p <= z) if up else (p >= z)) & has_next(up))
                def _():
                    for q in range(plane):
                        for group in (0, 1):
                            z_copy(group, p * plane + q, up).wait_send()

    vmem = pl.BlockSpec(memory_space=pltpu.VMEM)
    hbm = pl.BlockSpec(memory_space=pltpu.HBM)
    freqs = np.float32(theta) ** (-np.arange(half, dtype=np.float32) * np.float32(2.0 / ROPE))
    inputs = (
        scan_input,
        scan_write,
        scan_read,
        scan_gate,
        tokens,
        mix_gain[None, :],
        compressed_projection,
        compressed_norm_gain[None, :],
        rope_proj.T,
        jnp.asarray(freqs[None, :], f32),
        query_proj,
        key_up,
        value_up_weight,
        decay_offset.T,
        step_proj.T,
        conv_input,
        conv_write,
        conv_read,
        group_gain[None, :],
        decay_log,
        skip_gain,
    )
    loaded = len(inputs)
    dma = pltpu.SemaphoreType.DMA
    positions = plane * length
    results = (
        jax.ShapeDtypeStruct((length, heads * VALUE_WIDTH), bf16),
        jax.ShapeDtypeStruct((length, scan_input.shape[1]), bf16),
    )
    outs = pl.pallas_call(
        kernel,
        out_shape=results,
        in_specs=[hbm] * loaded,
        out_specs=(vmem, vmem),
        scratch_shapes=[pltpu.VMEM(value.shape, value.dtype) for value in inputs[:-2]]
        + [pltpu.SMEM(value.shape, value.dtype) for value in inputs[-2:]]
        + [
            dma((loaded,)),
            pltpu.VMEM((plane, depth, wide), bf16),
            pltpu.VMEM((devices, depth, wide), bf16),
            pltpu.VMEM((planes, positions + edge, kblock), bf16),
            pltpu.VMEM((devices * cores, key_rows, 128), bf16),
            pltpu.VMEM((heads, length, whole), bf16),
            pltpu.VMEM((heads, length, 128), f32),
            pltpu.VMEM((heads, length, 128), f32),
            pltpu.VMEM((heads, length, VALUE_WIDTH), f32),
            pltpu.VMEM((128, width), bf16),
            pltpu.VMEM((plane, length, 128), f32),
            pltpu.VMEM((plane, 8, length), f32),
            pltpu.VMEM((plane, 8, length), f32),
            pltpu.VMEM((edge + positions, lower), f32),
            pltpu.VMEM((positions, hw), f32),
            pltpu.VMEM((positions, lower), bf16),
            pltpu.VMEM((positions, hw), f32),
            pltpu.VMEM((plane, length, 128), f32),
            pltpu.VMEM((plane, own_heads * SSM_DIM, SSM_STATE), f32),
            pltpu.VMEM((plane, 8, 128), f32),
            pltpu.VMEM((own_heads * SSM_DIM, SSM_STATE), f32),
            pltpu.VMEM((8, 128), f32),
            pltpu.VMEM((own_heads * SSM_DIM, SSM_STATE), bf16),
            pltpu.VMEM((8, 128), f32),
            pltpu.VMEM((planes, own_heads * SSM_DIM, SSM_STATE), bf16),
            pltpu.VMEM((planes, 8, 128), f32),
            pltpu.VMEM((own_heads * SSM_DIM, SSM_STATE), f32),
            pltpu.VMEM((plane, length, hw), bf16),
            dma((2, plane)),
            dma((2, devices)),
            dma((2, 2, devices)),
            dma((planes,)),
            dma((devices,)),
            dma((devices,)),
            dma((devices * cores,)),
            dma((2, 2)),
            dma((plane,)),
            dma((plane * cores,)),
            dma((2,)),
            dma((plane, 2)),
            dma((plane,)),
            dma((plane,)),
            dma((plane + 1,)),
            dma,
            dma((planes,)),
            dma((planes,)),
            dma((planes,)),
            dma((planes,)),
            dma((plane,)),
            dma((plane,)),
        ],
        compiler_params=pltpu.CompilerParams(
            collective_id=1, has_side_effects=True, vmem_limit_bytes=48 * 1024 * 1024
        ),
        name="fused",
    )(*[pltpu.with_memory_space_constraint(value, pltpu.HBM) for value in inputs])

    def settle(a_in, b_in, a_out, b_out, sems):
        copies = [
            pltpu.make_async_copy(a_in, a_out, sems.at[0]),
            pltpu.make_async_copy(b_in, b_out, sems.at[1]),
        ]
        for copy in copies:
            copy.start()
        for copy in copies:
            copy.wait()

    return pl.pallas_call(
        settle,
        out_shape=results,
        in_specs=[vmem, vmem],
        out_specs=(hbm, hbm),
        scratch_shapes=[dma((2,))],
        compiler_params=pltpu.CompilerParams(vmem_limit_bytes=4 * 1024 * 1024),
        name="settle",
    )(*outs)


def shards(
    tokens,
    mix_gain,
    query_proj,
    compressed_projection,
    compressed_norm_gain,
    rope_proj,
    key_up,
    value_up_weight,
    scan_input,
    scan_gate,
    scan_write,
    scan_read,
    step_proj,
    conv_input,
    conv_write,
    conv_read,
    decay_log,
    decay_offset,
    skip_gain,
    group_gain,
):
    groups = scan_write.shape[1] // SSM_STATE
    devices, cores = lax.axis_size("sp"), lax.axis_size("tp")
    plane = groups if devices % groups == 0 else 1
    planes = devices // plane
    sp_index, core = lax.axis_index("sp"), lax.axis_index("tp")
    across, within = sp_index // plane, sp_index % plane
    own_groups = groups // plane
    direct = plane > 1
    if direct and cores == 2 and own_groups == 1 and plane == 4 and planes > 1:
        return fused(
            plane,
            tokens,
            mix_gain,
            query_proj,
            compressed_projection,
            compressed_norm_gain,
            rope_proj,
            key_up,
            value_up_weight,
            scan_input,
            scan_gate,
            scan_write,
            scan_read,
            step_proj,
            conv_input,
            conv_write,
            conv_read,
            decay_log,
            decay_offset,
            skip_gain,
            group_gain,
        )

    def move(items, name, number, columns=False):
        if direct:
            return exchange(items, plane, name, number, columns)
        return plain_exchange(items, plane)

    depth = scan_input.shape[0]
    widths = [w.shape[1] // plane for w in (scan_input, scan_gate, scan_write, scan_read)]
    offsets = [sum(widths[:i]) for i in range(4)]
    packed = jnp.stack(
        [
            jnp.concatenate(
                [
                    w[:, n * size : (n + 1) * size]
                    for w, size in zip((scan_input, scan_gate, scan_write, scan_read), widths)
                ],
                axis=1,
            )
            for n in range(plane)
        ]
    )
    (part_weights,) = move([(packed, "plane", False, True)], "weights_in_plane", 1)
    weights = lax.all_gather(
        part_weights.reshape(plane * depth, -1),
        "sp",
        axis=0,
        tiled=True,
        axis_index_groups=[[p * plane + n for p in range(planes)] for n in range(plane)],
    )

    own_normed = rms_scale(tokens, mix_gain).astype(jnp.bfloat16)
    part = tokens.shape[0]
    length = part * cores
    latent_width = compressed_projection.shape[1]
    small = jnp.dot(
        own_normed,
        jnp.concatenate([compressed_projection, rope_proj], axis=1),
        preferred_element_type=jnp.float32,
    )
    latent = rms_scale(small[:, :latent_width], compressed_norm_gain).astype(jnp.bfloat16)
    part_positions = sp_index * length + core * part + jnp.arange(part, dtype=jnp.int32)
    key_turned = rotate(small[:, latent_width:], part_positions).astype(jnp.bfloat16)
    padding = jnp.zeros((part, -(latent_width + ROPE) % 128), jnp.bfloat16)
    own_keys = jnp.concatenate([latent, key_turned, padding], axis=1)
    all_keys, all_rows, offsets_seen = move(
        [
            (own_keys, "all", True, False),
            (own_normed, "plane", True, False),
            (decay_offset.T, "plane", False, False),
        ],
        "rows_and_keys",
        2,
    )
    all_keys = all_keys.reshape(devices * length, -1)
    all_rows = all_rows.reshape(plane * length, -1)
    edge_rows = from_behind(all_rows[plane * length - 8 :], "sp", plane)
    positions = sp_index * length + jnp.arange(length, dtype=jnp.int32)
    rows = lax.dynamic_slice_in_dim(all_rows, within * length, length, 0)
    query = jnp.dot(rows, query_proj, preferred_element_type=jnp.float32).astype(jnp.bfloat16)
    half = ROPE // 2
    freqs = theta ** (-jnp.arange(half, dtype=jnp.float32) * 2.0 / ROPE)
    angle = positions.astype(jnp.float32)[:, None] * freqs[None, :]
    attended = attend(
        query, jnp.cos(angle), jnp.sin(angle), all_keys, key_up, value_up_weight, length
    )

    def own_part(array, axis, size):
        return lax.dynamic_slice_in_dim(array, within * size, size, axis)

    local_heads = decay_log.shape[0]
    own_heads = local_heads // plane
    per_group = local_heads // groups
    step_raw = jnp.dot(
        all_rows,
        lax.dynamic_slice_in_dim(
            step_proj, core * local_heads + within * own_heads, own_heads, 1
        ),
        preferred_element_type=jnp.float32,
    )
    step_size = jax.nn.softplus(step_raw)
    own_offset = own_part(offsets_seen, 1, own_heads)
    step_values = jnp.transpose(step_size.reshape(plane, length, own_heads), (0, 2, 1))
    decay_values = (
        -jnp.exp(own_part(decay_log, 0, own_heads))[None, :, None] * step_values + own_offset
    )

    projected = jnp.dot(all_rows, weights, preferred_element_type=jnp.float32).astype(jnp.bfloat16)
    edge = jnp.dot(edge_rows, weights, preferred_element_type=jnp.float32).astype(jnp.bfloat16)
    span = conv_input.shape[0] - 1

    def convolved(i, taps):
        at = slice(offsets[i], offsets[i] + widths[i])
        return short_conv(projected[:, at], edge[8 - span :, at], own_part(taps, 1, widths[i]))

    head_conv = convolved(0, conv_input)
    gate = projected[:, offsets[1] : offsets[1] + widths[1]]
    writes = convolved(2, conv_write)
    reads = convolved(3, conv_read)
    blocks = plane * own_groups

    def by_block(values, last):
        split = values.reshape(plane, length, own_groups, last)
        return jnp.transpose(split, (0, 2, 1, 3)).reshape(blocks, length, last)

    head_values = jnp.transpose(
        head_conv.reshape(plane, length, own_groups, per_group, SSM_DIM), (0, 2, 3, 1, 4)
    ).reshape(blocks, per_group, length, SSM_DIM)
    write_values = by_block(writes, SSM_STATE)
    read_values = by_block(reads, SSM_STATE)
    running, state, mixed = local_scan(
        head_values,
        step_values.reshape(blocks, per_group, length),
        decay_values.reshape(blocks, per_group, length),
        write_values,
        read_values,
    )
    states = state.reshape(plane, own_heads, SSM_DIM, SSM_STATE)
    totals = running[..., -1].reshape(plane, own_heads)
    before, decayed = [jnp.zeros_like(states[0])], [jnp.zeros_like(totals[0])]
    for index in range(plane):
        before.append(jnp.exp(totals[index])[:, None, None] * before[-1] + states[index])
        decayed.append(totals[index] + decayed[-1])
    sent_total = jnp.pad(decayed[-1][None, :], ((0, 7), (0, 128 - own_heads)))
    seen_states, seen_totals = move(
        [
            (before[-1].reshape(-1, SSM_STATE).astype(jnp.bfloat16), "line", False, False),
            (sent_total, "line", False, False),
        ],
        "states",
        3,
    )
    seen_states = seen_states.reshape(planes, own_heads, SSM_DIM, SSM_STATE).astype(jnp.float32)
    seen_totals = seen_totals[:, 0, :own_heads]
    index = jnp.arange(planes)
    between = (index[None, :] > index[:, None]) & (index[None, :] < across)
    path = jnp.sum(jnp.where(between[:, :, None], seen_totals[None], 0.0), axis=1)
    reached = (index < across)[:, None]
    factor = jnp.where(reached, jnp.exp(path), 0.0)
    incoming = jnp.sum(seen_states * factor[:, :, None, None], axis=0)
    entered = jnp.stack(
        [
            before[k] + jnp.exp(decayed[k])[:, None, None] * incoming
            for k in range(plane)
        ]
    ).reshape(blocks, per_group, SSM_DIM, SSM_STATE)
    carried = jnp.einsum(
        "gln,grpn->grlp",
        read_values,
        entered.astype(jnp.bfloat16),
        preferred_element_type=jnp.float32,
    )
    skip = jnp.broadcast_to(
        own_part(skip_gain, 0, own_heads).reshape(1, own_groups, per_group),
        (plane, own_groups, per_group),
    ).reshape(blocks, per_group, 1, 1)
    mixed = (
        mixed
        + carried * jnp.exp(running)[..., None]
        + skip * head_values.astype(jnp.float32)
    )
    mixed = jnp.transpose(
        mixed.reshape(plane, own_groups, per_group, length, SSM_DIM), (0, 3, 1, 2, 4)
    ).reshape(plane * length, own_groups, per_group, SSM_DIM)
    scanned = gated_norm(mixed, gate, own_part(group_gain, 0, widths[0]))
    (columns,) = move(
        [(scanned.reshape(plane, length, -1), "plane", False, True)], "outputs_in_plane", 4, True
    )
    scanned = columns.reshape(length, -1)
    return (attended, scanned)


def solution(mesh):
    in_specs = (
        P(("sp", "tp"), None),
        P(),
        P(None, "tp"),
        P(),
        P(),
        P(),
        P(None, "tp"),
        P(None, "tp"),
        P("sp", "tp"),
        P("sp", "tp"),
        P("sp", "tp"),
        P("sp", "tp"),
        P(),
        P(None, "tp"),
        P(None, "tp"),
        P(None, "tp"),
        P("tp"),
        P("sp", "tp"),
        P("tp"),
        P("tp"),
    )
    out_specs = (P("sp", "tp"), P("sp", "tp"))
    return jax.shard_map(shards, mesh=mesh, in_specs=in_specs, out_specs=out_specs, check_vma=False)
```

```python
import jax
import jax.numpy as jnp
import numpy as np
from jax import lax
from jax.experimental import pallas as pl
from jax.experimental.pallas import tpu as pltpu
from jax.sharding import PartitionSpec as P

UNROTATED_WIDTH = 128
ROPE = 64
VALUE_WIDTH = 128
SSM_DIM = 64
SSM_STATE = 128


eps = 1e-06
theta = 10000.0
floor_score = -1e30


def from_behind(value, axis, steps):
    count = lax.axis_size(axis)
    initial, last = (max(0, -steps), min(count, count - steps))
    return lax.ppermute(value, axis, [(source, source + steps) for source in range(initial, last)])


def rms_scale(values, gain):
    wide = values.astype(jnp.float32)
    return wide * lax.rsqrt(jnp.mean(wide * wide, axis=-1, keepdims=True) + eps) * gain


def rotate(values, positions):
    half = values.shape[-1] // 2
    freqs = theta ** (-jnp.arange(half, dtype=jnp.float32) * 2.0 / values.shape[-1])
    angle = positions.astype(jnp.float32)[:, None] * freqs[None, :]
    cosine = jnp.cos(angle)
    sine = jnp.sin(angle)
    if values.ndim == 3:
        cosine = cosine[:, None, :]
        sine = sine[:, None, :]
    first = values[..., :half]
    second = values[..., half:]
    return jnp.concatenate(
        [first * cosine - second * sine, second * cosine + first * sine], axis=-1
    )


def short_conv(values, edge, taps):
    span = taps.shape[0]
    length = values.shape[0]
    padded = jnp.concatenate([edge, values], axis=0).astype(jnp.float32)
    result = jnp.zeros(values.shape, jnp.float32)
    for index in range(span):
        result = result + taps[index].astype(jnp.float32)[None, :] * padded[index : index + length]
    return jax.nn.silu(result).astype(jnp.bfloat16)


def local_scan(heads, steps, decays, writes, reads):
    length = decays.shape[-1]
    running = jnp.einsum(
        "grs,ls->grl",
        decays,
        jnp.tril(jnp.ones((length, length), jnp.float32)),
        precision=lax.Precision.HIGHEST,
    )
    causal = jnp.tril(jnp.ones((length, length), dtype=bool))
    spread = jnp.where(causal, running[..., :, None] - running[..., None, :], -jnp.inf)
    inner = jnp.einsum("gln,gsn->gls", reads, writes, preferred_element_type=jnp.float32)
    mixing = inner[:, None] * jnp.exp(spread) * steps[:, :, None, :]
    within = jnp.einsum(
        "grls,grsp->grlp",
        mixing.astype(jnp.bfloat16),
        heads,
        preferred_element_type=jnp.float32,
    )
    to_end = jnp.exp(running[..., -1:] - running) * steps
    weighted = (heads.astype(jnp.float32) * to_end[..., None]).astype(jnp.bfloat16)
    state = jnp.einsum(
        "grsp,gsn->grpn", weighted, writes, preferred_element_type=jnp.float32
    )
    return running, state, within


def exchange(items, plane, name, number, columns=False):
    devices, cores = lax.axis_size("sp"), lax.axis_size("tp")
    planes = devices // plane
    counts = [{"plane": plane, "line": planes, "all": devices}[item[1]] for item in items]
    amount = len(items)
    starts = [sum(counts[:i]) for i in range(amount)]
    shared = any(item[2] for item in items)

    def kernel(*refs):
        ins, outs = refs[:amount], refs[amount : 2 * amount]
        send, recv, pass_send, pass_recv, own = refs[2 * amount :]
        here, core = lax.axis_index("sp"), lax.axis_index("tp")
        across, within = here // plane, here % plane

        def place(reach, step):
            if reach == "plane":
                slot = (within + step + plane) % plane
                return across * plane + slot, slot
            if reach == "line":
                slot = (across + step + planes) % planes
                return slot * plane + within, slot
            up, along = step // plane, step % plane
            if step < 0:
                up, along = -((-step) // plane), -((-step) % plane)
            slot = (across + up + planes) % planes * plane + (within + along + plane) % plane
            return slot, slot

        barrier = pltpu.get_barrier_semaphore()
        greeted = 0
        for reach in ("plane", "line"):
            if not any(item[1] in (reach, "all") for item in items):
                continue
            size = {"plane": plane, "line": planes}[reach]
            for step in range(1, size):
                pl.semaphore_signal(
                    barrier,
                    inc=1,
                    device_id=(place(reach, step)[0], core),
                    device_id_type=pl.DeviceIdType.MESH,
                )
                greeted += 1
        if shared:
            for turn in range(1, cores):
                pl.semaphore_signal(
                    barrier,
                    inc=1,
                    device_id=(here, (core + turn) % cores),
                    device_id_type=pl.DeviceIdType.MESH,
                )
                greeted += 1
        pl.semaphore_wait(barrier, greeted)

        def target(i, slot, who):
            if columns:
                size = ins[i].shape[-1]
                return outs[i].at[:, pl.ds(pl.multiple_of(slot * size, size), size)]
            return outs[i].at[slot, who] if items[i][2] else outs[i].at[slot]

        def sent(i, step):
            goal, goal_slot = place(items[i][1], step)
            mine = place(items[i][1], 0)[1]
            if items[i][1] == "all" and step % plane and step >= plane:
                from_line = place("all", -(step // plane * plane))[1]
                return pltpu.make_async_remote_copy(
                    src_ref=target(i, from_line, core),
                    dst_ref=target(i, from_line, core),
                    send_sem=send.at[starts[i] + step],
                    recv_sem=recv.at[starts[i] + step],
                    device_id=(place("plane", step % plane)[0], core),
                    device_id_type=pl.DeviceIdType.MESH,
                )
            return pltpu.make_async_remote_copy(
                src_ref=ins[i].at[goal_slot] if items[i][3] else ins[i],
                dst_ref=target(i, mine, core),
                send_sem=send.at[starts[i] + step],
                recv_sem=recv.at[starts[i] + step],
                device_id=(goal, core),
                device_id_type=pl.DeviceIdType.MESH,
            )

        def arrived(i, step):
            slot = place(items[i][1], -step)[1]
            return pltpu.make_async_remote_copy(
                src_ref=ins[i].at[slot] if items[i][3] else ins[i],
                dst_ref=target(i, slot, core),
                send_sem=send.at[starts[i] + step],
                recv_sem=recv.at[starts[i] + step],
                device_id=(here, core),
                device_id_type=pl.DeviceIdType.MESH,
            )

        def passed(i, step, turn, outgoing):
            slot = place(items[i][1], -step)[1]
            other = (core + turn) % cores
            owner = core if outgoing else (core - turn + cores) % cores
            return pltpu.make_async_remote_copy(
                src_ref=ins[i] if step == 0 else target(i, slot, core),
                dst_ref=target(i, slot, owner),
                send_sem=pass_send.at[(starts[i] + step) * cores + turn],
                recv_sem=pass_recv.at[(starts[i] + step) * cores + turn],
                device_id=(here, other),
                device_id_type=pl.DeviceIdType.MESH,
            )

        kept = []
        for i in range(amount):
            if items[i][1] == "all":
                for up in range(1, planes):
                    sent(i, up * plane).start()
                for step in range(1, plane):
                    sent(i, step).start()
        for i in range(amount):
            if items[i][1] != "all":
                for step in range(1, counts[i]):
                    sent(i, step).start()
        for i in range(amount):
            slot = place(items[i][1], 0)[1]
            local = pltpu.make_async_copy(
                ins[i].at[slot] if items[i][3] else ins[i], target(i, slot, core), own.at[i]
            )
            local.start()
            kept.append(local)
            if items[i][2]:
                for turn in range(1, cores):
                    passed(i, 0, turn, True).start()
        for i in range(amount):
            if items[i][1] == "all":
                for up in range(1, planes):
                    arrived(i, up * plane).wait_recv()
                    for step in range(up * plane + 1, (up + 1) * plane):
                        sent(i, step).start()
                    for turn in range(1, cores):
                        passed(i, up * plane, turn, True).start()
        for i in range(amount):
            for step in range(1, counts[i]):
                if items[i][1] == "all" and step % plane == 0:
                    continue
                arrived(i, step).wait_recv()
                if items[i][2]:
                    for turn in range(1, cores):
                        passed(i, step, turn, True).start()
        for i in range(amount):
            kept[i].wait()
            for step in range(counts[i]):
                if step > 0:
                    sent(i, step).wait_send()
                if items[i][2]:
                    for turn in range(1, cores):
                        passed(i, step, turn, True).wait_send()
                        passed(i, step, turn, False).wait_recv()

    shapes = []
    for (array, reach, over, selected), count in zip(items, counts):
        lead = (count, cores) if over else (count,)
        tail = array.shape[1:] if selected else array.shape
        if columns:
            lead, tail = (), (tail[0], count * tail[1])
        shapes.append(jax.ShapeDtypeStruct(lead + tail, array.dtype))
    slots = sum(counts)
    return pl.pallas_call(
        kernel,
        out_shape=shapes,
        in_specs=[pl.BlockSpec(memory_space=pltpu.VMEM)] * amount,
        out_specs=[pl.BlockSpec(memory_space=pl.ANY)] * amount,
        scratch_shapes=[
            pltpu.SemaphoreType.DMA((slots,)),
            pltpu.SemaphoreType.DMA((slots,)),
            pltpu.SemaphoreType.DMA((slots * cores,)),
            pltpu.SemaphoreType.DMA((slots * cores,)),
            pltpu.SemaphoreType.DMA((amount,)),
        ],
        compiler_params=pltpu.CompilerParams(
            collective_id=number, has_side_effects=True, vmem_limit_bytes=16 * 1024 * 1024
        ),
        cost_estimate=pl.CostEstimate(
            flops=10**8, bytes_accessed=4 * 2**20, transcendentals=0
        ),
        name=name,
    )(*[item[0] for item in items])


def plain_exchange(items, plane):
    results = []
    for array, reach, over, selected in items:
        value = array
        if over:
            value = lax.all_gather(value, "tp")
        if reach == "plane":
            value = value if selected else value[None]
        else:
            value = lax.all_gather(value, "sp")
        results.append(value)
    return results


def gated_norm(mixed, gate, gain):
    length = mixed.shape[0]
    groups = mixed.shape[1]
    flat = mixed.reshape(length, groups, -1)
    gated = flat * jax.nn.silu(gate.astype(jnp.float32)).reshape(length, groups, -1)
    scaled = gated * lax.rsqrt(jnp.mean(gated * gated, axis=-1, keepdims=True) + eps)
    return (scaled * gain.reshape(groups, -1)[None]).reshape(length, -1).astype(jnp.bfloat16)


def attend(query, cosine, sine, keys, key_up, value_up_weight, length):
    heads = key_up.shape[1] // UNROTATED_WIDTH
    latent_width = key_up.shape[0]
    whole = UNROTATED_WIDTH + ROPE
    half = ROPE // 2
    step = 2 * length if keys.shape[0] % (2 * length) == 0 else length
    scale = whole ** (-0.5)
    contract = (((1,), (1,)), ((), ()))

    def kernel(q_ref, cos_ref, sin_ref, k_ref, ku_ref, vu_ref, out_ref, q_all, top, total, summed):
        start = lax.axis_index("sp") * length
        for h in range(heads):
            base = h * whole
            turn = q_ref[:, base + UNROTATED_WIDTH : base + whole].astype(jnp.float32)
            first, second = turn[:, :half], turn[:, half:]
            turned = jnp.concatenate(
                [
                    first * cos_ref[...] - second * sin_ref[...],
                    second * cos_ref[...] + first * sin_ref[...],
                ],
                axis=1,
            )
            q_all[h] = jnp.concatenate(
                [q_ref[:, base : base + UNROTATED_WIDTH], turned.astype(jnp.bfloat16)], axis=1
            )
        top[...] = jnp.full(top.shape, floor_score, jnp.float32)
        total[...] = jnp.zeros(total.shape, jnp.float32)
        summed[...] = jnp.zeros(summed.shape, jnp.float32)
        row = start + lax.broadcasted_iota(jnp.int32, (length, step), 0)
        column = lax.broadcasted_iota(jnp.int32, (length, step), 1)

        def visit(j, carry):
            at = pl.ds(pl.multiple_of(j * step, step), step)
            latent = k_ref[at, :latent_width]
            turned = k_ref[at, latent_width : latent_width + ROPE]
            seen = column + j * step <= row
            plain = jnp.dot(latent, ku_ref[...], preferred_element_type=jnp.float32).astype(
                jnp.bfloat16
            )
            all_values = jnp.dot(latent, vu_ref[...], preferred_element_type=jnp.float32).astype(
                jnp.bfloat16
            )
            for h in range(heads):
                values = all_values[:, h * VALUE_WIDTH : (h + 1) * VALUE_WIDTH]
                key = jnp.concatenate(
                    [plain[:, h * UNROTATED_WIDTH : (h + 1) * UNROTATED_WIDTH], turned], axis=1
                )
                scores = (
                    lax.dot_general(q_all[h], key, contract, preferred_element_type=jnp.float32)
                    * scale
                )
                scores = jnp.where(seen, scores, -jnp.inf)
                old = top[h][:, :1]
                new = jnp.maximum(old, jnp.max(scores, axis=1, keepdims=True))
                weights = jnp.exp(scores - new)
                shrink = jnp.exp(old - new)
                now = jnp.sum(weights, axis=1, keepdims=True)
                total[h] = total[h] * shrink + now
                summed[h] = summed[h] * shrink + jnp.dot(
                    weights.astype(jnp.bfloat16), values, preferred_element_type=jnp.float32
                )
                top[h] = jnp.broadcast_to(new, top.shape[1:])
            return carry

        lax.fori_loop(0, (start + length + step - 1) // step, visit, 0)
        for h in range(heads):
            out_ref[:, h * VALUE_WIDTH : (h + 1) * VALUE_WIDTH] = (
                summed[h] / total[h][:, :1]
            ).astype(jnp.bfloat16)

    return pl.pallas_call(
        kernel,
        out_shape=jax.ShapeDtypeStruct((length, heads * VALUE_WIDTH), jnp.bfloat16),
        in_specs=[pl.BlockSpec(memory_space=pltpu.VMEM)] * 6,
        out_specs=pl.BlockSpec(memory_space=pltpu.VMEM),
        scratch_shapes=[
            pltpu.VMEM((heads, length, whole), jnp.bfloat16),
            pltpu.VMEM((heads, length, 128), jnp.float32),
            pltpu.VMEM((heads, length, 128), jnp.float32),
            pltpu.VMEM((heads, length, VALUE_WIDTH), jnp.float32),
        ],
        compiler_params=pltpu.CompilerParams(vmem_limit_bytes=40 * 1024 * 1024),
        cost_estimate=pl.CostEstimate(
            flops=4 * 10**10, bytes_accessed=4 * 2**20, transcendentals=0
        ),
        name="attend",
    )(query, cosine, sine, keys, key_up, value_up_weight)


def fused(
    plane,
    tokens,
    mix_gain,
    query_proj,
    compressed_projection,
    compressed_norm_gain,
    rope_proj,
    key_up,
    value_up_weight,
    scan_input,
    scan_gate,
    scan_write,
    scan_read,
    step_proj,
    conv_input,
    conv_write,
    conv_read,
    decay_log,
    decay_offset,
    skip_gain,
    group_gain,
):
    devices, cores = lax.axis_size("sp"), lax.axis_size("tp")
    planes = devices // plane
    part, width = tokens.shape
    length = part * cores
    depth = scan_input.shape[0]
    kblock = depth * plane
    hw, ww = scan_input.shape[1] // plane, scan_write.shape[1] // plane
    lower, wide = hw + 2 * ww, 2 * hw + 2 * ww
    bounds = ((0, lower), (lower, wide))
    own_heads = decay_log.shape[0] // plane
    heads = key_up.shape[1] // UNROTATED_WIDTH
    latent_width = key_up.shape[0]
    key_rows = (latent_width + ROPE) * part // 128
    whole = UNROTATED_WIDTH + ROPE
    half = ROPE // 2
    scale = whole ** (-0.5)
    span = conv_input.shape[0]
    edge = 8
    bf16, f32 = jnp.bfloat16, jnp.float32
    MESH = pl.DeviceIdType.MESH
    last_contract = (((1,), (1,)), ((), ()))
    first_contract = (((0,), (0,)), ((), ()))
    best = lax.Precision.HIGHEST
    group_step = 2

    def mm(a, b):
        return jnp.dot(a, b, preferred_element_type=f32)

    def kernel(
        *refs
    ):
        sources, (att_out, scan_out) = refs[:loaded], refs[loaded : loaded + 2]
        targets = refs[loaded + 2 : 2 * loaded + 2]
        (
            w_in, w_write, w_read, w_gate, tok, mix, comp, comp_gain, rope, freqs, wq, ku, vu,
            doff, w_step, t_in, t_write, t_read, ggain, dlog, skip,
        ) = targets
        (
            load_sem, packed, wbuf, rows, keys, q_all, top, total, summed, stepw, steps, osend,
            obuf, projf, gatef, cbuf, ybuf, runs, before, decayed, state, dsum, ssend, tsend,
            srecv, trecv, incoming, stage, wsend, wrecv, zsend, ksend_up, ksend_plane,
            ksend_core, krecv, rsend, rsend_core, rrecv, rdiag_send,
            rhalf, o_send, o_recv, e_send, e_recv, s_send, s_recv, t_send, t_recv,
            out_send, out_recv,
        ) = refs[2 * loaded + 2 :]
        here, core = lax.axis_index("sp"), lax.axis_index("tp")
        z, n = here // plane, here % plane
        other = cores - 1 - core
        beside, above, across = n + 1 - 2 * (n % 2), (n + 2) % plane, plane - 1 - n
        at_end = (z == 0) | (z == planes - 1)
        nearest = (z + planes - 1) // planes
        farthest = planes - 1 - z

        loads = [
            pltpu.make_async_copy(source, target, load_sem.at[i])
            for i, (source, target) in enumerate(zip(sources, targets))
        ]
        for load in loads:
            load.start()

        def rcopy(src, dst, ss, rs, sp, c):
            return pltpu.make_async_remote_copy(
                src_ref=src, dst_ref=dst, send_sem=ss, recv_sem=rs,
                device_id=(sp, c), device_id_type=MESH,
            )

        def turned_slot(flip):
            return (n // 2 + flip // 2) % 2 * 2 + (n + flip) % 2

        def peer(step):
            return z * plane + (n + step) % plane

        barrier = pltpu.get_barrier_semaphore()
        greeted = 0
        for step in range(1, plane):
            pl.semaphore_signal(barrier, inc=1, device_id=(peer(step), core), device_id_type=MESH)
            greeted += 1
        for step in range(1, planes):
            pl.semaphore_signal(
                barrier, inc=1, device_id=((z + step) % planes * plane + n, core),
                device_id_type=MESH,
            )
            greeted += 1
        pl.semaphore_signal(barrier, inc=1, device_id=(here, other), device_id_type=MESH)
        greeted += 1
        for load in loads[:4]:
            load.wait()

        for m in range(plane):
            packed[m, :, :hw] = w_in[:, m * hw : (m + 1) * hw]
            packed[m, :, hw : hw + ww] = w_write[:, m * ww : (m + 1) * ww]
            packed[m, :, hw + ww : lower] = w_read[:, m * ww : (m + 1) * ww]
            packed[m, :, lower:] = w_gate[:, m * hw : (m + 1) * hw]
        wbuf[here] = packed[n]

        pl.semaphore_wait(barrier, greeted)

        def key_slot(sp, c):
            return keys.at[sp * cores + c]

        def key_copy(sp, c, ss, to_sp, to_c):
            return rcopy(
                key_slot(sp, c), key_slot(sp, c), ss, krecv.at[sp * cores + c], to_sp, to_c
            )

        def key_arrived(sp, c):
            key_copy(sp, c, ksend_up.at[0], here, core).wait_recv()

        def key_up_copy(d):
            return key_copy(here, core, ksend_up.at[d], here + d * plane, core)

        sides = (beside, above)

        def key_plane_copy(d, step):
            return key_copy(
                here - d * plane, core, ksend_plane.at[d * plane + step], peer(step), core
            )

        def key_core_copy(sp):
            return key_copy(sp, core, ksend_core.at[sp], here, other)

        sides = (beside, above)

        def chunk(group, index):
            low, high = bounds[group]
            return wbuf.at[index, :, low:high]

        def w_arrived(group, index):
            rcopy(
                chunk(group, index), chunk(group, index), zsend.at[0, group, index],
                wrecv.at[group, index], here, core,
            ).wait_recv()

        def w_plane_copy(group, step):
            low, high = bounds[group]
            goal = turned_slot(step)
            return rcopy(
                packed.at[goal, :, low:high], chunk(group, here), wsend.at[group, step],
                wrecv.at[group, here], z * plane + goal, core,
            )

        def z_copy(group, index, up):
            return rcopy(
                chunk(group, index), chunk(group, index), zsend.at[up, group, index],
                wrecv.at[group, index], here + (plane if up else -plane), core,
            )

        def has_next(up):
            return z + 1 < planes if up else z > 0

        def own_weights(group, steps_of):
            for step in steps_of:
                index = z * plane + turned_slot(step)
                if step:
                    w_arrived(group, index)
                for up in (0, 1):
                    @pl.when(has_next(up))
                    def _():
                        z_copy(group, index, up).start()

        def far_weights(group, d, forward, pieces=range(plane), ways=(0, 1)):
            for up in ways:
                source = z - d if up else z + d
                exists = (source >= 0) & (source < planes)
                gate = has_next(up) if forward else jnp.logical_not(has_next(up))

                @pl.when(exists & gate)
                def _():
                    for step in pieces:
                        index = source * plane + turned_slot(step)
                        w_arrived(group, index)
                        if forward:
                            z_copy(group, index, up).start()

        for step in range(1, plane):
            w_plane_copy(0, step).start()
        own_weights(0, (0,))
        own_weights(1, (0,))

        for load in loads[4:10]:
            load.wait()
        def normed_rows(values, gain, count):
            mean = jnp.sum(values * values, axis=-1, keepdims=True) / count
            return values * lax.rsqrt(mean + eps) * gain

        normed = normed_rows(tok[...].astype(f32), mix[...], width).astype(bf16)

        def rows_at(slot, c):
            return pl.ds(pl.multiple_of(slot * length + c * part, part), part)

        for p in range(planes):
            rows[p, rows_at(n, core), :] = normed[:, p * kblock : (p + 1) * kblock]

        def angles(start, count):
            position = (start + lax.broadcasted_iota(jnp.int32, (count, 1), 0)).astype(f32)
            angle = position * freqs[...]
            return jnp.cos(angle), jnp.sin(angle)

        def turn(first, second, cosine, sine):
            return [first * cosine - second * sine, second * cosine + first * sine]

        latent = normed_rows(mm(normed, comp[...]), comp_gain[...], latent_width)
        small = lax.dot_general(normed, rope[...], last_contract, preferred_element_type=f32)
        cosine, sine = angles(here * length + core * part, part)
        own_slot = here * cores + core
        for low in range(0, latent_width, 128):
            keys[own_slot, low * part // 128 : (low + 128) * part // 128] = latent[
                :, low : low + 128
            ].astype(bf16)
        turned_key = jnp.concatenate(
            turn(small[:, :half], small[:, half:], cosine, sine), axis=1
        ).astype(bf16)
        keys[own_slot, latent_width * part // 128 :] = jnp.concatenate(
            [turned_key[: part // 2], turned_key[part // 2 :]], axis=1
        )

        for d in range(1, planes):
            @pl.when(z + d < planes)
            def _():
                key_up_copy(d).start()
        key_core_copy(here).start()

        def row_copy(slot, ss, to_sp, to_c):
            at = rows.at[:, rows_at(slot, core), :]
            return rcopy(at, at, ss, rrecv.at[slot * cores + core], to_sp, to_c)

        def row_part(slot, part_of, ss, rs, to_sp):
            low, high = part_of * planes // 2, (part_of + 1) * planes // 2
            at = rows.at[low:high, rows_at(slot, core), :]
            return rcopy(at, at, ss, rs, to_sp, core)

        def row_plane_copy(side, part_of):
            return row_part(
                n, part_of, rsend.at[side, part_of], rhalf.at[n, part_of],
                z * plane + sides[side],
            )

        def row_half_arrived(slot, part_of):
            row_part(
                slot, part_of, rsend.at[0, 0], rhalf.at[slot, part_of], here
            ).wait_recv()

        def row_relay(side):
            slot = sides[side]
            return row_part(
                slot, side, rdiag_send.at[side], rhalf.at[slot, side],
                z * plane + sides[1 - side],
            )

        def row_core_copy(slot):
            return row_copy(slot, rsend_core.at[slot], here, other)

        def row_arrived(slot, c):
            at = rows.at[:, rows_at(slot, c), :]
            rcopy(at, at, rsend.at[0], rrecv.at[slot * cores + c], here, core).wait_recv()

        def offset_copy(step):
            goal = (n + step) % plane
            return rcopy(
                osend.at[goal], obuf.at[n], o_send.at[step], o_recv.at[n],
                z * plane + goal, core,
            )

        row_core_copy(n).start()

        positions = plane * length
        at_edge = rows.at[:, positions : positions + edge, :]
        closing = (n == plane - 1) & (core == cores - 1)

        def edge_up_copy():
            return rcopy(
                rows.at[:, positions - edge : positions, :], at_edge, e_send.at[0], e_recv,
                here + plane, core,
            )

        def edge_plane_copy(step):
            return rcopy(at_edge, at_edge, e_send.at[step], e_recv, peer(step), core)

        def edge_core_copy():
            return rcopy(at_edge, at_edge, e_send.at[plane], e_recv, here, other)

        def edge_arrived():
            rcopy(at_edge, at_edge, e_send.at[0], e_recv, here, core).wait_recv()

        @pl.when(closing & (z + 1 < planes))
        def _():
            edge_up_copy().start()

        for load in loads[10:]:
            load.wait()
        for m in range(plane):
            osend[m, :own_heads] = doff[m * own_heads : (m + 1) * own_heads]
        obuf[n] = osend[n]

        @pl.when(z == 0)
        def _():
            rows[:, plane * length :, :] = jnp.zeros((planes, edge, kblock), bf16)

        row_arrived(n, other)
        own_rows = pl.ds(pl.multiple_of(n * length, length), length)
        query = mm(rows[0, own_rows, :], wq[:kblock, :])
        for p in range(1, planes):
            query += mm(rows[p, own_rows, :], wq[p * kblock : (p + 1) * kblock, :])
        query = query.astype(bf16)
        cosine, sine = angles(here * length, length)
        for h in range(heads):
            base = h * whole
            rope_part = query[:, base + UNROTATED_WIDTH : base + whole].astype(f32)
            q_all[h] = jnp.concatenate(
                [query[:, base : base + UNROTATED_WIDTH]]
                + [
                    v.astype(bf16)
                    for v in turn(rope_part[:, :half], rope_part[:, half:], cosine, sine)
                ],
                axis=1,
            )
        top[...] = jnp.full(top.shape, floor_score, f32)
        total[...] = jnp.zeros(total.shape, f32)
        summed[...] = jnp.zeros(summed.shape, f32)

        own_weights(0, range(1, plane))
        for step in range(1, plane):
            key_plane_copy(0, step).start()
        for d in range(1, planes):
            @pl.when(z >= d)
            def _():
                key_arrived(here - d * plane, core)
                for step in range(1, plane):
                    key_plane_copy(d, step).start()
                key_core_copy(here - d * plane).start()

        @pl.when(closing & (z > 0))
        def _():
            edge_arrived()
            for step in range(1, plane):
                edge_plane_copy(step).start()
            edge_core_copy().start()

        for step in range(1, plane):
            w_plane_copy(1, step).start()
        for first in (0, 1):
            for side in (0, 1):
                row_plane_copy(side, (side + first) % 2).start()
        for step in range(1, plane):
            offset_copy(step).start()

        def pass_keys(d):
            for step in range(1, plane):
                sp = (z - d) * plane + (n + step) % plane
                key_arrived(sp, core)
                key_core_copy(sp).start()

        def other_keys(d):
            for q in range(plane):
                key_arrived((z - d) * plane + q, other)

        size = group_step * length
        row = lax.broadcasted_iota(jnp.int32, (length, size), 0)
        column = lax.broadcasted_iota(jnp.int32, (length, size), 1)

        def visit(first_block, limit):
            count = group_step * cores
            block = keys[pl.ds(first_block * cores, count)]
            lat = jnp.concatenate(
                [
                    block[:, low * part // 128 : (low + 128) * part // 128].reshape(size, 128)
                    for low in range(0, latent_width, 128)
                ],
                axis=1,
            )
            turned = block[:, latent_width * part // 128 :]
            turned = jnp.concatenate([turned[:, :, :ROPE], turned[:, :, ROPE:]], axis=1)
            turned = turned.reshape(size, ROPE)
            plain = mm(lat, ku[...]).astype(bf16)
            all_values = mm(lat, vu[...]).astype(bf16)
            if limit is not None:
                seen = column <= row + limit
            for h in range(heads):
                values = all_values[:, h * VALUE_WIDTH : (h + 1) * VALUE_WIDTH]
                key = jnp.concatenate(
                    [plain[:, h * UNROTATED_WIDTH : (h + 1) * UNROTATED_WIDTH], turned], axis=1
                )
                scores = (
                    lax.dot_general(q_all[h], key, last_contract, preferred_element_type=f32)
                    * scale
                )
                if limit is not None:
                    scores = jnp.where(seen, scores, -jnp.inf)
                old = top[h][:, :1]
                new = jnp.maximum(old, jnp.max(scores, axis=1, keepdims=True))
                weights = jnp.exp(scores - new)
                shrink = jnp.exp(old - new)
                now = jnp.sum(weights, axis=1, keepdims=True)
                total[h] = total[h] * shrink + now
                summed[h] = summed[h] * shrink + mm(weights.astype(bf16), values)
                top[h] = jnp.broadcast_to(new, top.shape[1:])

        pass_keys(0)

        @pl.when(z >= 1)
        def _():
            pass_keys(1)

        far_weights(0, 1, True)
        other_keys(0)

        def near(j, carry):
            visit(z * plane + j * group_step, (n - j * group_step) * length)
            return carry

        lax.fori_loop(0, n // group_step + 1, near, 0)

        late = min(2, planes - 1)

        def further(d, carry):
            @pl.when(z > d)
            def _():
                pass_keys(d + 1)

            @pl.when(d == late)
            def _():
                for far in range(2, planes - 1):
                    far_weights(0, far, True, range(plane // 2))

            @pl.when(z >= d)
            def _():
                other_keys(d)

                def inner(j, carry):
                    visit((z - d) * plane + j * group_step, None)
                    return carry

                lax.fori_loop(0, plane // group_step, inner, 0)

            @pl.when(d == late)
            def _():
                for far in range(2, planes - 1):
                    far_weights(0, far, True, range(plane // 2, plane))
                own_weights(1, range(1, plane))

            @pl.when((d == late) & (z == 1))
            def _():
                far_weights(1, 1, True, ways=(1,))

            return carry

        lax.fori_loop(1, planes, further, 0)
        for h in range(heads):
            att_out[:, h * VALUE_WIDTH : (h + 1) * VALUE_WIDTH] = (
                summed[h] / total[h][:, :1]
            ).astype(bf16)

        @pl.when((z > 0) & (core == cores - 1) & (n < plane - 1))
        def _():
            edge_arrived()
            edge_core_copy().start()

        for side in (0, 1):
            row_half_arrived(sides[side], side)
            row_relay(side).start()
        for side in (0, 1):
            row_half_arrived(sides[side], 1 - side)
            row_core_copy(sides[side]).start()
        for d in range(1, planes - 1):
            far_weights(0, d, False)

        def tile(k):
            return pl.ds(pl.multiple_of(k * length, length), length)

        def project(p, values, group):
            low, high = bounds[group]
            block = wbuf[pl.ds(p * plane, plane), :, low:high]
            return mm(values, block.reshape(kblock, high - low))

        def sum_near(group, at, store):
            @pl.when(at_end)
            def _():
                out = project(nearest, rows[nearest, at, :], group)
                for p in range(1, planes - 1):
                    out += project(nearest + p, rows[nearest + p, at, :], group)
                store(out, False)

            @pl.when(jnp.logical_not(at_end))
            def _():
                out = project(0, rows[0, at, :], group)
                for p in range(1, planes):
                    out += project(p, rows[p, at, :], group)
                store(out, False)

        def sum_far(group, at, store):
            store(project(farthest, rows[farthest, at, :], group), True)

        def into(low, count):
            def store(out, add):
                at = pl.ds(low, count)
                projf[at, :] = projf[at, :] + out if add else out

            return store

        def edge_sum(method):
            method(0, pl.ds(positions, edge), into(0, edge))

        def tile_sum(method, k):
            method(0, tile(k), into(pl.multiple_of(k * length + edge, edge), length))

        lane = lax.broadcasted_iota(jnp.int32, (128, w_step.shape[0]), 0)
        which = lax.broadcasted_iota(jnp.int32, (128, w_step.shape[0]), 1)
        first_head = (core * plane + n) * own_heads
        chosen = ((which == lane + first_head) & (lane < own_heads)).astype(bf16)
        stepw[...] = mm(chosen, w_step[...]).astype(bf16)

        def step_tile(k):
            raw = jnp.zeros((length, 128), f32)
            for p in range(planes):
                raw += lax.dot_general(
                    rows[p, tile(k), :], stepw[:, p * kblock : (p + 1) * kblock],
                    last_contract, preferred_element_type=f32,
                )
            steps[k] = jnp.maximum(raw, 0.0) + jnp.log1p(jnp.exp(-jnp.abs(raw)))

        @pl.when((z > 0) & (core < cores - 1))
        def _():
            edge_arrived()

        edge_sum(sum_near)

        def first_sums(flip, carry):
            slot = turned_slot(flip)

            @pl.when(flip == plane - 1)
            def _():
                for part_of in (0, 1):
                    row_half_arrived(across, part_of)
                row_core_copy(across).start()

            @pl.when(flip > 0)
            def _():
                row_arrived(slot, other)

            tile_sum(sum_near, slot)
            step_tile(slot)
            return carry

        lax.fori_loop(0, plane, first_sums, 0)
        far_weights(1, 1, True, ways=(0,))

        @pl.when(z > 1)
        def _():
            far_weights(1, 1, True, ways=(1,))

        far_weights(0, planes - 1, False)

        @pl.when(at_end)
        def _():
            edge_sum(sum_far)

            def last_sums(k, carry):
                tile_sum(sum_far, k)
                return carry

            lax.fori_loop(0, plane, last_sums, 0)


        for d in range(2, planes - 1):
            far_weights(1, d, True, range(plane // 2), (1,))

        taps = jnp.concatenate(
            [
                t_in[:, pl.ds(pl.multiple_of(n * hw, hw), hw)],
                t_write[:, pl.ds(pl.multiple_of(n * ww, ww), ww)],
                t_read[:, pl.ds(pl.multiple_of(n * ww, ww), ww)],
            ],
            axis=1,
        ).astype(f32)

        def conv_tile(k, carry):
            base = pl.ds(pl.multiple_of(k * length, length), length + edge)
            for low in range(0, lower, 128):
                at = slice(low, low + 128)
                values = projf[base, at].astype(bf16).astype(f32)
                result = jnp.zeros((length, 128), f32)
                for i in range(span):
                    shift = edge - span + 1 + i
                    result = result + taps[i : i + 1, at] * values[shift : shift + length]
                cbuf[tile(k), at] = (result * jax.nn.sigmoid(result)).astype(bf16)
            return carry

        lax.fori_loop(0, plane, conv_tile, 0)

        for step in range(1, plane):
            slot = (n - step + plane) % plane
            rcopy(
                obuf.at[slot], obuf.at[slot], o_send.at[0], o_recv.at[slot], here, core
            ).wait_recv()
        lane_row = lax.broadcasted_iota(jnp.int32, (1, 128), 1)
        rate = jnp.zeros((1, 128), f32)
        for h in range(own_heads):
            rate = jnp.where(lane_row == h, dlog[n * own_heads + h], rate)
        rate = -jnp.exp(rate)
        causal = lax.broadcasted_iota(jnp.int32, (length, length), 0) >= lax.broadcasted_iota(
            jnp.int32, (length, length), 1
        )
        tri = causal.astype(f32)

        def per_lane(columns):
            return jnp.concatenate(
                [
                    jnp.broadcast_to(columns[:, h : h + 1], (columns.shape[0], SSM_DIM))
                    for h in range(own_heads)
                ],
                axis=1,
            )

        def per_row(values):
            return jnp.concatenate(
                [
                    jnp.broadcast_to(values[:, h : h + 1], (SSM_DIM, SSM_STATE))
                    for h in range(own_heads)
                ],
                axis=0,
            )

        state[...] = jnp.zeros(state.shape, f32)
        dsum[...] = jnp.zeros(dsum.shape, f32)

        def scan_tile(k, carry):
            step_col = steps[k]
            off_col = jnp.concatenate(
                [obuf[k], jnp.zeros((128 - obuf.shape[1], length), f32)], axis=0
            ).T
            decay = jnp.where(lane_row < own_heads, rate * step_col + off_col, 0.0)
            running = jnp.dot(tri, decay, precision=best, preferred_element_type=f32)
            runs[k] = running
            run_row, step_row = running.T, step_col.T
            x = cbuf[tile(k), :hw]
            w = cbuf[tile(k), hw : hw + ww]
            r = cbuf[tile(k), hw + ww : lower]
            inner = lax.dot_general(r, w, last_contract, preferred_element_type=f32)
            for h in range(own_heads):
                at = slice(h * SSM_DIM, (h + 1) * SSM_DIM)
                spread = jnp.where(
                    causal, running[:, h : h + 1] - run_row[h : h + 1, :], -jnp.inf
                )
                mixing = inner * jnp.exp(spread) * step_row[h : h + 1, :]
                ybuf[tile(k), at] = (
                    mm(mixing.astype(bf16), x[:, at])
                    + skip[n * own_heads + h] * x[:, at].astype(f32)
                )
            last = running[length - 1 : length, :]
            to_end = jnp.exp(last - running) * step_col
            weighted = (x.astype(f32) * per_lane(to_end)).astype(bf16)
            update = lax.dot_general(weighted, w, first_contract, preferred_element_type=f32)
            before[k] = state[...]
            decayed[k] = dsum[...]
            state[...] = per_row(jnp.exp(last)) * state[...] + update
            dsum[...] = dsum[...] + last
            return carry

        lax.fori_loop(0, plane, scan_tile, 0)

        def state_arrived(p):
            rcopy(ssend, srecv.at[p], s_send.at[0], s_recv.at[p], here, core).wait_recv()
            rcopy(tsend, trecv.at[p], t_send.at[0], t_recv.at[p], here, core).wait_recv()

        def state_copies(d):
            to = here + d * plane
            return (
                rcopy(ssend, srecv.at[z], s_send.at[d], s_recv.at[z], to, core),
                rcopy(tsend, trecv.at[z], t_send.at[d], t_recv.at[z], to, core),
            )

        def to_send(d):
            return (z + d < planes) & ((z == 0) | (d == 1))

        @pl.when((z > 1) & (z + 1 < planes))
        def _():
            state_arrived(z - 1)
            ssend[...] = (
                per_row(jnp.exp(dsum[:1])) * srecv[z - 1].astype(f32) + state[...]
            ).astype(bf16)
            tsend[...] = dsum[...] + trecv[z - 1]

        @pl.when(z <= 1)
        def _():
            ssend[...] = state[...].astype(bf16)
            tsend[...] = dsum[...]

        for d in range(1, planes):
            @pl.when(to_send(d))
            def _():
                for copy in state_copies(d):
                    copy.start()

        for d in range(2, planes - 1):
            far_weights(1, d, True, range(plane // 2, plane), (1,))
            far_weights(1, d, True, ways=(0,))
        for d in range(1, planes - 1):
            far_weights(1, d, False)

        def gate_tile(k, carry):
            def store(out, add):
                gatef[tile(k), :] = out

            sum_near(1, tile(k), store)
            return carry

        lax.fori_loop(0, plane, gate_tile, 0)
        @pl.when((z > 1) & (z + 1 == planes))
        def _():
            state_arrived(z - 1)

        @pl.when(z > 0)
        def _():
            state_arrived(0)

        @pl.when(z == 1)
        def _():
            incoming[...] = srecv[0].astype(f32)

        @pl.when(z > 1)
        def _():
            incoming[...] = (
                per_row(jnp.exp(trecv[z - 1][:1])) * srecv[0].astype(f32)
                + srecv[z - 1].astype(f32)
            )

        def carry_tile(k, carry):
            entered = (
                before[k] + per_row(jnp.exp(decayed[k][:1])) * incoming[...]
            ).astype(bf16)
            carried = lax.dot_general(
                cbuf[tile(k), hw + ww : lower], entered, last_contract,
                preferred_element_type=f32,
            )
            ybuf[tile(k), :] = ybuf[tile(k), :] + carried * per_lane(jnp.exp(runs[k]))
            return carry

        @pl.when(z == 0)
        def _():
            incoming[...] = jnp.zeros(incoming.shape, f32)

        lax.fori_loop(0, plane, carry_tile, 0)
        far_weights(1, planes - 1, False)
        own_columns = pl.ds(pl.multiple_of(n * hw, hw), hw)
        gain = ggain[:, own_columns]

        def out_copy(k):
            return rcopy(
                stage.at[k], scan_out.at[:, own_columns], out_send.at[k], out_recv.at[n],
                z * plane + k, core,
            )

        def finish(i, carry):
            k = turned_slot(plane - 1 - i)

            @pl.when(at_end)
            def _():
                def store(out, add):
                    gatef[tile(k), :] = gatef[tile(k), :] + out

                sum_far(1, tile(k), store)

            gate = gatef[tile(k), :].astype(bf16).astype(f32)
            mixed = ybuf[tile(k), :]
            gated = mixed * (gate * jax.nn.sigmoid(gate))
            out = normed_rows(gated, gain, hw).astype(bf16)
            stage[k] = out

            @pl.when(k != n)
            def _():
                out_copy(k).start()

            @pl.when(k == n)
            def _():
                scan_out[:, own_columns] = out

            return carry

        lax.fori_loop(0, plane, finish, 0)
        for step in range(1, plane):
            slot = (n + step) % plane
            at = scan_out.at[:, pl.ds(pl.multiple_of(slot * hw, hw), hw)]
            rcopy(stage.at[0], at, out_send.at[0], out_recv.at[slot], here, core).wait_recv()

        for d in range(1, planes):
            @pl.when(z + d < planes)
            def _():
                key_up_copy(d).wait_send()

            @pl.when(to_send(d))
            def _():
                for copy in state_copies(d):
                    copy.wait_send()

        for d in range(planes):
            @pl.when(z >= d)
            def _():
                for step in range(1, plane):
                    key_plane_copy(d, step).wait_send()
                for q in range(plane):
                    key_core_copy((z - d) * plane + q).wait_send()
        for step in range(1, plane):
            for group in (0, 1):
                w_plane_copy(group, step).wait_send()
            offset_copy(step).wait_send()
            out_copy((n + step) % plane).wait_send()
        for side in (0, 1):
            for part_of in (0, 1):
                row_plane_copy(side, part_of).wait_send()
            row_relay(side).wait_send()
        for slot in range(plane):
            row_core_copy(slot).wait_send()

        @pl.when(closing & (z + 1 < planes))
        def _():
            edge_up_copy().wait_send()

        @pl.when(closing & (z > 0))
        def _():
            for step in range(1, plane):
                edge_plane_copy(step).wait_send()

        @pl.when((z > 0) & (core == cores - 1))
        def _():
            edge_core_copy().wait_send()

        for up in (0, 1):
            for p in range(planes):
                @pl.when(((p <= z) if up else (p >= z)) & has_next(up))
                def _():
                    for q in range(plane):
                        for group in (0, 1):
                            z_copy(group, p * plane + q, up).wait_send()

    vmem = pl.BlockSpec(memory_space=pltpu.VMEM)
    hbm = pl.BlockSpec(memory_space=pltpu.HBM)
    freqs = np.float32(theta) ** (-np.arange(half, dtype=np.float32) * np.float32(2.0 / ROPE))
    inputs = (
        scan_input,
        scan_write,
        scan_read,
        scan_gate,
        tokens,
        mix_gain[None, :],
        compressed_projection,
        compressed_norm_gain[None, :],
        rope_proj.T,
        jnp.asarray(freqs[None, :], f32),
        query_proj,
        key_up,
        value_up_weight,
        decay_offset.T,
        step_proj.T,
        conv_input,
        conv_write,
        conv_read,
        group_gain[None, :],
        decay_log,
        skip_gain,
    )
    loaded = len(inputs)
    dma = pltpu.SemaphoreType.DMA
    positions = plane * length
    results = (
        jax.ShapeDtypeStruct((length, heads * VALUE_WIDTH), bf16),
        jax.ShapeDtypeStruct((length, scan_input.shape[1]), bf16),
    )
    outs = pl.pallas_call(
        kernel,
        out_shape=results,
        in_specs=[hbm] * loaded,
        out_specs=(vmem, vmem),
        scratch_shapes=[pltpu.VMEM(value.shape, value.dtype) for value in inputs[:-2]]
        + [pltpu.SMEM(value.shape, value.dtype) for value in inputs[-2:]]
        + [
            dma((loaded,)),
            pltpu.VMEM((plane, depth, wide), bf16),
            pltpu.VMEM((devices, depth, wide), bf16),
            pltpu.VMEM((planes, positions + edge, kblock), bf16),
            pltpu.VMEM((devices * cores, key_rows, 128), bf16),
            pltpu.VMEM((heads, length, whole), bf16),
            pltpu.VMEM((heads, length, 128), f32),
            pltpu.VMEM((heads, length, 128), f32),
            pltpu.VMEM((heads, length, VALUE_WIDTH), f32),
            pltpu.VMEM((128, width), bf16),
            pltpu.VMEM((plane, length, 128), f32),
            pltpu.VMEM((plane, 8, length), f32),
            pltpu.VMEM((plane, 8, length), f32),
            pltpu.VMEM((edge + positions, lower), f32),
            pltpu.VMEM((positions, hw), f32),
            pltpu.VMEM((positions, lower), bf16),
            pltpu.VMEM((positions, hw), f32),
            pltpu.VMEM((plane, length, 128), f32),
            pltpu.VMEM((plane, own_heads * SSM_DIM, SSM_STATE), f32),
            pltpu.VMEM((plane, 8, 128), f32),
            pltpu.VMEM((own_heads * SSM_DIM, SSM_STATE), f32),
            pltpu.VMEM((8, 128), f32),
            pltpu.VMEM((own_heads * SSM_DIM, SSM_STATE), bf16),
            pltpu.VMEM((8, 128), f32),
            pltpu.VMEM((planes, own_heads * SSM_DIM, SSM_STATE), bf16),
            pltpu.VMEM((planes, 8, 128), f32),
            pltpu.VMEM((own_heads * SSM_DIM, SSM_STATE), f32),
            pltpu.VMEM((plane, length, hw), bf16),
            dma((2, plane)),
            dma((2, devices)),
            dma((2, 2, devices)),
            dma((planes,)),
            dma((devices,)),
            dma((devices,)),
            dma((devices * cores,)),
            dma((2, 2)),
            dma((plane,)),
            dma((plane * cores,)),
            dma((2,)),
            dma((plane, 2)),
            dma((plane,)),
            dma((plane,)),
            dma((plane + 1,)),
            dma,
            dma((planes,)),
            dma((planes,)),
            dma((planes,)),
            dma((planes,)),
            dma((plane,)),
            dma((plane,)),
        ],
        compiler_params=pltpu.CompilerParams(
            collective_id=1, has_side_effects=True, vmem_limit_bytes=48 * 1024 * 1024
        ),
        name="fused",
    )(*[pltpu.with_memory_space_constraint(value, pltpu.HBM) for value in inputs])

    def settle(a_in, b_in, a_out, b_out, sems):
        copies = [
            pltpu.make_async_copy(a_in, a_out, sems.at[0]),
            pltpu.make_async_copy(b_in, b_out, sems.at[1]),
        ]
        for copy in copies:
            copy.start()
        for copy in copies:
            copy.wait()

    return pl.pallas_call(
        settle,
        out_shape=results,
        in_specs=[vmem, vmem],
        out_specs=(hbm, hbm),
        scratch_shapes=[dma((2,))],
        compiler_params=pltpu.CompilerParams(vmem_limit_bytes=4 * 1024 * 1024),
        name="settle",
    )(*outs)


def shards(
    tokens,
    mix_gain,
    query_proj,
    compressed_projection,
    compressed_norm_gain,
    rope_proj,
    key_up,
    value_up_weight,
    scan_input,
    scan_gate,
    scan_write,
    scan_read,
    step_proj,
    conv_input,
    conv_write,
    conv_read,
    decay_log,
    decay_offset,
    skip_gain,
    group_gain,
):
    groups = scan_write.shape[1] // SSM_STATE
    devices, cores = lax.axis_size("sp"), lax.axis_size("tp")
    plane = groups if devices % groups == 0 else 1
    planes = devices // plane
    sp_index, core = lax.axis_index("sp"), lax.axis_index("tp")
    across, within = sp_index // plane, sp_index % plane
    own_groups = groups // plane
    direct = plane > 1
    if direct and cores == 2 and own_groups == 1 and plane == 4 and planes > 1:
        return fused(
            plane,
            tokens,
            mix_gain,
            query_proj,
            compressed_projection,
            compressed_norm_gain,
            rope_proj,
            key_up,
            value_up_weight,
            scan_input,
            scan_gate,
            scan_write,
            scan_read,
            step_proj,
            conv_input,
            conv_write,
            conv_read,
            decay_log,
            decay_offset,
            skip_gain,
            group_gain,
        )

    def move(items, name, number, columns=False):
        if direct:
            return exchange(items, plane, name, number, columns)
        return plain_exchange(items, plane)

    depth = scan_input.shape[0]
    widths = [w.shape[1] // plane for w in (scan_input, scan_gate, scan_write, scan_read)]
    offsets = [sum(widths[:i]) for i in range(4)]
    packed = jnp.stack(
        [
            jnp.concatenate(
                [
                    w[:, n * size : (n + 1) * size]
                    for w, size in zip((scan_input, scan_gate, scan_write, scan_read), widths)
                ],
                axis=1,
            )
            for n in range(plane)
        ]
    )
    (part_weights,) = move([(packed, "plane", False, True)], "weights_in_plane", 1)
    weights = lax.all_gather(
        part_weights.reshape(plane * depth, -1),
        "sp",
        axis=0,
        tiled=True,
        axis_index_groups=[[p * plane + n for p in range(planes)] for n in range(plane)],
    )

    own_normed = rms_scale(tokens, mix_gain).astype(jnp.bfloat16)
    part = tokens.shape[0]
    length = part * cores
    latent_width = compressed_projection.shape[1]
    small = jnp.dot(
        own_normed,
        jnp.concatenate([compressed_projection, rope_proj], axis=1),
        preferred_element_type=jnp.float32,
    )
    latent = rms_scale(small[:, :latent_width], compressed_norm_gain).astype(jnp.bfloat16)
    part_positions = sp_index * length + core * part + jnp.arange(part, dtype=jnp.int32)
    key_turned = rotate(small[:, latent_width:], part_positions).astype(jnp.bfloat16)
    padding = jnp.zeros((part, -(latent_width + ROPE) % 128), jnp.bfloat16)
    own_keys = jnp.concatenate([latent, key_turned, padding], axis=1)
    all_keys, all_rows, offsets_seen = move(
        [
            (own_keys, "all", True, False),
            (own_normed, "plane", True, False),
            (decay_offset.T, "plane", False, False),
        ],
        "rows_and_keys",
        2,
    )
    all_keys = all_keys.reshape(devices * length, -1)
    all_rows = all_rows.reshape(plane * length, -1)
    edge_rows = from_behind(all_rows[plane * length - 8 :], "sp", plane)
    positions = sp_index * length + jnp.arange(length, dtype=jnp.int32)
    rows = lax.dynamic_slice_in_dim(all_rows, within * length, length, 0)
    query = jnp.dot(rows, query_proj, preferred_element_type=jnp.float32).astype(jnp.bfloat16)
    half = ROPE // 2
    freqs = theta ** (-jnp.arange(half, dtype=jnp.float32) * 2.0 / ROPE)
    angle = positions.astype(jnp.float32)[:, None] * freqs[None, :]
    attended = attend(
        query, jnp.cos(angle), jnp.sin(angle), all_keys, key_up, value_up_weight, length
    )

    def own_part(array, axis, size):
        return lax.dynamic_slice_in_dim(array, within * size, size, axis)

    local_heads = decay_log.shape[0]
    own_heads = local_heads // plane
    per_group = local_heads // groups
    step_raw = jnp.dot(
        all_rows,
        lax.dynamic_slice_in_dim(
            step_proj, core * local_heads + within * own_heads, own_heads, 1
        ),
        preferred_element_type=jnp.float32,
    )
    step_size = jax.nn.softplus(step_raw)
    own_offset = own_part(offsets_seen, 1, own_heads)
    step_values = jnp.transpose(step_size.reshape(plane, length, own_heads), (0, 2, 1))
    decay_values = (
        -jnp.exp(own_part(decay_log, 0, own_heads))[None, :, None] * step_values + own_offset
    )

    projected = jnp.dot(all_rows, weights, preferred_element_type=jnp.float32).astype(jnp.bfloat16)
    edge = jnp.dot(edge_rows, weights, preferred_element_type=jnp.float32).astype(jnp.bfloat16)
    span = conv_input.shape[0] - 1

    def convolved(i, taps):
        at = slice(offsets[i], offsets[i] + widths[i])
        return short_conv(projected[:, at], edge[8 - span :, at], own_part(taps, 1, widths[i]))

    head_conv = convolved(0, conv_input)
    gate = projected[:, offsets[1] : offsets[1] + widths[1]]
    writes = convolved(2, conv_write)
    reads = convolved(3, conv_read)
    blocks = plane * own_groups

    def by_block(values, last):
        split = values.reshape(plane, length, own_groups, last)
        return jnp.transpose(split, (0, 2, 1, 3)).reshape(blocks, length, last)

    head_values = jnp.transpose(
        head_conv.reshape(plane, length, own_groups, per_group, SSM_DIM), (0, 2, 3, 1, 4)
    ).reshape(blocks, per_group, length, SSM_DIM)
    write_values = by_block(writes, SSM_STATE)
    read_values = by_block(reads, SSM_STATE)
    running, state, mixed = local_scan(
        head_values,
        step_values.reshape(blocks, per_group, length),
        decay_values.reshape(blocks, per_group, length),
        write_values,
        read_values,
    )
    states = state.reshape(plane, own_heads, SSM_DIM, SSM_STATE)
    totals = running[..., -1].reshape(plane, own_heads)
    before, decayed = [jnp.zeros_like(states[0])], [jnp.zeros_like(totals[0])]
    for index in range(plane):
        before.append(jnp.exp(totals[index])[:, None, None] * before[-1] + states[index])
        decayed.append(totals[index] + decayed[-1])
    sent_total = jnp.pad(decayed[-1][None, :], ((0, 7), (0, 128 - own_heads)))
    seen_states, seen_totals = move(
        [
            (before[-1].reshape(-1, SSM_STATE).astype(jnp.bfloat16), "line", False, False),
            (sent_total, "line", False, False),
        ],
        "states",
        3,
    )
    seen_states = seen_states.reshape(planes, own_heads, SSM_DIM, SSM_STATE).astype(jnp.float32)
    seen_totals = seen_totals[:, 0, :own_heads]
    index = jnp.arange(planes)
    between = (index[None, :] > index[:, None]) & (index[None, :] < across)
    path = jnp.sum(jnp.where(between[:, :, None], seen_totals[None], 0.0), axis=1)
    reached = (index < across)[:, None]
    factor = jnp.where(reached, jnp.exp(path), 0.0)
    incoming = jnp.sum(seen_states * factor[:, :, None, None], axis=0)
    entered = jnp.stack(
        [
            before[k] + jnp.exp(decayed[k])[:, None, None] * incoming
            for k in range(plane)
        ]
    ).reshape(blocks, per_group, SSM_DIM, SSM_STATE)
    carried = jnp.einsum(
        "gln,grpn->grlp",
        read_values,
        entered.astype(jnp.bfloat16),
        preferred_element_type=jnp.float32,
    )
    skip = jnp.broadcast_to(
        own_part(skip_gain, 0, own_heads).reshape(1, own_groups, per_group),
        (plane, own_groups, per_group),
    ).reshape(blocks, per_group, 1, 1)
    mixed = (
        mixed
        + carried * jnp.exp(running)[..., None]
        + skip * head_values.astype(jnp.float32)
    )
    mixed = jnp.transpose(
        mixed.reshape(plane, own_groups, per_group, length, SSM_DIM), (0, 3, 1, 2, 4)
    ).reshape(plane * length, own_groups, per_group, SSM_DIM)
    scanned = gated_norm(mixed, gate, own_part(group_gain, 0, widths[0]))
    (columns,) = move(
        [(scanned.reshape(plane, length, -1), "plane", False, True)], "outputs_in_plane", 4, True
    )
    scanned = columns.reshape(length, -1)
    return (attended, scanned)


def solution(mesh):
    in_specs = (
        P(("sp", "tp"), None),
        P(),
        P(None, "tp"),
        P(),
        P(),
        P(),
        P(None, "tp"),
        P(None, "tp"),
        P("sp", "tp"),
        P("sp", "tp"),
        P("sp", "tp"),
        P("sp", "tp"),
        P(),
        P(None, "tp"),
        P(None, "tp"),
        P(None, "tp"),
        P("tp"),
        P("sp", "tp"),
        P("tp"),
        P("tp"),
    )
    out_specs = (P("sp", "tp"), P("sp", "tp"))
    return jax.shard_map(shards, mesh=mesh, in_specs=in_specs, out_specs=out_specs, check_vma=False)
```

```python
import jax
import jax.numpy as jnp
import numpy as np
from jax import lax
from jax.experimental import pallas as pl
from jax.experimental.pallas import tpu as pltpu
from jax.sharding import PartitionSpec as P

UNROTATED_WIDTH = 128
ROPE = 64
VALUE_WIDTH = 128
SSM_DIM = 64
SSM_STATE = 128


eps = 1e-06
theta = 10000.0
floor_score = -1e30


def from_behind(value, axis, steps):
    count = lax.axis_size(axis)
    initial, last = (max(0, -steps), min(count, count - steps))
    return lax.ppermute(value, axis, [(source, source + steps) for source in range(initial, last)])


def rms_scale(values, gain):
    wide = values.astype(jnp.float32)
    return wide * lax.rsqrt(jnp.mean(wide * wide, axis=-1, keepdims=True) + eps) * gain


def rotate(values, positions):
    half = values.shape[-1] // 2
    freqs = theta ** (-jnp.arange(half, dtype=jnp.float32) * 2.0 / values.shape[-1])
    angle = positions.astype(jnp.float32)[:, None] * freqs[None, :]
    cosine = jnp.cos(angle)
    sine = jnp.sin(angle)
    if values.ndim == 3:
        cosine = cosine[:, None, :]
        sine = sine[:, None, :]
    first = values[..., :half]
    second = values[..., half:]
    return jnp.concatenate(
        [first * cosine - second * sine, second * cosine + first * sine], axis=-1
    )


def short_conv(values, edge, taps):
    span = taps.shape[0]
    length = values.shape[0]
    padded = jnp.concatenate([edge, values], axis=0).astype(jnp.float32)
    result = jnp.zeros(values.shape, jnp.float32)
    for index in range(span):
        result = result + taps[index].astype(jnp.float32)[None, :] * padded[index : index + length]
    return jax.nn.silu(result).astype(jnp.bfloat16)


def local_scan(heads, steps, decays, writes, reads):
    length = decays.shape[-1]
    running = jnp.einsum(
        "grs,ls->grl",
        decays,
        jnp.tril(jnp.ones((length, length), jnp.float32)),
        precision=lax.Precision.HIGHEST,
    )
    causal = jnp.tril(jnp.ones((length, length), dtype=bool))
    spread = jnp.where(causal, running[..., :, None] - running[..., None, :], -jnp.inf)
    inner = jnp.einsum("gln,gsn->gls", reads, writes, preferred_element_type=jnp.float32)
    mixing = inner[:, None] * jnp.exp(spread) * steps[:, :, None, :]
    within = jnp.einsum(
        "grls,grsp->grlp",
        mixing.astype(jnp.bfloat16),
        heads,
        preferred_element_type=jnp.float32,
    )
    to_end = jnp.exp(running[..., -1:] - running) * steps
    weighted = (heads.astype(jnp.float32) * to_end[..., None]).astype(jnp.bfloat16)
    state = jnp.einsum(
        "grsp,gsn->grpn", weighted, writes, preferred_element_type=jnp.float32
    )
    return running, state, within


def exchange(items, plane, name, number, columns=False):
    devices, cores = lax.axis_size("sp"), lax.axis_size("tp")
    planes = devices // plane
    counts = [{"plane": plane, "line": planes, "all": devices}[item[1]] for item in items]
    amount = len(items)
    starts = [sum(counts[:i]) for i in range(amount)]
    shared = any(item[2] for item in items)

    def kernel(*refs):
        ins, outs = refs[:amount], refs[amount : 2 * amount]
        send, recv, pass_send, pass_recv, own = refs[2 * amount :]
        here, core = lax.axis_index("sp"), lax.axis_index("tp")
        across, within = here // plane, here % plane

        def place(reach, step):
            if reach == "plane":
                slot = (within + step + plane) % plane
                return across * plane + slot, slot
            if reach == "line":
                slot = (across + step + planes) % planes
                return slot * plane + within, slot
            up, along = step // plane, step % plane
            if step < 0:
                up, along = -((-step) // plane), -((-step) % plane)
            slot = (across + up + planes) % planes * plane + (within + along + plane) % plane
            return slot, slot

        barrier = pltpu.get_barrier_semaphore()
        greeted = 0
        for reach in ("plane", "line"):
            if not any(item[1] in (reach, "all") for item in items):
                continue
            size = {"plane": plane, "line": planes}[reach]
            for step in range(1, size):
                pl.semaphore_signal(
                    barrier,
                    inc=1,
                    device_id=(place(reach, step)[0], core),
                    device_id_type=pl.DeviceIdType.MESH,
                )
                greeted += 1
        if shared:
            for turn in range(1, cores):
                pl.semaphore_signal(
                    barrier,
                    inc=1,
                    device_id=(here, (core + turn) % cores),
                    device_id_type=pl.DeviceIdType.MESH,
                )
                greeted += 1
        pl.semaphore_wait(barrier, greeted)

        def target(i, slot, who):
            if columns:
                size = ins[i].shape[-1]
                return outs[i].at[:, pl.ds(pl.multiple_of(slot * size, size), size)]
            return outs[i].at[slot, who] if items[i][2] else outs[i].at[slot]

        def sent(i, step):
            goal, goal_slot = place(items[i][1], step)
            mine = place(items[i][1], 0)[1]
            if items[i][1] == "all" and step % plane and step >= plane:
                from_line = place("all", -(step // plane * plane))[1]
                return pltpu.make_async_remote_copy(
                    src_ref=target(i, from_line, core),
                    dst_ref=target(i, from_line, core),
                    send_sem=send.at[starts[i] + step],
                    recv_sem=recv.at[starts[i] + step],
                    device_id=(place("plane", step % plane)[0], core),
                    device_id_type=pl.DeviceIdType.MESH,
                )
            return pltpu.make_async_remote_copy(
                src_ref=ins[i].at[goal_slot] if items[i][3] else ins[i],
                dst_ref=target(i, mine, core),
                send_sem=send.at[starts[i] + step],
                recv_sem=recv.at[starts[i] + step],
                device_id=(goal, core),
                device_id_type=pl.DeviceIdType.MESH,
            )

        def arrived(i, step):
            slot = place(items[i][1], -step)[1]
            return pltpu.make_async_remote_copy(
                src_ref=ins[i].at[slot] if items[i][3] else ins[i],
                dst_ref=target(i, slot, core),
                send_sem=send.at[starts[i] + step],
                recv_sem=recv.at[starts[i] + step],
                device_id=(here, core),
                device_id_type=pl.DeviceIdType.MESH,
            )

        def passed(i, step, turn, outgoing):
            slot = place(items[i][1], -step)[1]
            other = (core + turn) % cores
            owner = core if outgoing else (core - turn + cores) % cores
            return pltpu.make_async_remote_copy(
                src_ref=ins[i] if step == 0 else target(i, slot, core),
                dst_ref=target(i, slot, owner),
                send_sem=pass_send.at[(starts[i] + step) * cores + turn],
                recv_sem=pass_recv.at[(starts[i] + step) * cores + turn],
                device_id=(here, other),
                device_id_type=pl.DeviceIdType.MESH,
            )

        kept = []
        for i in range(amount):
            if items[i][1] == "all":
                for up in range(1, planes):
                    sent(i, up * plane).start()
                for step in range(1, plane):
                    sent(i, step).start()
        for i in range(amount):
            if items[i][1] != "all":
                for step in range(1, counts[i]):
                    sent(i, step).start()
        for i in range(amount):
            slot = place(items[i][1], 0)[1]
            local = pltpu.make_async_copy(
                ins[i].at[slot] if items[i][3] else ins[i], target(i, slot, core), own.at[i]
            )
            local.start()
            kept.append(local)
            if items[i][2]:
                for turn in range(1, cores):
                    passed(i, 0, turn, True).start()
        for i in range(amount):
            if items[i][1] == "all":
                for up in range(1, planes):
                    arrived(i, up * plane).wait_recv()
                    for step in range(up * plane + 1, (up + 1) * plane):
                        sent(i, step).start()
                    for turn in range(1, cores):
                        passed(i, up * plane, turn, True).start()
        for i in range(amount):
            for step in range(1, counts[i]):
                if items[i][1] == "all" and step % plane == 0:
                    continue
                arrived(i, step).wait_recv()
                if items[i][2]:
                    for turn in range(1, cores):
                        passed(i, step, turn, True).start()
        for i in range(amount):
            kept[i].wait()
            for step in range(counts[i]):
                if step > 0:
                    sent(i, step).wait_send()
                if items[i][2]:
                    for turn in range(1, cores):
                        passed(i, step, turn, True).wait_send()
                        passed(i, step, turn, False).wait_recv()

    shapes = []
    for (array, reach, over, selected), count in zip(items, counts):
        lead = (count, cores) if over else (count,)
        tail = array.shape[1:] if selected else array.shape
        if columns:
            lead, tail = (), (tail[0], count * tail[1])
        shapes.append(jax.ShapeDtypeStruct(lead + tail, array.dtype))
    slots = sum(counts)
    return pl.pallas_call(
        kernel,
        out_shape=shapes,
        in_specs=[pl.BlockSpec(memory_space=pltpu.VMEM)] * amount,
        out_specs=[pl.BlockSpec(memory_space=pl.ANY)] * amount,
        scratch_shapes=[
            pltpu.SemaphoreType.DMA((slots,)),
            pltpu.SemaphoreType.DMA((slots,)),
            pltpu.SemaphoreType.DMA((slots * cores,)),
            pltpu.SemaphoreType.DMA((slots * cores,)),
            pltpu.SemaphoreType.DMA((amount,)),
        ],
        compiler_params=pltpu.CompilerParams(
            collective_id=number, has_side_effects=True, vmem_limit_bytes=16 * 1024 * 1024
        ),
        cost_estimate=pl.CostEstimate(
            flops=10**8, bytes_accessed=4 * 2**20, transcendentals=0
        ),
        name=name,
    )(*[item[0] for item in items])


def plain_exchange(items, plane):
    results = []
    for array, reach, over, selected in items:
        value = array
        if over:
            value = lax.all_gather(value, "tp")
        if reach == "plane":
            value = value if selected else value[None]
        else:
            value = lax.all_gather(value, "sp")
        results.append(value)
    return results


def gated_norm(mixed, gate, gain):
    length = mixed.shape[0]
    groups = mixed.shape[1]
    flat = mixed.reshape(length, groups, -1)
    gated = flat * jax.nn.silu(gate.astype(jnp.float32)).reshape(length, groups, -1)
    scaled = gated * lax.rsqrt(jnp.mean(gated * gated, axis=-1, keepdims=True) + eps)
    return (scaled * gain.reshape(groups, -1)[None]).reshape(length, -1).astype(jnp.bfloat16)


def attend(query, cosine, sine, keys, key_up, value_up_weight, length):
    heads = key_up.shape[1] // UNROTATED_WIDTH
    latent_width = key_up.shape[0]
    whole = UNROTATED_WIDTH + ROPE
    half = ROPE // 2
    step = 2 * length if keys.shape[0] % (2 * length) == 0 else length
    scale = whole ** (-0.5)
    contract = (((1,), (1,)), ((), ()))

    def kernel(q_ref, cos_ref, sin_ref, k_ref, ku_ref, vu_ref, out_ref, q_all, top, total, summed):
        start = lax.axis_index("sp") * length
        for h in range(heads):
            base = h * whole
            turn = q_ref[:, base + UNROTATED_WIDTH : base + whole].astype(jnp.float32)
            first, second = turn[:, :half], turn[:, half:]
            turned = jnp.concatenate(
                [
                    first * cos_ref[...] - second * sin_ref[...],
                    second * cos_ref[...] + first * sin_ref[...],
                ],
                axis=1,
            )
            q_all[h] = jnp.concatenate(
                [q_ref[:, base : base + UNROTATED_WIDTH], turned.astype(jnp.bfloat16)], axis=1
            )
        top[...] = jnp.full(top.shape, floor_score, jnp.float32)
        total[...] = jnp.zeros(total.shape, jnp.float32)
        summed[...] = jnp.zeros(summed.shape, jnp.float32)
        row = start + lax.broadcasted_iota(jnp.int32, (length, step), 0)
        column = lax.broadcasted_iota(jnp.int32, (length, step), 1)

        def visit(j, carry):
            at = pl.ds(pl.multiple_of(j * step, step), step)
            latent = k_ref[at, :latent_width]
            turned = k_ref[at, latent_width : latent_width + ROPE]
            seen = column + j * step <= row
            plain = jnp.dot(latent, ku_ref[...], preferred_element_type=jnp.float32).astype(
                jnp.bfloat16
            )
            all_values = jnp.dot(latent, vu_ref[...], preferred_element_type=jnp.float32).astype(
                jnp.bfloat16
            )
            for h in range(heads):
                values = all_values[:, h * VALUE_WIDTH : (h + 1) * VALUE_WIDTH]
                key = jnp.concatenate(
                    [plain[:, h * UNROTATED_WIDTH : (h + 1) * UNROTATED_WIDTH], turned], axis=1
                )
                scores = (
                    lax.dot_general(q_all[h], key, contract, preferred_element_type=jnp.float32)
                    * scale
                )
                scores = jnp.where(seen, scores, -jnp.inf)
                old = top[h][:, :1]
                new = jnp.maximum(old, jnp.max(scores, axis=1, keepdims=True))
                weights = jnp.exp(scores - new)
                shrink = jnp.exp(old - new)
                now = jnp.sum(weights, axis=1, keepdims=True)
                total[h] = total[h] * shrink + now
                summed[h] = summed[h] * shrink + jnp.dot(
                    weights.astype(jnp.bfloat16), values, preferred_element_type=jnp.float32
                )
                top[h] = jnp.broadcast_to(new, top.shape[1:])
            return carry

        lax.fori_loop(0, (start + length + step - 1) // step, visit, 0)
        for h in range(heads):
            out_ref[:, h * VALUE_WIDTH : (h + 1) * VALUE_WIDTH] = (
                summed[h] / total[h][:, :1]
            ).astype(jnp.bfloat16)

    return pl.pallas_call(
        kernel,
        out_shape=jax.ShapeDtypeStruct((length, heads * VALUE_WIDTH), jnp.bfloat16),
        in_specs=[pl.BlockSpec(memory_space=pltpu.VMEM)] * 6,
        out_specs=pl.BlockSpec(memory_space=pltpu.VMEM),
        scratch_shapes=[
            pltpu.VMEM((heads, length, whole), jnp.bfloat16),
            pltpu.VMEM((heads, length, 128), jnp.float32),
            pltpu.VMEM((heads, length, 128), jnp.float32),
            pltpu.VMEM((heads, length, VALUE_WIDTH), jnp.float32),
        ],
        compiler_params=pltpu.CompilerParams(vmem_limit_bytes=40 * 1024 * 1024),
        cost_estimate=pl.CostEstimate(
            flops=4 * 10**10, bytes_accessed=4 * 2**20, transcendentals=0
        ),
        name="attend",
    )(query, cosine, sine, keys, key_up, value_up_weight)


def fused(
    plane,
    tokens,
    mix_gain,
    query_proj,
    compressed_projection,
    compressed_norm_gain,
    rope_proj,
    key_up,
    value_up_weight,
    scan_input,
    scan_gate,
    scan_write,
    scan_read,
    step_proj,
    conv_input,
    conv_write,
    conv_read,
    decay_log,
    decay_offset,
    skip_gain,
    group_gain,
):
    devices, cores = lax.axis_size("sp"), lax.axis_size("tp")
    planes = devices // plane
    part, width = tokens.shape
    length = part * cores
    depth = scan_input.shape[0]
    kblock = depth * plane
    hw, ww = scan_input.shape[1] // plane, scan_write.shape[1] // plane
    lower, wide = hw + 2 * ww, 2 * hw + 2 * ww
    bounds = ((0, lower), (lower, wide))
    own_heads = decay_log.shape[0] // plane
    heads = key_up.shape[1] // UNROTATED_WIDTH
    latent_width = key_up.shape[0]
    key_rows = (latent_width + ROPE) * part // 128
    whole = UNROTATED_WIDTH + ROPE
    half = ROPE // 2
    scale = whole ** (-0.5)
    span = conv_input.shape[0]
    edge = 8
    bf16, f32 = jnp.bfloat16, jnp.float32
    MESH = pl.DeviceIdType.MESH
    last_contract = (((1,), (1,)), ((), ()))
    first_contract = (((0,), (0,)), ((), ()))
    best = lax.Precision.HIGHEST
    group_step = 2

    def mm(a, b):
        return jnp.dot(a, b, preferred_element_type=f32)

    def kernel(
        *refs
    ):
        sources, (att_out, scan_out) = refs[:loaded], refs[loaded : loaded + 2]
        targets = refs[loaded + 2 : 2 * loaded + 2]
        (
            w_in, w_write, w_read, w_gate, tok, mix, comp, comp_gain, rope, freqs, wq, ku, vu,
            doff, w_step, t_in, t_write, t_read, ggain, dlog, skip,
        ) = targets
        (
            load_sem, packed, wbuf, rows, keys, q_all, top, total, summed, stepw, steps, osend,
            obuf, projf, gatef, cbuf, ybuf, runs, before, decayed, state, dsum, ssend, tsend,
            srecv, trecv, incoming, stage, wsend, wrecv, zsend, ksend_up, ksend_plane,
            ksend_core, krecv, rsend, rsend_core, rrecv, rdiag_send,
            rhalf, o_send, o_recv, e_send, e_recv, s_send, s_recv, t_send, t_recv,
            out_send, out_recv,
        ) = refs[2 * loaded + 2 :]
        here, core = lax.axis_index("sp"), lax.axis_index("tp")
        z, n = here // plane, here % plane
        other = cores - 1 - core
        beside, above, across = n + 1 - 2 * (n % 2), (n + 2) % plane, plane - 1 - n
        at_end = (z == 0) | (z == planes - 1)
        nearest = (z + planes - 1) // planes
        farthest = planes - 1 - z

        loads = [
            pltpu.make_async_copy(source, target, load_sem.at[i])
            for i, (source, target) in enumerate(zip(sources, targets))
        ]
        for load in loads:
            load.start()

        def rcopy(src, dst, ss, rs, sp, c):
            return pltpu.make_async_remote_copy(
                src_ref=src, dst_ref=dst, send_sem=ss, recv_sem=rs,
                device_id=(sp, c), device_id_type=MESH,
            )

        def turned_slot(flip):
            return (n // 2 + flip // 2) % 2 * 2 + (n + flip) % 2

        def peer(step):
            return z * plane + (n + step) % plane

        barrier = pltpu.get_barrier_semaphore()
        greeted = 0
        for step in range(1, plane):
            pl.semaphore_signal(barrier, inc=1, device_id=(peer(step), core), device_id_type=MESH)
            greeted += 1
        for step in range(1, planes):
            pl.semaphore_signal(
                barrier, inc=1, device_id=((z + step) % planes * plane + n, core),
                device_id_type=MESH,
            )
            greeted += 1
        pl.semaphore_signal(barrier, inc=1, device_id=(here, other), device_id_type=MESH)
        greeted += 1
        for load in loads[:4]:
            load.wait()

        for m in range(plane):
            packed[m, :, :hw] = w_in[:, m * hw : (m + 1) * hw]
            packed[m, :, hw : hw + ww] = w_write[:, m * ww : (m + 1) * ww]
            packed[m, :, hw + ww : lower] = w_read[:, m * ww : (m + 1) * ww]
            packed[m, :, lower:] = w_gate[:, m * hw : (m + 1) * hw]
        wbuf[here] = packed[n]

        pl.semaphore_wait(barrier, greeted)

        def key_slot(sp, c):
            return keys.at[sp * cores + c]

        def key_copy(sp, c, ss, to_sp, to_c):
            return rcopy(
                key_slot(sp, c), key_slot(sp, c), ss, krecv.at[sp * cores + c], to_sp, to_c
            )

        def key_arrived(sp, c):
            key_copy(sp, c, ksend_up.at[0], here, core).wait_recv()

        def key_up_copy(d):
            return key_copy(here, core, ksend_up.at[d], here + d * plane, core)

        sides = (beside, above)

        def key_plane_copy(d, step):
            return key_copy(
                here - d * plane, core, ksend_plane.at[d * plane + step], peer(step), core
            )

        def key_core_copy(sp):
            return key_copy(sp, core, ksend_core.at[sp], here, other)

        sides = (beside, above)

        def chunk(group, index):
            low, high = bounds[group]
            return wbuf.at[index, :, low:high]

        def w_arrived(group, index):
            rcopy(
                chunk(group, index), chunk(group, index), zsend.at[0, group, index],
                wrecv.at[group, index], here, core,
            ).wait_recv()

        def w_plane_copy(group, step):
            low, high = bounds[group]
            goal = turned_slot(step)
            return rcopy(
                packed.at[goal, :, low:high], chunk(group, here), wsend.at[group, step],
                wrecv.at[group, here], z * plane + goal, core,
            )

        def z_copy(group, index, up):
            return rcopy(
                chunk(group, index), chunk(group, index), zsend.at[up, group, index],
                wrecv.at[group, index], here + (plane if up else -plane), core,
            )

        def has_next(up):
            return z + 1 < planes if up else z > 0

        def own_weights(group, steps_of):
            for step in steps_of:
                index = z * plane + turned_slot(step)
                if step:
                    w_arrived(group, index)
                for up in (0, 1):
                    @pl.when(has_next(up))
                    def _():
                        z_copy(group, index, up).start()

        def far_weights(group, d, forward, pieces=range(plane), ways=(0, 1)):
            for up in ways:
                source = z - d if up else z + d
                exists = (source >= 0) & (source < planes)
                gate = has_next(up) if forward else jnp.logical_not(has_next(up))

                @pl.when(exists & gate)
                def _():
                    for step in pieces:
                        index = source * plane + turned_slot(step)
                        w_arrived(group, index)
                        if forward:
                            z_copy(group, index, up).start()

        for step in range(1, plane):
            w_plane_copy(0, step).start()
        own_weights(0, (0,))
        own_weights(1, (0,))

        for load in loads[4:10]:
            load.wait()
        def normed_rows(values, gain, count):
            mean = jnp.sum(values * values, axis=-1, keepdims=True) / count
            return values * lax.rsqrt(mean + eps) * gain

        normed = normed_rows(tok[...].astype(f32), mix[...], width).astype(bf16)

        def rows_at(slot, c):
            return pl.ds(pl.multiple_of(slot * length + c * part, part), part)

        for p in range(planes):
            rows[p, rows_at(n, core), :] = normed[:, p * kblock : (p + 1) * kblock]

        def angles(start, count):
            position = (start + lax.broadcasted_iota(jnp.int32, (count, 1), 0)).astype(f32)
            angle = position * freqs[...]
            return jnp.cos(angle), jnp.sin(angle)

        def turn(first, second, cosine, sine):
            return [first * cosine - second * sine, second * cosine + first * sine]

        latent = normed_rows(mm(normed, comp[...]), comp_gain[...], latent_width)
        small = lax.dot_general(normed, rope[...], last_contract, preferred_element_type=f32)
        cosine, sine = angles(here * length + core * part, part)
        own_slot = here * cores + core
        for low in range(0, latent_width, 128):
            keys[own_slot, low * part // 128 : (low + 128) * part // 128] = latent[
                :, low : low + 128
            ].astype(bf16)
        turned_key = jnp.concatenate(
            turn(small[:, :half], small[:, half:], cosine, sine), axis=1
        ).astype(bf16)
        keys[own_slot, latent_width * part // 128 :] = jnp.concatenate(
            [turned_key[: part // 2], turned_key[part // 2 :]], axis=1
        )

        for d in range(1, planes):
            @pl.when(z + d < planes)
            def _():
                key_up_copy(d).start()
        key_core_copy(here).start()

        def row_copy(slot, ss, to_sp, to_c):
            at = rows.at[:, rows_at(slot, core), :]
            return rcopy(at, at, ss, rrecv.at[slot * cores + core], to_sp, to_c)

        def row_part(slot, part_of, ss, rs, to_sp):
            low, high = part_of * planes // 2, (part_of + 1) * planes // 2
            at = rows.at[low:high, rows_at(slot, core), :]
            return rcopy(at, at, ss, rs, to_sp, core)

        def row_plane_copy(side, part_of):
            return row_part(
                n, part_of, rsend.at[side, part_of], rhalf.at[n, part_of],
                z * plane + sides[side],
            )

        def row_half_arrived(slot, part_of):
            row_part(
                slot, part_of, rsend.at[0, 0], rhalf.at[slot, part_of], here
            ).wait_recv()

        def row_relay(side):
            slot = sides[side]
            return row_part(
                slot, side, rdiag_send.at[side], rhalf.at[slot, side],
                z * plane + sides[1 - side],
            )

        def row_core_copy(slot):
            return row_copy(slot, rsend_core.at[slot], here, other)

        def row_arrived(slot, c):
            at = rows.at[:, rows_at(slot, c), :]
            rcopy(at, at, rsend.at[0], rrecv.at[slot * cores + c], here, core).wait_recv()

        def offset_copy(step):
            goal = (n + step) % plane
            return rcopy(
                osend.at[goal], obuf.at[n], o_send.at[step], o_recv.at[n],
                z * plane + goal, core,
            )

        row_core_copy(n).start()

        positions = plane * length
        at_edge = rows.at[:, positions : positions + edge, :]
        closing = (n == plane - 1) & (core == cores - 1)

        def edge_up_copy():
            return rcopy(
                rows.at[:, positions - edge : positions, :], at_edge, e_send.at[0], e_recv,
                here + plane, core,
            )

        def edge_plane_copy(step):
            return rcopy(at_edge, at_edge, e_send.at[step], e_recv, peer(step), core)

        def edge_core_copy():
            return rcopy(at_edge, at_edge, e_send.at[plane], e_recv, here, other)

        def edge_arrived():
            rcopy(at_edge, at_edge, e_send.at[0], e_recv, here, core).wait_recv()

        @pl.when(closing & (z + 1 < planes))
        def _():
            edge_up_copy().start()

        for load in loads[10:]:
            load.wait()
        for m in range(plane):
            osend[m, :own_heads] = doff[m * own_heads : (m + 1) * own_heads]
        obuf[n] = osend[n]

        @pl.when(z == 0)
        def _():
            rows[:, plane * length :, :] = jnp.zeros((planes, edge, kblock), bf16)

        row_arrived(n, other)
        own_rows = pl.ds(pl.multiple_of(n * length, length), length)
        query = mm(rows[0, own_rows, :], wq[:kblock, :])
        for p in range(1, planes):
            query += mm(rows[p, own_rows, :], wq[p * kblock : (p + 1) * kblock, :])
        query = query.astype(bf16)
        cosine, sine = angles(here * length, length)
        for h in range(heads):
            base = h * whole
            rope_part = query[:, base + UNROTATED_WIDTH : base + whole].astype(f32)
            q_all[h] = jnp.concatenate(
                [query[:, base : base + UNROTATED_WIDTH]]
                + [
                    v.astype(bf16)
                    for v in turn(rope_part[:, :half], rope_part[:, half:], cosine, sine)
                ],
                axis=1,
            )
        top[...] = jnp.full(top.shape, floor_score, f32)
        total[...] = jnp.zeros(total.shape, f32)
        summed[...] = jnp.zeros(summed.shape, f32)

        own_weights(0, range(1, plane))
        for step in range(1, plane):
            key_plane_copy(0, step).start()
        for d in range(1, planes):
            @pl.when(z >= d)
            def _():
                key_arrived(here - d * plane, core)
                for step in range(1, plane):
                    key_plane_copy(d, step).start()
                key_core_copy(here - d * plane).start()

        @pl.when(closing & (z > 0))
        def _():
            edge_arrived()
            for step in range(1, plane):
                edge_plane_copy(step).start()
            edge_core_copy().start()

        for step in range(1, plane):
            w_plane_copy(1, step).start()
        for first in (0, 1):
            for side in (0, 1):
                row_plane_copy(side, (side + first) % 2).start()
        for step in range(1, plane):
            offset_copy(step).start()

        def pass_keys(d):
            for step in range(1, plane):
                sp = (z - d) * plane + (n + step) % plane
                key_arrived(sp, core)
                key_core_copy(sp).start()

        def other_keys(d):
            for q in range(plane):
                key_arrived((z - d) * plane + q, other)

        size = group_step * length
        row = lax.broadcasted_iota(jnp.int32, (length, size), 0)
        column = lax.broadcasted_iota(jnp.int32, (length, size), 1)

        def visit(first_block, limit):
            count = group_step * cores
            block = keys[pl.ds(first_block * cores, count)]
            lat = jnp.concatenate(
                [
                    block[:, low * part // 128 : (low + 128) * part // 128].reshape(size, 128)
                    for low in range(0, latent_width, 128)
                ],
                axis=1,
            )
            turned = block[:, latent_width * part // 128 :]
            turned = jnp.concatenate([turned[:, :, :ROPE], turned[:, :, ROPE:]], axis=1)
            turned = turned.reshape(size, ROPE)
            plain = mm(lat, ku[...]).astype(bf16)
            all_values = mm(lat, vu[...]).astype(bf16)
            if limit is not None:
                seen = column <= row + limit
            for h in range(heads):
                values = all_values[:, h * VALUE_WIDTH : (h + 1) * VALUE_WIDTH]
                key = jnp.concatenate(
                    [plain[:, h * UNROTATED_WIDTH : (h + 1) * UNROTATED_WIDTH], turned], axis=1
                )
                scores = (
                    lax.dot_general(q_all[h], key, last_contract, preferred_element_type=f32)
                    * scale
                )
                if limit is not None:
                    scores = jnp.where(seen, scores, -jnp.inf)
                old = top[h][:, :1]
                new = jnp.maximum(old, jnp.max(scores, axis=1, keepdims=True))
                weights = jnp.exp(scores - new)
                shrink = jnp.exp(old - new)
                now = jnp.sum(weights, axis=1, keepdims=True)
                total[h] = total[h] * shrink + now
                summed[h] = summed[h] * shrink + mm(weights.astype(bf16), values)
                top[h] = jnp.broadcast_to(new, top.shape[1:])

        pass_keys(0)

        @pl.when(z >= 1)
        def _():
            pass_keys(1)

        far_weights(0, 1, True)
        other_keys(0)

        def near(j, carry):
            visit(z * plane + j * group_step, (n - j * group_step) * length)
            return carry

        lax.fori_loop(0, n // group_step + 1, near, 0)

        late = min(2, planes - 1)

        def further(d, carry):
            @pl.when(z > d)
            def _():
                pass_keys(d + 1)

            @pl.when(d == late)
            def _():
                for far in range(2, planes - 1):
                    far_weights(0, far, True, range(plane // 2))

            @pl.when(z >= d)
            def _():
                other_keys(d)

                def inner(j, carry):
                    visit((z - d) * plane + j * group_step, None)
                    return carry

                lax.fori_loop(0, plane // group_step, inner, 0)

            @pl.when(d == late)
            def _():
                for far in range(2, planes - 1):
                    far_weights(0, far, True, range(plane // 2, plane))
                own_weights(1, range(1, plane))

            @pl.when((d == late) & (z == 1))
            def _():
                far_weights(1, 1, True, ways=(1,))

            return carry

        lax.fori_loop(1, planes, further, 0)
        for h in range(heads):
            att_out[:, h * VALUE_WIDTH : (h + 1) * VALUE_WIDTH] = (
                summed[h] / total[h][:, :1]
            ).astype(bf16)

        @pl.when((z > 0) & (core == cores - 1) & (n < plane - 1))
        def _():
            edge_arrived()
            edge_core_copy().start()

        for side in (0, 1):
            row_half_arrived(sides[side], side)
            row_relay(side).start()
        for side in (0, 1):
            row_half_arrived(sides[side], 1 - side)
            row_core_copy(sides[side]).start()
        for d in range(1, planes - 1):
            far_weights(0, d, False)

        def tile(k):
            return pl.ds(pl.multiple_of(k * length, length), length)

        def project(p, values, group):
            low, high = bounds[group]
            block = wbuf[pl.ds(p * plane, plane), :, low:high]
            return mm(values, block.reshape(kblock, high - low))

        def sum_near(group, at, store):
            @pl.when(at_end)
            def _():
                out = project(nearest, rows[nearest, at, :], group)
                for p in range(1, planes - 1):
                    out += project(nearest + p, rows[nearest + p, at, :], group)
                store(out, False)

            @pl.when(jnp.logical_not(at_end))
            def _():
                out = project(0, rows[0, at, :], group)
                for p in range(1, planes):
                    out += project(p, rows[p, at, :], group)
                store(out, False)

        def sum_far(group, at, store):
            store(project(farthest, rows[farthest, at, :], group), True)

        def into(low, count):
            def store(out, add):
                at = pl.ds(low, count)
                projf[at, :] = projf[at, :] + out if add else out

            return store

        def edge_sum(method):
            method(0, pl.ds(positions, edge), into(0, edge))

        def tile_sum(method, k):
            method(0, tile(k), into(pl.multiple_of(k * length + edge, edge), length))

        lane = lax.broadcasted_iota(jnp.int32, (128, w_step.shape[0]), 0)
        which = lax.broadcasted_iota(jnp.int32, (128, w_step.shape[0]), 1)
        first_head = (core * plane + n) * own_heads
        chosen = ((which == lane + first_head) & (lane < own_heads)).astype(bf16)
        stepw[...] = mm(chosen, w_step[...]).astype(bf16)

        def step_tile(k):
            raw = jnp.zeros((length, 128), f32)
            for p in range(planes):
                raw += lax.dot_general(
                    rows[p, tile(k), :], stepw[:, p * kblock : (p + 1) * kblock],
                    last_contract, preferred_element_type=f32,
                )
            steps[k] = jnp.maximum(raw, 0.0) + jnp.log1p(jnp.exp(-jnp.abs(raw)))

        @pl.when((z > 0) & (core < cores - 1))
        def _():
            edge_arrived()

        edge_sum(sum_near)

        def first_sums(flip, carry):
            slot = turned_slot(flip)

            @pl.when(flip == plane - 1)
            def _():
                for part_of in (0, 1):
                    row_half_arrived(across, part_of)
                row_core_copy(across).start()

            @pl.when(flip > 0)
            def _():
                row_arrived(slot, other)

            tile_sum(sum_near, slot)
            step_tile(slot)
            return carry

        lax.fori_loop(0, plane, first_sums, 0)
        far_weights(1, 1, True, ways=(0,))

        @pl.when(z > 1)
        def _():
            far_weights(1, 1, True, ways=(1,))

        far_weights(0, planes - 1, False)

        @pl.when(at_end)
        def _():
            edge_sum(sum_far)

            def last_sums(k, carry):
                tile_sum(sum_far, k)
                return carry

            lax.fori_loop(0, plane, last_sums, 0)


        for d in range(2, planes - 1):
            far_weights(1, d, True, range(plane // 2), (1,))

        taps = jnp.concatenate(
            [
                t_in[:, pl.ds(pl.multiple_of(n * hw, hw), hw)],
                t_write[:, pl.ds(pl.multiple_of(n * ww, ww), ww)],
                t_read[:, pl.ds(pl.multiple_of(n * ww, ww), ww)],
            ],
            axis=1,
        ).astype(f32)

        def conv_tile(k, carry):
            base = pl.ds(pl.multiple_of(k * length, length), length + edge)
            for low in range(0, lower, 128):
                at = slice(low, low + 128)
                values = projf[base, at].astype(bf16).astype(f32)
                result = jnp.zeros((length, 128), f32)
                for i in range(span):
                    shift = edge - span + 1 + i
                    result = result + taps[i : i + 1, at] * values[shift : shift + length]
                cbuf[tile(k), at] = (result * jax.nn.sigmoid(result)).astype(bf16)
            return carry

        lax.fori_loop(0, plane, conv_tile, 0)

        for step in range(1, plane):
            slot = (n - step + plane) % plane
            rcopy(
                obuf.at[slot], obuf.at[slot], o_send.at[0], o_recv.at[slot], here, core
            ).wait_recv()
        lane_row = lax.broadcasted_iota(jnp.int32, (1, 128), 1)
        rate = jnp.zeros((1, 128), f32)
        for h in range(own_heads):
            rate = jnp.where(lane_row == h, dlog[n * own_heads + h], rate)
        rate = -jnp.exp(rate)
        causal = lax.broadcasted_iota(jnp.int32, (length, length), 0) >= lax.broadcasted_iota(
            jnp.int32, (length, length), 1
        )
        tri = causal.astype(f32)

        def per_lane(columns):
            return jnp.concatenate(
                [
                    jnp.broadcast_to(columns[:, h : h + 1], (columns.shape[0], SSM_DIM))
                    for h in range(own_heads)
                ],
                axis=1,
            )

        def per_row(values):
            return jnp.concatenate(
                [
                    jnp.broadcast_to(values[:, h : h + 1], (SSM_DIM, SSM_STATE))
                    for h in range(own_heads)
                ],
                axis=0,
            )

        state[...] = jnp.zeros(state.shape, f32)
        dsum[...] = jnp.zeros(dsum.shape, f32)

        def scan_tile(k, carry):
            step_col = steps[k]
            off_col = jnp.concatenate(
                [obuf[k], jnp.zeros((128 - obuf.shape[1], length), f32)], axis=0
            ).T
            decay = jnp.where(lane_row < own_heads, rate * step_col + off_col, 0.0)
            running = jnp.dot(tri, decay, precision=best, preferred_element_type=f32)
            runs[k] = running
            run_row, step_row = running.T, step_col.T
            x = cbuf[tile(k), :hw]
            w = cbuf[tile(k), hw : hw + ww]
            r = cbuf[tile(k), hw + ww : lower]
            inner = lax.dot_general(r, w, last_contract, preferred_element_type=f32)
            for h in range(own_heads):
                at = slice(h * SSM_DIM, (h + 1) * SSM_DIM)
                spread = jnp.where(
                    causal, running[:, h : h + 1] - run_row[h : h + 1, :], -jnp.inf
                )
                mixing = inner * jnp.exp(spread) * step_row[h : h + 1, :]
                ybuf[tile(k), at] = (
                    mm(mixing.astype(bf16), x[:, at])
                    + skip[n * own_heads + h] * x[:, at].astype(f32)
                )
            last = running[length - 1 : length, :]
            to_end = jnp.exp(last - running) * step_col
            weighted = (x.astype(f32) * per_lane(to_end)).astype(bf16)
            update = lax.dot_general(weighted, w, first_contract, preferred_element_type=f32)
            before[k] = state[...]
            decayed[k] = dsum[...]
            state[...] = per_row(jnp.exp(last)) * state[...] + update
            dsum[...] = dsum[...] + last
            return carry

        lax.fori_loop(0, plane, scan_tile, 0)

        def state_arrived(p):
            rcopy(ssend, srecv.at[p], s_send.at[0], s_recv.at[p], here, core).wait_recv()
            rcopy(tsend, trecv.at[p], t_send.at[0], t_recv.at[p], here, core).wait_recv()

        def state_copies(d):
            to = here + d * plane
            return (
                rcopy(ssend, srecv.at[z], s_send.at[d], s_recv.at[z], to, core),
                rcopy(tsend, trecv.at[z], t_send.at[d], t_recv.at[z], to, core),
            )

        def to_send(d):
            if d == 1:
                return z + 1 < planes
            return (z == 0) & (d + 1 < planes)

        gather_all = (z > 0) & (z + 2 == planes)

        def gather_states():
            @pl.when(z == 0)
            def _():
                incoming[...] = jnp.zeros(incoming.shape, f32)

            @pl.when(z > 0)
            def _():
                state_arrived(0)

            @pl.when(z == 1)
            def _():
                incoming[...] = srecv[0].astype(f32)

            @pl.when(z > 1)
            def _():
                incoming[...] = (
                    per_row(jnp.exp(trecv[z - 1][:1])) * srecv[0].astype(f32)
                    + srecv[z - 1].astype(f32)
                )

        @pl.when((z > 1) & (z + 1 < planes))
        def _():
            state_arrived(z - 1)

        @pl.when((z > 1) & (z + 2 < planes))
        def _():
            ssend[...] = (
                per_row(jnp.exp(dsum[:1])) * srecv[z - 1].astype(f32) + state[...]
            ).astype(bf16)
            tsend[...] = dsum[...] + trecv[z - 1]

        @pl.when(gather_all)
        def _():
            gather_states()
            ssend[...] = (per_row(jnp.exp(dsum[:1])) * incoming[...] + state[...]).astype(bf16)
            tsend[...] = dsum[...]

        @pl.when((z <= 1) & jnp.logical_not(gather_all))
        def _():
            ssend[...] = state[...].astype(bf16)
            tsend[...] = dsum[...]

        for d in range(1, planes):
            @pl.when(to_send(d))
            def _():
                for copy in state_copies(d):
                    copy.start()

        for d in range(2, planes - 1):
            far_weights(1, d, True, range(plane // 2, plane), (1,))
            far_weights(1, d, True, ways=(0,))
        for d in range(1, planes - 1):
            far_weights(1, d, False)

        def gate_tile(k, carry):
            def store(out, add):
                gatef[tile(k), :] = out

            sum_near(1, tile(k), store)
            return carry

        lax.fori_loop(0, plane, gate_tile, 0)
        @pl.when(z + 1 == planes)
        def _():
            state_arrived(z - 1)
            incoming[...] = srecv[z - 1].astype(f32)

        @pl.when((z + 1 < planes) & jnp.logical_not(gather_all))
        def _():
            gather_states()

        far_weights(1, planes - 1, False)
        own_columns = pl.ds(pl.multiple_of(n * hw, hw), hw)
        gain = ggain[:, own_columns]

        def out_copy(k):
            return rcopy(
                stage.at[k], scan_out.at[:, own_columns], out_send.at[k], out_recv.at[n],
                z * plane + k, core,
            )

        def finish(i, carry):
            k = turned_slot(plane - 1 - i)

            @pl.when(at_end)
            def _():
                def store(out, add):
                    gatef[tile(k), :] = gatef[tile(k), :] + out

                sum_far(1, tile(k), store)

            gate = gatef[tile(k), :].astype(bf16).astype(f32)
            entered = (
                before[k] + per_row(jnp.exp(decayed[k][:1])) * incoming[...]
            ).astype(bf16)
            carried = lax.dot_general(
                cbuf[tile(k), hw + ww : lower], entered, last_contract,
                preferred_element_type=f32,
            )
            mixed = ybuf[tile(k), :] + carried * per_lane(jnp.exp(runs[k]))
            gated = mixed * (gate * jax.nn.sigmoid(gate))
            out = normed_rows(gated, gain, hw).astype(bf16)
            stage[k] = out

            @pl.when(k != n)
            def _():
                out_copy(k).start()

            @pl.when(k == n)
            def _():
                scan_out[:, own_columns] = out

            return carry

        lax.fori_loop(0, plane, finish, 0)
        for step in range(1, plane):
            slot = (n + step) % plane
            at = scan_out.at[:, pl.ds(pl.multiple_of(slot * hw, hw), hw)]
            rcopy(stage.at[0], at, out_send.at[0], out_recv.at[slot], here, core).wait_recv()

        for d in range(1, planes):
            @pl.when(z + d < planes)
            def _():
                key_up_copy(d).wait_send()

            @pl.when(to_send(d))
            def _():
                for copy in state_copies(d):
                    copy.wait_send()

        for d in range(planes):
            @pl.when(z >= d)
            def _():
                for step in range(1, plane):
                    key_plane_copy(d, step).wait_send()
                for q in range(plane):
                    key_core_copy((z - d) * plane + q).wait_send()
        for step in range(1, plane):
            for group in (0, 1):
                w_plane_copy(group, step).wait_send()
            offset_copy(step).wait_send()
            out_copy((n + step) % plane).wait_send()
        for side in (0, 1):
            for part_of in (0, 1):
                row_plane_copy(side, part_of).wait_send()
            row_relay(side).wait_send()
        for slot in range(plane):
            row_core_copy(slot).wait_send()

        @pl.when(closing & (z + 1 < planes))
        def _():
            edge_up_copy().wait_send()

        @pl.when(closing & (z > 0))
        def _():
            for step in range(1, plane):
                edge_plane_copy(step).wait_send()

        @pl.when((z > 0) & (core == cores - 1))
        def _():
            edge_core_copy().wait_send()

        for up in (0, 1):
            for p in range(planes):
                @pl.when(((p <= z) if up else (p >= z)) & has_next(up))
                def _():
                    for q in range(plane):
                        for group in (0, 1):
                            z_copy(group, p * plane + q, up).wait_send()

    vmem = pl.BlockSpec(memory_space=pltpu.VMEM)
    hbm = pl.BlockSpec(memory_space=pltpu.HBM)
    freqs = np.float32(theta) ** (-np.arange(half, dtype=np.float32) * np.float32(2.0 / ROPE))
    inputs = (
        scan_input,
        scan_write,
        scan_read,
        scan_gate,
        tokens,
        mix_gain[None, :],
        compressed_projection,
        compressed_norm_gain[None, :],
        rope_proj.T,
        jnp.asarray(freqs[None, :], f32),
        query_proj,
        key_up,
        value_up_weight,
        decay_offset.T,
        step_proj.T,
        conv_input,
        conv_write,
        conv_read,
        group_gain[None, :],
        decay_log,
        skip_gain,
    )
    loaded = len(inputs)
    dma = pltpu.SemaphoreType.DMA
    positions = plane * length
    results = (
        jax.ShapeDtypeStruct((length, heads * VALUE_WIDTH), bf16),
        jax.ShapeDtypeStruct((length, scan_input.shape[1]), bf16),
    )
    outs = pl.pallas_call(
        kernel,
        out_shape=results,
        in_specs=[hbm] * loaded,
        out_specs=(vmem, vmem),
        scratch_shapes=[pltpu.VMEM(value.shape, value.dtype) for value in inputs[:-2]]
        + [pltpu.SMEM(value.shape, value.dtype) for value in inputs[-2:]]
        + [
            dma((loaded,)),
            pltpu.VMEM((plane, depth, wide), bf16),
            pltpu.VMEM((devices, depth, wide), bf16),
            pltpu.VMEM((planes, positions + edge, kblock), bf16),
            pltpu.VMEM((devices * cores, key_rows, 128), bf16),
            pltpu.VMEM((heads, length, whole), bf16),
            pltpu.VMEM((heads, length, 128), f32),
            pltpu.VMEM((heads, length, 128), f32),
            pltpu.VMEM((heads, length, VALUE_WIDTH), f32),
            pltpu.VMEM((128, width), bf16),
            pltpu.VMEM((plane, length, 128), f32),
            pltpu.VMEM((plane, 8, length), f32),
            pltpu.VMEM((plane, 8, length), f32),
            pltpu.VMEM((edge + positions, lower), f32),
            pltpu.VMEM((positions, hw), f32),
            pltpu.VMEM((positions, lower), bf16),
            pltpu.VMEM((positions, hw), f32),
            pltpu.VMEM((plane, length, 128), f32),
            pltpu.VMEM((plane, own_heads * SSM_DIM, SSM_STATE), f32),
            pltpu.VMEM((plane, 8, 128), f32),
            pltpu.VMEM((own_heads * SSM_DIM, SSM_STATE), f32),
            pltpu.VMEM((8, 128), f32),
            pltpu.VMEM((own_heads * SSM_DIM, SSM_STATE), bf16),
            pltpu.VMEM((8, 128), f32),
            pltpu.VMEM((planes, own_heads * SSM_DIM, SSM_STATE), bf16),
            pltpu.VMEM((planes, 8, 128), f32),
            pltpu.VMEM((own_heads * SSM_DIM, SSM_STATE), f32),
            pltpu.VMEM((plane, length, hw), bf16),
            dma((2, plane)),
            dma((2, devices)),
            dma((2, 2, devices)),
            dma((planes,)),
            dma((devices,)),
            dma((devices,)),
            dma((devices * cores,)),
            dma((2, 2)),
            dma((plane,)),
            dma((plane * cores,)),
            dma((2,)),
            dma((plane, 2)),
            dma((plane,)),
            dma((plane,)),
            dma((plane + 1,)),
            dma,
            dma((planes,)),
            dma((planes,)),
            dma((planes,)),
            dma((planes,)),
            dma((plane,)),
            dma((plane,)),
        ],
        compiler_params=pltpu.CompilerParams(
            collective_id=1, has_side_effects=True, vmem_limit_bytes=48 * 1024 * 1024
        ),
        name="fused",
    )(*[pltpu.with_memory_space_constraint(value, pltpu.HBM) for value in inputs])

    def settle(a_in, b_in, a_out, b_out, sems):
        copies = [
            pltpu.make_async_copy(a_in, a_out, sems.at[0]),
            pltpu.make_async_copy(b_in, b_out, sems.at[1]),
        ]
        for copy in copies:
            copy.start()
        for copy in copies:
            copy.wait()

    return pl.pallas_call(
        settle,
        out_shape=results,
        in_specs=[vmem, vmem],
        out_specs=(hbm, hbm),
        scratch_shapes=[dma((2,))],
        compiler_params=pltpu.CompilerParams(vmem_limit_bytes=4 * 1024 * 1024),
        name="settle",
    )(*outs)


def shards(
    tokens,
    mix_gain,
    query_proj,
    compressed_projection,
    compressed_norm_gain,
    rope_proj,
    key_up,
    value_up_weight,
    scan_input,
    scan_gate,
    scan_write,
    scan_read,
    step_proj,
    conv_input,
    conv_write,
    conv_read,
    decay_log,
    decay_offset,
    skip_gain,
    group_gain,
):
    groups = scan_write.shape[1] // SSM_STATE
    devices, cores = lax.axis_size("sp"), lax.axis_size("tp")
    plane = groups if devices % groups == 0 else 1
    planes = devices // plane
    sp_index, core = lax.axis_index("sp"), lax.axis_index("tp")
    across, within = sp_index // plane, sp_index % plane
    own_groups = groups // plane
    direct = plane > 1
    if direct and cores == 2 and own_groups == 1 and plane == 4 and planes > 1:
        return fused(
            plane,
            tokens,
            mix_gain,
            query_proj,
            compressed_projection,
            compressed_norm_gain,
            rope_proj,
            key_up,
            value_up_weight,
            scan_input,
            scan_gate,
            scan_write,
            scan_read,
            step_proj,
            conv_input,
            conv_write,
            conv_read,
            decay_log,
            decay_offset,
            skip_gain,
            group_gain,
        )

    def move(items, name, number, columns=False):
        if direct:
            return exchange(items, plane, name, number, columns)
        return plain_exchange(items, plane)

    depth = scan_input.shape[0]
    widths = [w.shape[1] // plane for w in (scan_input, scan_gate, scan_write, scan_read)]
    offsets = [sum(widths[:i]) for i in range(4)]
    packed = jnp.stack(
        [
            jnp.concatenate(
                [
                    w[:, n * size : (n + 1) * size]
                    for w, size in zip((scan_input, scan_gate, scan_write, scan_read), widths)
                ],
                axis=1,
            )
            for n in range(plane)
        ]
    )
    (part_weights,) = move([(packed, "plane", False, True)], "weights_in_plane", 1)
    weights = lax.all_gather(
        part_weights.reshape(plane * depth, -1),
        "sp",
        axis=0,
        tiled=True,
        axis_index_groups=[[p * plane + n for p in range(planes)] for n in range(plane)],
    )

    own_normed = rms_scale(tokens, mix_gain).astype(jnp.bfloat16)
    part = tokens.shape[0]
    length = part * cores
    latent_width = compressed_projection.shape[1]
    small = jnp.dot(
        own_normed,
        jnp.concatenate([compressed_projection, rope_proj], axis=1),
        preferred_element_type=jnp.float32,
    )
    latent = rms_scale(small[:, :latent_width], compressed_norm_gain).astype(jnp.bfloat16)
    part_positions = sp_index * length + core * part + jnp.arange(part, dtype=jnp.int32)
    key_turned = rotate(small[:, latent_width:], part_positions).astype(jnp.bfloat16)
    padding = jnp.zeros((part, -(latent_width + ROPE) % 128), jnp.bfloat16)
    own_keys = jnp.concatenate([latent, key_turned, padding], axis=1)
    all_keys, all_rows, offsets_seen = move(
        [
            (own_keys, "all", True, False),
            (own_normed, "plane", True, False),
            (decay_offset.T, "plane", False, False),
        ],
        "rows_and_keys",
        2,
    )
    all_keys = all_keys.reshape(devices * length, -1)
    all_rows = all_rows.reshape(plane * length, -1)
    edge_rows = from_behind(all_rows[plane * length - 8 :], "sp", plane)
    positions = sp_index * length + jnp.arange(length, dtype=jnp.int32)
    rows = lax.dynamic_slice_in_dim(all_rows, within * length, length, 0)
    query = jnp.dot(rows, query_proj, preferred_element_type=jnp.float32).astype(jnp.bfloat16)
    half = ROPE // 2
    freqs = theta ** (-jnp.arange(half, dtype=jnp.float32) * 2.0 / ROPE)
    angle = positions.astype(jnp.float32)[:, None] * freqs[None, :]
    attended = attend(
        query, jnp.cos(angle), jnp.sin(angle), all_keys, key_up, value_up_weight, length
    )

    def own_part(array, axis, size):
        return lax.dynamic_slice_in_dim(array, within * size, size, axis)

    local_heads = decay_log.shape[0]
    own_heads = local_heads // plane
    per_group = local_heads // groups
    step_raw = jnp.dot(
        all_rows,
        lax.dynamic_slice_in_dim(
            step_proj, core * local_heads + within * own_heads, own_heads, 1
        ),
        preferred_element_type=jnp.float32,
    )
    step_size = jax.nn.softplus(step_raw)
    own_offset = own_part(offsets_seen, 1, own_heads)
    step_values = jnp.transpose(step_size.reshape(plane, length, own_heads), (0, 2, 1))
    decay_values = (
        -jnp.exp(own_part(decay_log, 0, own_heads))[None, :, None] * step_values + own_offset
    )

    projected = jnp.dot(all_rows, weights, preferred_element_type=jnp.float32).astype(jnp.bfloat16)
    edge = jnp.dot(edge_rows, weights, preferred_element_type=jnp.float32).astype(jnp.bfloat16)
    span = conv_input.shape[0] - 1

    def convolved(i, taps):
        at = slice(offsets[i], offsets[i] + widths[i])
        return short_conv(projected[:, at], edge[8 - span :, at], own_part(taps, 1, widths[i]))

    head_conv = convolved(0, conv_input)
    gate = projected[:, offsets[1] : offsets[1] + widths[1]]
    writes = convolved(2, conv_write)
    reads = convolved(3, conv_read)
    blocks = plane * own_groups

    def by_block(values, last):
        split = values.reshape(plane, length, own_groups, last)
        return jnp.transpose(split, (0, 2, 1, 3)).reshape(blocks, length, last)

    head_values = jnp.transpose(
        head_conv.reshape(plane, length, own_groups, per_group, SSM_DIM), (0, 2, 3, 1, 4)
    ).reshape(blocks, per_group, length, SSM_DIM)
    write_values = by_block(writes, SSM_STATE)
    read_values = by_block(reads, SSM_STATE)
    running, state, mixed = local_scan(
        head_values,
        step_values.reshape(blocks, per_group, length),
        decay_values.reshape(blocks, per_group, length),
        write_values,
        read_values,
    )
    states = state.reshape(plane, own_heads, SSM_DIM, SSM_STATE)
    totals = running[..., -1].reshape(plane, own_heads)
    before, decayed = [jnp.zeros_like(states[0])], [jnp.zeros_like(totals[0])]
    for index in range(plane):
        before.append(jnp.exp(totals[index])[:, None, None] * before[-1] + states[index])
        decayed.append(totals[index] + decayed[-1])
    sent_total = jnp.pad(decayed[-1][None, :], ((0, 7), (0, 128 - own_heads)))
    seen_states, seen_totals = move(
        [
            (before[-1].reshape(-1, SSM_STATE).astype(jnp.bfloat16), "line", False, False),
            (sent_total, "line", False, False),
        ],
        "states",
        3,
    )
    seen_states = seen_states.reshape(planes, own_heads, SSM_DIM, SSM_STATE).astype(jnp.float32)
    seen_totals = seen_totals[:, 0, :own_heads]
    index = jnp.arange(planes)
    between = (index[None, :] > index[:, None]) & (index[None, :] < across)
    path = jnp.sum(jnp.where(between[:, :, None], seen_totals[None], 0.0), axis=1)
    reached = (index < across)[:, None]
    factor = jnp.where(reached, jnp.exp(path), 0.0)
    incoming = jnp.sum(seen_states * factor[:, :, None, None], axis=0)
    entered = jnp.stack(
        [
            before[k] + jnp.exp(decayed[k])[:, None, None] * incoming
            for k in range(plane)
        ]
    ).reshape(blocks, per_group, SSM_DIM, SSM_STATE)
    carried = jnp.einsum(
        "gln,grpn->grlp",
        read_values,
        entered.astype(jnp.bfloat16),
        preferred_element_type=jnp.float32,
    )
    skip = jnp.broadcast_to(
        own_part(skip_gain, 0, own_heads).reshape(1, own_groups, per_group),
        (plane, own_groups, per_group),
    ).reshape(blocks, per_group, 1, 1)
    mixed = (
        mixed
        + carried * jnp.exp(running)[..., None]
        + skip * head_values.astype(jnp.float32)
    )
    mixed = jnp.transpose(
        mixed.reshape(plane, own_groups, per_group, length, SSM_DIM), (0, 3, 1, 2, 4)
    ).reshape(plane * length, own_groups, per_group, SSM_DIM)
    scanned = gated_norm(mixed, gate, own_part(group_gain, 0, widths[0]))
    (columns,) = move(
        [(scanned.reshape(plane, length, -1), "plane", False, True)], "outputs_in_plane", 4, True
    )
    scanned = columns.reshape(length, -1)
    return (attended, scanned)


def solution(mesh):
    in_specs = (
        P(("sp", "tp"), None),
        P(),
        P(None, "tp"),
        P(),
        P(),
        P(),
        P(None, "tp"),
        P(None, "tp"),
        P("sp", "tp"),
        P("sp", "tp"),
        P("sp", "tp"),
        P("sp", "tp"),
        P(),
        P(None, "tp"),
        P(None, "tp"),
        P(None, "tp"),
        P("tp"),
        P("sp", "tp"),
        P("tp"),
        P("tp"),
    )
    out_specs = (P("sp", "tp"), P("sp", "tp"))
    return jax.shard_map(shards, mesh=mesh, in_specs=in_specs, out_specs=out_specs, check_vma=False)
```
